32 devices in a mesh: sp: 16 (over z, y, x), tp: 2 (over core).
Axes of the slice: x: 2, y: 2, z: 4, core: 2. Of those that a mesh axis runs over, the one named last changes fastest.
Arguments:
- stream_in: bfloat16 [4096, 2048], P('sp'), may hold values from -6 to 6
- norm_gain: float32 [2, 2048], replicated, may hold values from 0.1 to 1.9
- value_weight: bfloat16 [2, 2048, 2048], P(None, 'sp', 'tp'), may hold values from -0.125 to 0.125
- gate_weight: bfloat16 [2, 2048, 2048], P(None, 'sp', 'tp'), may hold values from -0.125 to 0.125
- conv_taps: float32 [2, 31, 2048], P(None, None, 'tp'), may hold values from -5 to 5
- channel_gain: float32 [2, 2048], P(None, 'tp'), may hold values from 0.1 to 1.9
- out_weight: bfloat16 [2, 2048, 2048], P(None, 'tp', 'sp'), may hold values from -0.125 to 0.125
Outputs:
- stream_out: bfloat16 [4096, 2048], P('sp')
The draws below stay inside these ranges and needn't reach their ends.
All inputs are finite; a program needn't handle non-finite values.
Results may differ from the reference program's by a relative error of at most 0.015.
Values may be sent and summed in bfloat16 or wider, within the bound.
A program may use at most 64 MiB of HBM per device.

```python
import jax
import jax.numpy as jnp
from jax import lax

D = 2048
KERNEL = 31
LAYERS = 2
TOKENS = 4096


def draw_conv_taps(key, part):
    first, second = jax.random.split(jax.random.fold_in(key, 17))
    base = jnp.clip(jax.random.normal(first, (LAYERS, KERNEL, D), jnp.float32), -6.0, 6.0)
    blocks = jnp.exp(jax.random.uniform(second, (LAYERS, 1, 8), jnp.float32, -1.4, 1.4))
    scales = jnp.repeat(blocks, D // 8, axis=2)
    return base * scales / jnp.sqrt(jnp.float32(KERNEL))


def block_levels(key, shape, shards, low, top_value):
    def one(axis_at, parts):
        steps = jax.random.uniform(jax.random.fold_in(jax.random.fold_in(key, 6), axis_at), (parts,), jnp.float32, low / len(shards), top_value / len(shards))
        return jnp.repeat(jnp.exp(steps), shape[axis_at] // parts).reshape((-1,) + (1,) * (len(shape) - axis_at - 1))

    level = one(*shards[0])
    for cut in shards[1:]:
        level = level * one(*cut)
    return level


def scatter_about(rng, shape, width, limit, cuts=(), held_as=jnp.bfloat16):
    array = width * jax.random.normal(rng, shape, jnp.float32)
    if cuts:
        array = array * block_levels(rng, shape, cuts, -0.22, 0.18)
    return jnp.clip(array, -limit, limit).astype(held_as)


def setup_inputs(seed: int = 0) -> dict:
    splits = jax.random.split(jax.random.key(seed), 8)
    return {
        "stream_in": scatter_about(splits[0], (TOKENS, D), 1.0, 6.0, ((0, 16),)),
        "norm_gain": jnp.clip(1.0 + 0.18 * jax.random.normal(splits[1], (LAYERS, D), jnp.float32), 0.1, 1.9),
        "value_weight": scatter_about(splits[2], (LAYERS, D, D), D ** -0.5, 0.125, ((1, 16), (2, 2))),
        "gate_weight": scatter_about(splits[3], (LAYERS, D, D), D ** -0.5, 0.125, ((1, 16), (2, 2))),
        "conv_taps": draw_conv_taps(jax.random.fold_in(splits[7], 71), 0),
        "channel_gain": jnp.clip(1.0 + 0.18 * jax.random.normal(splits[5], (LAYERS, D), jnp.float32), 0.1, 1.9),
        "out_weight": scatter_about(splits[6], (LAYERS, D, D), D ** -0.5, 0.125, ((1, 2), (2, 16))),
    }


epsilon = 1e-05

def reference(stream_in, norm_gain, value_weight, gate_weight, conv_taps, channel_gain, out_weight):
    stream = stream_in
    for layer in range(LAYERS):
        wide = stream.astype(jnp.float32)
        normed = (wide * lax.rsqrt(lax.optimization_barrier(jnp.mean(wide * wide, axis=1, keepdims=True)) + epsilon) * norm_gain[layer]).astype(jnp.bfloat16)
        value = jnp.dot(normed, value_weight[layer], preferred_element_type=jnp.float32)
        gate = jnp.dot(normed, gate_weight[layer], preferred_element_type=jnp.float32)
        gated = (value * jax.nn.sigmoid(gate)).astype(jnp.bfloat16)
        padded = jnp.concatenate([jnp.zeros((KERNEL - 1, D), jnp.bfloat16), gated], axis=0).astype(jnp.float32)
        filtered = jnp.zeros((TOKENS, D), jnp.float32)
        for tap in range(KERNEL):
            filtered = filtered + conv_taps[layer, tap] * padded[tap:tap + TOKENS]
        mean_value = lax.optimization_barrier(jnp.mean(filtered, axis=1, keepdims=True))
        variance = lax.optimization_barrier(jnp.mean(filtered * filtered, axis=1, keepdims=True)) - mean_value * mean_value
        activated = jax.nn.silu((filtered - mean_value) * lax.rsqrt(variance + epsilon) * channel_gain[layer]).astype(jnp.bfloat16)
        branch = jnp.dot(activated, out_weight[layer], preferred_element_type=jnp.float32)
        stream = (wide + branch).astype(jnp.bfloat16)
    return stream
```

```python
import functools

import jax
import jax.numpy as jnp
from jax import lax
from jax.experimental import pallas as pl
from jax.experimental.pallas import tpu as pltpu
from jax.sharding import PartitionSpec as P

epsilon = 1e-05
MESH = pl.DeviceIdType.MESH
F32 = jnp.float32
BF16 = jnp.bfloat16
PAD = 32
CHUNK = 256
PARTS = 2


def kernel(n, layers, taps_n, stream_in, gain, vw, gw, taps, cgain, ow, out,
           wvg, wo, nrm, gat, fil, act, ssend, srecv, dsend, drecv,
           asend, arecv, bsend, brecv, mine, through, strm,
           loc_sem, wx_send, wx_recv, z_send, z_recv, msg_send, msg_recv):
    planes = n // 4
    s = lax.axis_index("sp")
    c = lax.axis_index("tp")
    z, q = s // 4, s % 4
    y, x = q // 2, q % 2
    quad = [q, q + 1 - 2 * x, q + 2 - 4 * y, 3 - q]
    toks, width = stream_in.shape
    group = 4 * toks
    rows, cols = vw.shape[1], vw.shape[2]
    ch = cols // 4
    half = width // 2
    near = (1 - c) * quad[1] + c * quad[2]
    far = c * quad[1] + (1 - c) * quad[2]
    diag = quad[3]
    near_dev, far_dev, core_dev = (z * 4 + near, c), (z * 4 + far, c), (s, 1 - c)
    up_dev, down_dev = (s + 4, c), (s - 4, c)

    def al(v, m):
        return pl.multiple_of(v, m)

    barrier = pltpu.get_barrier_semaphore()
    plane_devs = [(z * 4 + quad[k], cc) for k in range(4) for cc in (c, 1 - c)][1:]
    for dev in plane_devs:
        pl.semaphore_signal(barrier, inc=1, device_id=dev, device_id_type=MESH)

    @pl.when(z < planes - 1)
    def _():
        pl.semaphore_signal(barrier, inc=1, device_id=up_dev, device_id_type=MESH)

    @pl.when(z > 0)
    def _():
        pl.semaphore_signal(barrier, inc=1, device_id=down_dev, device_id_type=MESH)

    pl.semaphore_wait(barrier, len(plane_devs) + (z < planes - 1).astype(jnp.int32)
                      + (z > 0).astype(jnp.int32))

    shared = {}

    def share(l, kind):
        mine_rows = pl.ds(al(s * rows, rows), rows)
        for k in range(4):
            span = pl.ds(al(quad[k] * ch, ch), ch)
            if kind == 2:
                src, dst = ow.at[l, span, :], wo.at[l, :, mine_rows]
            else:
                src = (vw, gw)[kind].at[l, :, span]
                dst = wvg.at[l, mine_rows, pl.ds(kind * ch, ch)]
            idx = l * 3 + kind
            if k == 0:
                copy = pltpu.make_async_copy(src, dst, loc_sem.at[idx])
            else:
                copy = pltpu.make_async_remote_copy(
                    src, dst, wx_send.at[idx, k], wx_recv.at[idx, k],
                    device_id=(z * 4 + quad[k], c), device_id_type=MESH)
            copy.start()
            shared[l, kind, k] = copy

    def z_copy(l, grp, d, t, hop, k):
        plane = z - t if d == 0 else z + t
        block = pl.ds(al((plane * 4 + quad[k]) * rows, rows), rows)
        ref = wvg.at[l, block, :] if grp == 0 else wo.at[l, :, block]
        idx = (l * 2 + grp) * 2 + d
        return pltpu.make_async_remote_copy(
            ref, ref, z_send.at[idx, hop, k], z_recv.at[idx, hop, k],
            device_id=up_dev if d == 0 else down_dev, device_id_type=MESH)

    def holds(d, t):
        return z >= t if d == 0 else z + t < planes

    def sends(d):
        return z < planes - 1 if d == 0 else z > 0

    sent = []

    def pump(l, grp, t):
        for k in range(4):
            if t == 0:
                for kind in ((0, 1) if grp == 0 else (2,)):
                    shared[l, kind, k].wait()
            for d in range(2):
                @pl.when(holds(d, t) & sends(d))
                def _(k=k, d=d):
                    if t > 0:
                        z_copy(l, grp, d, t, t - 1, k).wait_recv()
                    z_copy(l, grp, d, t, t, k).start()

                sent.append((l, grp, d, t, k))

    def consume(l, grp):
        for t in range(1, planes):
            for d in range(2):
                @pl.when(holds(d, t) & jnp.logical_not(sends(d)))
                def _(t=t, d=d):
                    for k in range(4):
                        z_copy(l, grp, d, t, t - 1, k).wait_recv()

    slots = [0]

    def make(src, dst, dev):
        slot = slots[0]
        slots[0] += 1
        return pltpu.make_async_remote_copy(src, dst, msg_send.at[slot], msg_recv.at[slot],
                                            device_id=dev, device_id_type=MESH)

    def message(src, dst, dev):
        m = make(src, dst, dev)
        m.start()
        return m

    share(0, 0)
    share(0, 1)

    def block_rows(b):
        return pl.ds(al(b * toks, toks), toks)

    def half_cols(h):
        return pl.ds(al(h * half, half), half)

    total_rows = PAD + group
    tile = max(v for v in range(16, 257, 16) if total_rows % v == 0)
    part_rows = group // PARTS
    lanes = 128
    chunks = half // CHUNK
    halos = []

    for l in range(layers):
        last_layer = l + 1 == layers
        source = stream_in if l == 0 else strm.at[l - 1]

        def norm_step(r, _):
            at = al(r * 64, 64)
            wide = source[pl.ds(at, 64), :].astype(F32)
            scale = lax.rsqrt(jnp.mean(wide * wide, axis=1, keepdims=True) + epsilon)
            nrm[l, pl.ds(al(PAD + q * toks + at, 32), 64), :] = (
                wide * scale * gain[l:l + 1, :]).astype(BF16)
            return 0

        lax.fori_loop(0, toks // 64, norm_step, 0)

        @pl.when(z == 0)
        def _():
            nrm[l, 0:PAD, :] = jnp.zeros((PAD, width), BF16)

        def spot(b):
            return nrm.at[l, pl.ds(al(PAD + b * toks, 32), toks), half_cols(c)]

        own_near = message(spot(q), spot(q), near_dev)
        own_far = message(spot(q), spot(q), far_dev)
        if l == 0:
            pump(0, 0, 0)
            share(0, 2)
        own_near.wait()
        passed = message(spot(near), spot(near), far_dev)
        relays = [message(spot(near), spot(near), core_dev)]
        if l == 0:
            pump(0, 0, 1)
            for ll in range(1, layers):
                for kind in range(3):
                    share(ll, kind)
        else:
            pump(l, 1, 1)
        own_far.wait()
        relays.append(message(spot(far), spot(far), core_dev))
        if l == 0:
            for t in range(2, planes - 1):
                pump(0, 0, t)
            pump(0, 1, 0)
        passed.wait()
        relays.append(message(spot(diag), spot(diag), core_dev))
        border = nrm.at[l, pl.ds(group, PAD), half_cols(c)]
        first = nrm.at[l, pl.ds(0, PAD), half_cols(c)]
        halo = make(border, first, up_dev)
        swap_halo = make(first, first, core_dev)
        halos.append(halo)

        @pl.when(z < planes - 1)
        def _():
            halo.start()

        if l > 0:
            for t in range(2, planes - 1):
                pump(l, 1, t)

        @pl.when(z > 0)
        def _():
            halo.wait_recv()
            swap_halo.start()

        for m in relays:
            m.wait()

        @pl.when(z > 0)
        def _():
            swap_halo.wait()

        consume(l, 0)

        def gate_step(r, _):
            at = al(r * tile, tile)
            both = jnp.dot(nrm[l, pl.ds(at, tile), :], wvg[l], preferred_element_type=F32)
            gated = (both[:, :ch] * jax.nn.sigmoid(both[:, ch:])).astype(BF16)
            gat[pl.ds(at, tile), :] = gated.astype(F32)
            return 0

        lax.fori_loop(0, total_rows // tile, gate_step, 0)
        if l == 0:
            pump(0, 1, 1)

        lead = PAD - (taps_n - 1)
        step_rows = 64

        def conv_step(r, _):
            at = al(r * step_rows, step_rows)
            for lane in range(ch // lanes):
                cut = slice(lane * lanes, (lane + 1) * lanes)
                total = jnp.zeros((step_rows, lanes), F32)
                block = gat[pl.ds(at, step_rows + PAD), cut]
                for b in range(8):
                    moved = block if b == 0 else pltpu.roll(block, step_rows + PAD - b, 0)
                    for a in range(PAD // 8 + 1):
                        tap = 8 * a + b - lead
                        if 0 <= tap < taps_n:
                            total = total + taps[l, tap:tap + 1, cut] * moved[8 * a:8 * a + step_rows]
                fil[pl.ds(at, step_rows), cut] = total
            return 0

        per = part_rows // step_rows
        sums = []
        for part in range(PARTS):
            lax.fori_loop(part * per, (part + 1) * per, conv_step, 0)
            wide = fil[part * part_rows:(part + 1) * part_rows, :]
            first_sum = jnp.sum(wide, axis=1, keepdims=True)
            second_sum = jnp.sum(wide * wide, axis=1, keepdims=True)
            lane_id = lax.broadcasted_iota(jnp.int32, (part_rows, lanes), 1)
            stat = jnp.where(lane_id == 0, first_sum, jnp.where(lane_id == 1, second_sum, 0.0))
            ssend[l, part] = jnp.transpose(stat)[0:8, :]
            sums.append([message(ssend.at[l, part], srecv.at[l, part, k], dev)
                         for k, dev in enumerate(plane_devs)])
            if l == 0 and part == 0:
                for t in range(2, planes - 1):
                    pump(0, 1, t)
        if not last_layer:
            pump(l + 1, 0, 0)
        for part in range(PARTS):
            span = slice(part * part_rows, (part + 1) * part_rows)
            for m in sums[part]:
                m.wait()
            whole = ssend[l, part]
            for k in range(len(plane_devs)):
                whole = whole + srecv[l, part, k]
            stat = jnp.transpose(jnp.concatenate(
                [whole, jnp.zeros((lanes - 8, part_rows), F32)], axis=0))
            mean_value = stat[:, 0:1] / width
            variance = stat[:, 1:2] / width - mean_value * mean_value
            act[span, :] = jax.nn.silu((fil[span, :] - mean_value) * lax.rsqrt(variance + epsilon)
                                       * cgain[l:l + 1, pl.ds(al(q * ch, ch), ch)]).astype(BF16)

        consume(l, 1)
        swaps, firsts, seconds, lasts = [], [], [], []

        def out_cols(h, u):
            return pl.ds(al(h * half + u * CHUNK, CHUNK), CHUNK)

        def stage_swap(u):
            weights = wo[l, :, out_cols(1 - c, u)]
            for b in range(4):
                span = slice(b * toks, (b + 1) * toks)
                dsend[l, u, span, :] = jnp.dot(act[span, :], weights,
                                               preferred_element_type=F32).astype(BF16)
            swaps.append(message(dsend.at[l, u], drecv.at[l, u], core_dev))

        def stage_first(u):
            weights = wo[l, :, out_cols(c, u)]
            swaps[u].wait()

            def partial(b):
                return (jnp.dot(act[block_rows(b), :], weights, preferred_element_type=F32)
                        + drecv[l, u, block_rows(b), :].astype(F32))

            asend[l, u, 0] = partial(far).astype(BF16)
            asend[l, u, 1] = partial(diag).astype(BF16)
            firsts.append(message(asend.at[l, u], arecv.at[l, u], far_dev))
            through[u] = partial(near)
            mine[u] = partial(q) + source[:, out_cols(c, u)].astype(F32)

        def stage_second(u):
            firsts[u].wait()
            bsend[l, u] = (through[u] + arecv[l, u, 1].astype(F32)).astype(BF16)
            seconds.append(message(bsend.at[l, u], brecv.at[l, u], near_dev))
            mine[u] = mine[u] + arecv[l, u, 0].astype(F32)

        def stage_last(u):
            seconds[u].wait()
            strm[l, :, out_cols(c, u)] = (mine[u] + brecv[l, u].astype(F32)).astype(BF16)
            piece = strm.at[l, :, out_cols(c, u)]
            lasts.append(message(piece, piece, core_dev))

        lag = 4
        for i in range(chunks + lag + 1):
            if i < chunks:
                stage_swap(i)
            if 1 <= i <= chunks:
                stage_first(i - 1)
            if 0 <= i - lag < chunks:
                stage_second(i - lag)
            if 0 <= i - lag - 1 < chunks:
                stage_last(i - lag - 1)
            if not last_layer and i == 1:
                pump(l + 1, 0, 1)
            if not last_layer and i == 6:
                for t in range(2, planes - 1):
                    pump(l + 1, 0, t)
                pump(l + 1, 1, 0)
        for m in lasts:
            m.wait()

    out[...] = strm[layers - 1]
    for l, grp, d, t, k in sent:
        @pl.when(holds(d, t) & sends(d))
        def _(l=l, grp=grp, d=d, t=t, k=k):
            z_copy(l, grp, d, t, t, k).wait_send()
    for halo in halos:
        @pl.when(z < planes - 1)
        def _(halo=halo):
            halo.wait_send()


def fused(n, layers):
    def body(stream_in, norm_gain, value_weight, gate_weight, conv_taps, channel_gain, out_weight):
        toks, width = stream_in.shape
        taps_n = conv_taps.shape[1]
        rows, cols = value_weight.shape[1], value_weight.shape[2]
        ch, half, group, planes = cols // 4, width // 2, 4 * toks, n // 4
        chunks = half // CHUNK
        q = lax.axis_index("sp") % 4
        taps = lax.dynamic_slice_in_dim(conv_taps, q * ch, ch, axis=2)
        vmem = pl.BlockSpec(memory_space=pltpu.VMEM)
        hbm = pl.BlockSpec(memory_space=pltpu.HBM)
        msgs = layers * (8 + 7 * PARTS + 4 * chunks)
        return pl.pallas_call(
            functools.partial(kernel, n, layers, taps_n),
            out_shape=jax.ShapeDtypeStruct((toks, width), BF16),
            in_specs=[vmem, vmem, hbm, hbm, vmem, vmem, hbm],
            out_specs=vmem,
            scratch_shapes=[
                pltpu.VMEM((layers, width, 2 * ch), BF16),
                pltpu.VMEM((layers, ch, width), BF16),
                pltpu.VMEM((layers, PAD + group, width), BF16),
                pltpu.VMEM((PAD + group, ch), F32),
                pltpu.VMEM((group, ch), F32),
                pltpu.VMEM((group, ch), BF16),
                pltpu.VMEM((layers, PARTS, 8, group // PARTS), F32),
                pltpu.VMEM((layers, PARTS, 7, 8, group // PARTS), F32),
                pltpu.VMEM((layers, chunks, group, CHUNK), BF16),
                pltpu.VMEM((layers, chunks, group, CHUNK), BF16),
                pltpu.VMEM((layers, chunks, 2, toks, CHUNK), BF16),
                pltpu.VMEM((layers, chunks, 2, toks, CHUNK), BF16),
                pltpu.VMEM((layers, chunks, toks, CHUNK), BF16),
                pltpu.VMEM((layers, chunks, toks, CHUNK), BF16),
                pltpu.VMEM((chunks, toks, CHUNK), F32),
                pltpu.VMEM((chunks, toks, CHUNK), F32),
                pltpu.VMEM((layers, toks, width), BF16),
                pltpu.SemaphoreType.DMA((layers * 3,)),
                pltpu.SemaphoreType.DMA((layers * 3, 4)),
                pltpu.SemaphoreType.DMA((layers * 3, 4)),
                pltpu.SemaphoreType.DMA((layers * 4, planes - 1, 4)),
                pltpu.SemaphoreType.DMA((layers * 4, planes - 1, 4)),
                pltpu.SemaphoreType.DMA((msgs,)),
                pltpu.SemaphoreType.DMA((msgs,)),
            ],
            compiler_params=pltpu.CompilerParams(
                collective_id=0, has_side_effects=True, vmem_limit_bytes=62 * 2**20),
        )(stream_in, norm_gain, value_weight, gate_weight, taps, channel_gain, out_weight)

    return body


def passed_along(value, axis, steps):
    count = lax.axis_size(axis)
    leading, last = (max(0, -steps), min(count, count - steps))
    return lax.ppermute(value, axis, [(source, source + steps) for source in range(leading, last)])


def general(stream_in, norm_gain, value_weight, gate_weight, conv_taps, channel_gain, out_weight):
    stream = stream_in
    tok_rows = stream_in.shape[0]
    width = stream_in.shape[1]
    taps_n = conv_taps.shape[1]
    local_cols = value_weight.shape[2]
    for layer in range(norm_gain.shape[0]):
        wide = stream.astype(F32)
        normed = (
            wide
            * lax.rsqrt(jnp.mean(wide * wide, axis=1, keepdims=True) + epsilon)
            * norm_gain[layer]
        ).astype(BF16)
        value = jnp.dot(normed, lax.all_gather(value_weight[layer], "sp", axis=0, tiled=True),
                        preferred_element_type=F32)
        gate = jnp.dot(normed, lax.all_gather(gate_weight[layer], "sp", axis=0, tiled=True),
                       preferred_element_type=F32)
        gated = (value * jax.nn.sigmoid(gate)).astype(BF16)
        earlier = passed_along(gated[tok_rows - (taps_n - 1):], "sp", 1)
        padded = jnp.concatenate([earlier, gated], axis=0).astype(F32)
        taps = conv_taps[layer]
        filtered = jnp.zeros((tok_rows, local_cols), F32)
        for tap in range(taps_n):
            filtered = filtered + taps[tap] * padded[tap:tap + tok_rows]
        sum_first, sum_second = lax.psum(
            (jnp.sum(filtered, axis=1), jnp.sum(filtered * filtered, axis=1)), "tp")
        mean_value = (sum_first / width)[:, None]
        variance = (sum_second / width)[:, None] - mean_value * mean_value
        activated = jax.nn.silu(
            (filtered - mean_value) * lax.rsqrt(variance + epsilon) * channel_gain[layer]
        ).astype(BF16)
        whole_out = lax.all_gather(out_weight[layer], "sp", axis=1, tiled=True)
        terms = jnp.dot(activated, whole_out, preferred_element_type=F32)
        summed = lax.psum(terms.astype(BF16), "tp").astype(F32)
        stream = (wide + summed).astype(BF16)
    return stream


def solution(mesh):
    n, tp = mesh.shape["sp"], mesh.shape["tp"]

    def body(stream_in, norm_gain, value_weight, *rest):
        rows, cols = value_weight.shape[1], value_weight.shape[2]
        quads = tp == 2 and n % 4 == 0 and n >= 8 and rows % 128 == 0 and cols % 512 == 0
        fits = (stream_in.shape[0] % 64 == 0 and rest[1].shape[1] <= PAD
                and stream_in.shape[1] % (2 * CHUNK) == 0)
        chosen = fused(n, norm_gain.shape[0]) if quads and fits else general
        return chosen(stream_in, norm_gain, value_weight, *rest)

    return jax.shard_map(
        body,
        mesh=mesh,
        in_specs=(
            P("sp", None),
            P(),
            P(None, "sp", "tp"),
            P(None, "sp", "tp"),
            P(None, None, "tp"),
            P(None, "tp"),
            P(None, "tp", "sp"),
        ),
        out_specs=P("sp", None),
        check_vma=False,
    )
```

```python
import functools

import jax
import jax.numpy as jnp
from jax import lax
from jax.experimental import pallas as pl
from jax.experimental.pallas import tpu as pltpu
from jax.sharding import PartitionSpec as P

epsilon = 1e-05
MESH = pl.DeviceIdType.MESH
F32 = jnp.float32
BF16 = jnp.bfloat16
PAD = 32
PARTS = 2


def kernel(n, layers, taps_n, stream_hbm, gain_hbm, vw, gw, taps_hbm, cgain_hbm, ow, out,
           stream_in, gain, taps, cgain, wvg, wo, nrm, gat, fil, act, ssend, srecv, dsend, drecv,
           asend, arecv, bsend, brecv, mine, through, strm,
           in_sem, out_sem, loc_sem, wx_send, wx_recv, z_send, z_recv, halo_send, halo_recv,
           msg_send, msg_recv):
    planes = n // 4
    s = lax.axis_index("sp")
    c = lax.axis_index("tp")
    z, q = s // 4, s % 4
    y, x = q // 2, q % 2
    quad = [q, q + 1 - 2 * x, q + 2 - 4 * y, 3 - q]
    toks, width = stream_in.shape
    group = 4 * toks
    rows, cols = vw.shape[1], vw.shape[2]
    ch = cols // 4
    half = width // 2
    chunk = 2 * rows
    near = (1 - c) * quad[1] + c * quad[2]
    far = c * quad[1] + (1 - c) * quad[2]
    diag = quad[3]
    near_dev, far_dev, core_dev = (z * 4 + near, c), (z * 4 + far, c), (s, 1 - c)
    up_dev, down_dev = (s + 4, c), (s - 4, c)

    def al(v, m):
        return pl.multiple_of(v, m)

    barrier = pltpu.get_barrier_semaphore()
    plane_devs = [(z * 4 + quad[k], cc) for k in range(4) for cc in (c, 1 - c)][1:]
    for dev in plane_devs:
        pl.semaphore_signal(barrier, inc=1, device_id=dev, device_id_type=MESH)

    @pl.when(z < planes - 1)
    def _():
        pl.semaphore_signal(barrier, inc=1, device_id=up_dev, device_id_type=MESH)

    @pl.when(z > 0)
    def _():
        pl.semaphore_signal(barrier, inc=1, device_id=down_dev, device_id_type=MESH)

    own_ch = pl.ds(al(q * ch, ch), ch)
    loads = [pltpu.make_async_copy(a, b, in_sem.at[k]) for k, (a, b) in enumerate((
        (stream_hbm, stream_in), (gain_hbm, gain), (taps_hbm.at[:, :, own_ch], taps),
        (cgain_hbm.at[:, own_ch], cgain)))]
    for load in loads:
        load.start()

    shared = {}

    def shared_copy(l, kind, k):
        mine_rows = pl.ds(al(s * rows, rows), rows)
        span = pl.ds(al(quad[k] * ch, ch), ch)
        if kind == 2:
            src, dst = ow.at[l, span, :], wo.at[l, :, mine_rows]
        else:
            src = (vw, gw)[kind].at[l, :, span]
            dst = wvg.at[l, mine_rows, pl.ds(kind * ch, ch)]
        idx = l * 3 + kind
        if k == 0:
            copy = pltpu.make_async_copy(src, dst, loc_sem.at[idx])
        else:
            copy = pltpu.make_async_remote_copy(
                src, dst, wx_send.at[idx, k], wx_recv.at[idx, k],
                device_id=(z * 4 + quad[k], c), device_id_type=MESH)
        copy.start()
        shared[l, kind, k] = copy

    def share(l, kinds, ks=(1, 2, 3)):
        for k in ks:
            for kind in kinds:
                shared_copy(l, kind, k)

    for l in range(layers):
        share(l, (0, 1, 2), (0,))

    pl.semaphore_wait(barrier, len(plane_devs) + (z < planes - 1).astype(jnp.int32)
                      + (z > 0).astype(jnp.int32))

    def z_copy(l, grp, d, t, hop, k):
        plane = z - t if d == 0 else z + t
        if k < 0:
            block = pl.ds(al(plane * 4 * rows, rows), 4 * rows)
        elif l == 0:
            block = pl.ds(al((plane * 4 + quad[k]) * rows, rows), rows)
        else:
            block = pl.ds(al((plane * 4 + 2 * k) * rows, rows), 2 * rows)
        ref = wvg.at[l, block, :] if grp == 0 else wo.at[l, :, block]
        idx = (l * 2 + grp) * 2 + d
        return pltpu.make_async_remote_copy(
            ref, ref, z_send.at[idx, hop], z_recv.at[idx, hop, max(k, 0)],
            device_id=up_dev if d == 0 else down_dev, device_id_type=MESH)

    def pieces(l):
        return 4 if l == 0 else 2

    def holds(d, t):
        return z >= t if d == 0 else z + t < planes

    def sends(d):
        return z < planes - 1 if d == 0 else z > 0

    def pump(l, grp, t):
        kinds = (0, 1) if grp == 0 else (2,)
        if t == 0 and l > 0:
            for k in range(4):
                for kind in kinds:
                    shared[l, kind, k].wait()
        for k in range(pieces(l)):
            if t == 0 and l == 0:
                for kind in kinds:
                    shared[l, kind, k].wait()
            for d in range(2):
                @pl.when(holds(d, t) & sends(d))
                def _(k=k, d=d):
                    if t > 0:
                        z_copy(l, grp, d, t, t - 1, k).wait_recv()
                    z_copy(l, grp, d, t, t, k).start()

    def consume(l, grp, t):
        for d in range(2):
            @pl.when(holds(d, t) & jnp.logical_not(sends(d)))
            def _(d=d):
                for k in range(pieces(l)):
                    z_copy(l, grp, d, t, t - 1, k).wait_recv()

    def drain(l, grp):
        for t in range(planes - 1):
            for d in range(2):
                @pl.when(holds(d, t) & sends(d))
                def _(t=t, d=d):
                    z_copy(l, grp, d, t, t, -1).wait_send()

    slots = [0]

    def make(src, dst, dev):
        slot = slots[0]
        slots[0] += 1
        return pltpu.make_async_remote_copy(src, dst, msg_send.at[slot], msg_recv.at[slot],
                                            device_id=dev, device_id_type=MESH)

    def message(src, dst, dev):
        m = make(src, dst, dev)
        m.start()
        return m

    share(0, (0, 1))
    for load in loads:
        load.wait()

    def block_rows(b):
        return pl.ds(al(b * toks, toks), toks)

    def half_cols(h):
        return pl.ds(al(h * half, half), half)

    unit = toks // 2
    part_rows = group // PARTS
    lanes = 128
    outs = []

    def plane_at(u):
        low = jnp.where(u <= z, z - u, u)
        zm = planes - 1 - z
        high = planes - 1 - jnp.where(u <= zm, zm - u, u)
        return jnp.where(2 * z < planes, low, high)

    for l in range(layers):
        last_layer = l + 1 == layers
        source = stream_in if l == 0 else strm.at[l - 1]

        def norm_step(r, _):
            at = al(r * 64, 64)
            wide = source[pl.ds(at, 64), :].astype(F32)
            scale = lax.rsqrt(jnp.mean(wide * wide, axis=1, keepdims=True) + epsilon)
            nrm[l, pl.ds(al(PAD + q * toks + at, 32), 64), :] = (
                wide * scale * gain[l:l + 1, :]).astype(BF16)
            return 0

        lax.fori_loop(0, toks // 64, norm_step, 0)

        @pl.when(z == 0)
        def _():
            nrm[l, 0:PAD, :] = jnp.zeros((PAD, width), BF16)

        def spot(b, j):
            return nrm.at[l, pl.ds(al(PAD + b * toks + j * unit, 32), unit), half_cols(c)]

        border = nrm.at[l, pl.ds(group, PAD), half_cols(c)]
        first = nrm.at[l, pl.ds(0, PAD), half_cols(c)]

        def halo_copy(k, dev, src, recv):
            return pltpu.make_async_remote_copy(
                src, first, halo_send.at[l, k], halo_recv.at[l, recv],
                device_id=dev, device_id_type=MESH)

        rise = halo_copy(0, up_dev, border, 0)
        spread = [halo_copy(k, (z * 4 + quad[k], c), first, 1) for k in (1, 2, 3)]
        swap_halo = halo_copy(4, core_dev, first, 2)

        @pl.when((q == 3) & (z < planes - 1))
        def _():
            rise.start()

        def halo_spread():
            @pl.when((q == 3) & (z > 0))
            def _():
                rise.wait_recv()
                for m in spread:
                    m.start()
                swap_halo.start()

        def halo_swap():
            @pl.when((q != 3) & (z > 0))
            def _():
                spread[0].wait_recv()
                swap_halo.start()

        def halo_finish():
            @pl.when(z > 0)
            def _():
                swap_halo.wait()

            @pl.when((q == 3) & (z > 0))
            def _():
                for m in spread:
                    m.wait_send()

            @pl.when((q == 3) & (z < planes - 1))
            def _():
                rise.wait_send()

        own_near = [message(spot(q, j), spot(q, j), near_dev) for j in range(2)]
        passed, relays, own_far = [], {}, []

        def to_far(j):
            own_near[j].wait_send()
            own_far.append(message(spot(q, j), spot(q, j), far_dev))

        def pass_on(j):
            own_near[j].wait_recv()
            passed.append(message(spot(near, j), spot(near, j), far_dev))
            relays[1, j] = message(spot(near, j), spot(near, j), core_dev)

        def relay(which, j):
            (own_far if which == 2 else passed)[j].wait()
            b = far if which == 2 else diag
            relays[which, j] = message(spot(b, j), spot(b, j), core_dev)

        def gate_rows(at, size):
            both = jnp.dot(nrm[l, pl.ds(at, size), :], wvg[l], preferred_element_type=F32)
            gated = (both[:, :ch] * jax.nn.sigmoid(both[:, ch:])).astype(BF16)
            gat[pl.ds(at, size), :] = gated.astype(F32)

        def gate_pair(which, j):
            b = (q, near, far, diag)[which]
            gate_rows(al(PAD + b * toks + j * unit, 32), unit)

        if l == 0:
            pump(0, 0, 0)
            halo_spread()
            to_far(0)
            to_far(1)
            pump(0, 0, 1)
            pass_on(0)
            pass_on(1)
            share(0, (2,))
            relay(2, 0)
            relay(2, 1)
            for t in range(2, planes - 1):
                pump(0, 0, t)
            relay(3, 0)
            relay(3, 1)
            for ll in range(1, layers):
                share(ll, (0, 1, 2))
            pump(0, 1, 0)
            pump(0, 1, 1)
            halo_swap()
            for m in relays.values():
                m.wait()
            for t in range(1, planes):
                consume(0, 0, t)
            for which in range(4):
                for j in range(2):
                    gate_pair(which, j)
        else:
            to_far(0)
            to_far(1)
            pass_on(0)
            pass_on(1)
            halo_spread()
            pump(l, 1, 1)
            relay(2, 0)
            relay(2, 1)
            drain(l - 1, 0)
            drain(l - 1, 1)
            relay(3, 0)
            relay(3, 1)
            for t in range(1, planes):
                consume(l, 0, t)
            gate_pair(0, 0)
            gate_pair(0, 1)
            halo_swap()
            for m in relays.values():
                m.wait()
            for which in range(1, 4):
                for j in range(2):
                    gate_pair(which, j)
        halo_finish()
        gate_rows(0, PAD)

        lead = PAD - (taps_n - 1)
        step_rows = 64

        def conv_step(r, _):
            at = al(r * step_rows, step_rows)
            for lane in range(ch // lanes):
                cut = slice(lane * lanes, (lane + 1) * lanes)
                total = jnp.zeros((step_rows, lanes), F32)
                block = gat[pl.ds(at, step_rows + PAD), cut]
                for b in range(8):
                    moved = block if b == 0 else pltpu.roll(block, step_rows + PAD - b, 0)
                    for a in range(PAD // 8 + 1):
                        tap = 8 * a + b - lead
                        if 0 <= tap < taps_n:
                            total = total + taps[tap, l:l + 1, cut] * moved[8 * a:8 * a + step_rows]
                fil[pl.ds(at, step_rows), cut] = total
            return 0

        per = part_rows // step_rows
        sums = []
        for part in range(PARTS):
            lax.fori_loop(part * per, (part + 1) * per, conv_step, 0)
            wide = fil[part * part_rows:(part + 1) * part_rows, :]
            first_sum = jnp.sum(wide, axis=1, keepdims=True)
            second_sum = jnp.sum(wide * wide, axis=1, keepdims=True)
            lane_id = lax.broadcasted_iota(jnp.int32, (part_rows, lanes), 1)
            stat = jnp.where(lane_id == 0, first_sum, jnp.where(lane_id == 1, second_sum, 0.0))
            ssend[l, part] = jnp.transpose(stat)[0:8, :]
            sums.append([message(ssend.at[l, part], srecv.at[l, part, k], dev)
                         for k, dev in enumerate(plane_devs)])
        for t in range(2, planes - 1):
            pump(l, 1, t)
        if not last_layer:
            pump(l + 1, 0, 0)
        for part in range(PARTS):
            span = slice(part * part_rows, (part + 1) * part_rows)
            for m in sums[part]:
                m.wait()
            whole = ssend[l, part]
            for k in range(len(plane_devs)):
                whole = whole + srecv[l, part, k]
            stat = jnp.transpose(jnp.concatenate(
                [whole, jnp.zeros((lanes - 8, part_rows), F32)], axis=0))
            mean_value = stat[:, 0:1] / width
            variance = stat[:, 1:2] / width - mean_value * mean_value
            act[span, :] = jax.nn.silu((fil[span, :] - mean_value) * lax.rsqrt(variance + epsilon)
                                       * cgain[l:l + 1, :]).astype(BF16)

        swaps, firsts, seconds, lasts = [], [], [], []

        def out_cols(h, u):
            return pl.ds(al(plane_at(u) * 4 * rows + h * chunk, chunk), chunk)

        def stage_swap(u):
            if u > 0:
                consume(l, 1, u)
            weights = wo[l, :, out_cols(1 - c, u)]
            for b in range(4):
                span = slice(b * toks, (b + 1) * toks)
                dsend[l, u, span, :] = jnp.dot(act[span, :], weights,
                                               preferred_element_type=F32).astype(BF16)
            swaps.append(message(dsend.at[l, u], drecv.at[l, u], core_dev))

        def stage_first(u):
            weights = wo[l, :, out_cols(c, u)]
            swaps[u].wait()

            def partial(b):
                return (jnp.dot(act[block_rows(b), :], weights, preferred_element_type=F32)
                        + drecv[l, u, block_rows(b), :].astype(F32))

            asend[l, u, 0] = partial(far).astype(BF16)
            asend[l, u, 1] = partial(diag).astype(BF16)
            firsts.append(message(asend.at[l, u], arecv.at[l, u], far_dev))
            through[u] = partial(near)
            mine[u] = partial(q) + source[:, out_cols(c, u)].astype(F32)

        def stage_second(u):
            firsts[u].wait()
            bsend[l, u] = (through[u] + arecv[l, u, 1].astype(F32)).astype(BF16)
            seconds.append(message(bsend.at[l, u], brecv.at[l, u], near_dev))
            mine[u] = mine[u] + arecv[l, u, 0].astype(F32)

        def stage_last(u):
            seconds[u].wait()
            strm[l, :, out_cols(c, u)] = (mine[u] + brecv[l, u].astype(F32)).astype(BF16)
            piece = strm.at[l, :, out_cols(c, u)]
            lasts.append(message(piece, piece, core_dev))
            if last_layer:
                outs.append(pltpu.make_async_copy(piece, out.at[:, out_cols(c, u)], out_sem.at[0, u]))
                outs[-1].start()

        def finish(u):
            lasts[u].wait()
            if last_layer:
                outs.append(pltpu.make_async_copy(
                    strm.at[l, :, out_cols(1 - c, u)], out.at[:, out_cols(1 - c, u)], out_sem.at[1, u]))
                outs[-1].start()

        lag = 4
        for i in range(planes + lag + 1):
            if i < planes:
                stage_swap(i)
            if 1 <= i <= planes:
                stage_first(i - 1)
            if 0 <= i - lag < planes:
                stage_second(i - lag)
            if 0 <= i - lag - 1 < planes:
                stage_last(i - lag - 1)
            if not last_layer and i == 1:
                pump(l + 1, 0, 1)
            if not last_layer and i == 6:
                for t in range(2, planes - 1):
                    pump(l + 1, 0, t)
                pump(l + 1, 1, 0)
            if last_layer and i == planes:
                drain(l, 0)
                drain(l, 1)
        for u in range(planes):
            finish(u)

    for copy in outs:
        copy.wait()


def fused(n, layers):
    def body(stream_in, norm_gain, value_weight, gate_weight, conv_taps, channel_gain, out_weight):
        toks, width = stream_in.shape
        taps_n = conv_taps.shape[1]
        rows, cols = value_weight.shape[1], value_weight.shape[2]
        ch, half, group, planes = cols // 4, width // 2, 4 * toks, n // 4
        chunk = 2 * rows
        taps = jnp.transpose(conv_taps, (1, 0, 2))
        hbm = pl.BlockSpec(memory_space=pltpu.HBM)
        msgs = layers * (12 + 7 * PARTS + 4 * planes)
        return pl.pallas_call(
            functools.partial(kernel, n, layers, taps_n),
            out_shape=jax.ShapeDtypeStruct((toks, width), BF16),
            in_specs=[hbm] * 7,
            out_specs=hbm,
            scratch_shapes=[
                pltpu.VMEM((toks, width), BF16),
                pltpu.VMEM((layers, width), F32),
                pltpu.VMEM((taps_n, layers, ch), F32),
                pltpu.VMEM((layers, ch), F32),
                pltpu.VMEM((layers, width, 2 * ch), BF16),
                pltpu.VMEM((layers, ch, width), BF16),
                pltpu.VMEM((layers, PAD + group, width), BF16),
                pltpu.VMEM((PAD + group, ch), F32),
                pltpu.VMEM((group, ch), F32),
                pltpu.VMEM((group, ch), BF16),
                pltpu.VMEM((layers, PARTS, 8, group // PARTS), F32),
                pltpu.VMEM((layers, PARTS, 7, 8, group // PARTS), F32),
                pltpu.VMEM((layers, planes, group, chunk), BF16),
                pltpu.VMEM((layers, planes, group, chunk), BF16),
                pltpu.VMEM((layers, planes, 2, toks, chunk), BF16),
                pltpu.VMEM((layers, planes, 2, toks, chunk), BF16),
                pltpu.VMEM((layers, planes, toks, chunk), BF16),
                pltpu.VMEM((layers, planes, toks, chunk), BF16),
                pltpu.VMEM((planes, toks, chunk), F32),
                pltpu.VMEM((planes, toks, chunk), F32),
                pltpu.VMEM((layers, toks, width), BF16),
                pltpu.SemaphoreType.DMA((4,)),
                pltpu.SemaphoreType.DMA((2, planes)),
                pltpu.SemaphoreType.DMA((layers * 3,)),
                pltpu.SemaphoreType.DMA((layers * 3, 4)),
                pltpu.SemaphoreType.DMA((layers * 3, 4)),
                pltpu.SemaphoreType.DMA((layers * 4, planes - 1)),
                pltpu.SemaphoreType.DMA((layers * 4, planes - 1, 4)),
                pltpu.SemaphoreType.DMA((layers, 5)),
                pltpu.SemaphoreType.DMA((layers, 3)),
                pltpu.SemaphoreType.DMA((msgs,)),
                pltpu.SemaphoreType.DMA((msgs,)),
            ],
            compiler_params=pltpu.CompilerParams(
                collective_id=0, has_side_effects=True, vmem_limit_bytes=62 * 2**20),
        )(stream_in, norm_gain, value_weight, gate_weight, taps, channel_gain, out_weight)

    return body


def passed_along(value, axis, steps):
    count = lax.axis_size(axis)
    leading, last = (max(0, -steps), min(count, count - steps))
    return lax.ppermute(value, axis, [(source, source + steps) for source in range(leading, last)])


def general(stream_in, norm_gain, value_weight, gate_weight, conv_taps, channel_gain, out_weight):
    stream = stream_in
    tok_rows = stream_in.shape[0]
    width = stream_in.shape[1]
    taps_n = conv_taps.shape[1]
    local_cols = value_weight.shape[2]
    for layer in range(norm_gain.shape[0]):
        wide = stream.astype(F32)
        normed = (
            wide
            * lax.rsqrt(jnp.mean(wide * wide, axis=1, keepdims=True) + epsilon)
            * norm_gain[layer]
        ).astype(BF16)
        value = jnp.dot(normed, lax.all_gather(value_weight[layer], "sp", axis=0, tiled=True),
                        preferred_element_type=F32)
        gate = jnp.dot(normed, lax.all_gather(gate_weight[layer], "sp", axis=0, tiled=True),
                       preferred_element_type=F32)
        gated = (value * jax.nn.sigmoid(gate)).astype(BF16)
        earlier = passed_along(gated[tok_rows - (taps_n - 1):], "sp", 1)
        padded = jnp.concatenate([earlier, gated], axis=0).astype(F32)
        taps = conv_taps[layer]
        filtered = jnp.zeros((tok_rows, local_cols), F32)
        for tap in range(taps_n):
            filtered = filtered + taps[tap] * padded[tap:tap + tok_rows]
        sum_first, sum_second = lax.psum(
            (jnp.sum(filtered, axis=1), jnp.sum(filtered * filtered, axis=1)), "tp")
        mean_value = (sum_first / width)[:, None]
        variance = (sum_second / width)[:, None] - mean_value * mean_value
        activated = jax.nn.silu(
            (filtered - mean_value) * lax.rsqrt(variance + epsilon) * channel_gain[layer]
        ).astype(BF16)
        whole_out = lax.all_gather(out_weight[layer], "sp", axis=1, tiled=True)
        terms = jnp.dot(activated, whole_out, preferred_element_type=F32)
        summed = lax.psum(terms.astype(BF16), "tp").astype(F32)
        stream = (wide + summed).astype(BF16)
    return stream


def solution(mesh):
    n, tp = mesh.shape["sp"], mesh.shape["tp"]

    def body(stream_in, norm_gain, value_weight, *rest):
        rows, cols = value_weight.shape[1], value_weight.shape[2]
        quads = tp == 2 and n % 4 == 0 and n >= 8 and rows % 128 == 0 and cols % 512 == 0
        fits = stream_in.shape[0] % 64 == 0 and rest[1].shape[1] <= PAD
        chosen = fused(n, norm_gain.shape[0]) if quads and fits else general
        return chosen(stream_in, norm_gain, value_weight, *rest)

    return jax.shard_map(
        body,
        mesh=mesh,
        in_specs=(
            P("sp", None),
            P(),
            P(None, "sp", "tp"),
            P(None, "sp", "tp"),
            P(None, None, "tp"),
            P(None, "tp"),
            P(None, "tp", "sp"),
        ),
        out_specs=P("sp", None),
        check_vma=False,
    )
```

```python
import functools

import jax
import jax.numpy as jnp
from jax import lax
from jax.experimental import pallas as pl
from jax.experimental.pallas import tpu as pltpu
from jax.sharding import PartitionSpec as P

epsilon = 1e-05
MESH = pl.DeviceIdType.MESH
F32 = jnp.float32
BF16 = jnp.bfloat16
PAD = 32
PARTS = 2


def kernel(n, layers, taps_n, stream_hbm, gain_hbm, vw, gw, taps_hbm, cgain_hbm, ow, out,
           stream_in, gain, taps, cgain, wvg, wo, nrm, gat, fil, act, ssend, srecv, dsend, drecv,
           asend, arecv, bsend, brecv, mine, through, strm, acc, turn,
           in_sem, out_sem, loc_sem, wx_send, wx_recv, z_send, z_recv, halo_send, halo_recv,
           msg_send, msg_recv):
    planes = n // 4
    s = lax.axis_index("sp")
    c = lax.axis_index("tp")
    z, q = s // 4, s % 4
    y, x = q // 2, q % 2
    quad = [q, q + 1 - 2 * x, q + 2 - 4 * y, 3 - q]
    toks, width = stream_in.shape
    group = 4 * toks
    rows, cols = vw.shape[1], vw.shape[2]
    ch = cols // 4
    half = width // 2
    chunk = 2 * rows
    near = (1 - c) * quad[1] + c * quad[2]
    far = c * quad[1] + (1 - c) * quad[2]
    diag = quad[3]
    near_dev, far_dev, core_dev = (z * 4 + near, c), (z * 4 + far, c), (s, 1 - c)
    up_dev, down_dev = (s + 4, c), (s - 4, c)

    def al(v, m):
        return pl.multiple_of(v, m)

    barrier = pltpu.get_barrier_semaphore()
    plane_devs = [(z * 4 + quad[k], cc) for k in range(4) for cc in (c, 1 - c)][1:]
    for dev in plane_devs:
        pl.semaphore_signal(barrier, inc=1, device_id=dev, device_id_type=MESH)

    @pl.when(z < planes - 1)
    def _():
        pl.semaphore_signal(barrier, inc=1, device_id=up_dev, device_id_type=MESH)

    @pl.when(z > 0)
    def _():
        pl.semaphore_signal(barrier, inc=1, device_id=down_dev, device_id_type=MESH)

    own_ch = pl.ds(al(q * ch, ch), ch)
    loads = [pltpu.make_async_copy(a, b, in_sem.at[k]) for k, (a, b) in enumerate((
        (stream_hbm, stream_in), (gain_hbm, gain), (taps_hbm.at[:, :, own_ch], taps),
        (cgain_hbm.at[:, own_ch], cgain)))]
    for load in loads:
        load.start()

    shared = {}

    def shared_copy(l, kind, k):
        mine_rows = pl.ds(al(s * rows, rows), rows)
        span = pl.ds(al(quad[k] * ch, ch), ch)
        if kind == 2:
            src, dst = ow.at[l, span, :], wo.at[l, :, mine_rows]
        else:
            src = (vw, gw)[kind].at[l, :, span]
            dst = wvg.at[l, mine_rows, pl.ds(kind * ch, ch)]
        idx = l * 3 + kind
        if k == 0:
            copy = pltpu.make_async_copy(src, dst, loc_sem.at[idx])
        else:
            copy = pltpu.make_async_remote_copy(
                src, dst, wx_send.at[idx, k - 1], wx_recv.at[idx, k - 1],
                device_id=(z * 4 + quad[k], c), device_id_type=MESH)
        copy.start()
        shared[l, kind, k] = copy

    def share(l, kinds, ks=(1, 2, 3)):
        for k in ks:
            for kind in kinds:
                shared_copy(l, kind, k)

    for l in range(layers):
        share(l, (0, 1, 2), (0,))

    pl.semaphore_wait(barrier, len(plane_devs) + (z < planes - 1).astype(jnp.int32)
                      + (z > 0).astype(jnp.int32))

    def z_copy(l, grp, d, t, hop, k):
        plane = z - t if d == 0 else z + t
        if k < 0:
            block = pl.ds(al(plane * 4 * rows, rows), 4 * rows)
        elif pieces(l, grp) == 4:
            block = pl.ds(al((plane * 4 + quad[k]) * rows, rows), rows)
        else:
            block = pl.ds(al((plane * 4 + 2 * k) * rows, rows), 2 * rows)
        ref = wvg.at[l, block, :] if grp == 0 else wo.at[l, :, block]
        idx = (l * 2 + grp) * 2 + d
        return pltpu.make_async_remote_copy(
            ref, ref, z_send.at[idx, hop], z_recv.at[first_recv(l, grp) + (d * (planes - 1) + hop) * pieces(l, grp) + max(k, 0)],
            device_id=up_dev if d == 0 else down_dev, device_id_type=MESH)

    def pieces(l, grp):
        return 4 if (l, grp) == (0, 0) else 2

    def first_recv(l, grp):
        return 2 * (planes - 1) * sum(pieces(*divmod(i, 2)) for i in range(l * 2 + grp))

    def holds(d, t):
        return z >= t if d == 0 else z + t < planes

    def sends(d):
        return z < planes - 1 if d == 0 else z > 0

    def pump(l, grp, t):
        kinds = (0, 1) if grp == 0 else (2,)
        if t == 0 and pieces(l, grp) == 2:
            for k in range(4):
                for kind in kinds:
                    shared[l, kind, k].wait()
        for k in range(pieces(l, grp)):
            if t == 0 and pieces(l, grp) == 4:
                for kind in kinds:
                    shared[l, kind, k].wait()
            for d in range(2):
                @pl.when(holds(d, t) & sends(d))
                def _(k=k, d=d):
                    if t > 0:
                        z_copy(l, grp, d, t, t - 1, k).wait_recv()
                    z_copy(l, grp, d, t, t, k).start()

    def consume_one(l, grp, t, d):
        @pl.when(jnp.logical_not(sends(d)))
        def _():
            for k in range(pieces(l, grp)):
                z_copy(l, grp, d, t, t - 1, k).wait_recv()

    def consume(l, grp, t):
        for d in range(2):
            @pl.when(holds(d, t))
            def _(d=d):
                consume_one(l, grp, t, d)

    def drain(l, grp):
        for t in range(planes - 1):
            for d in range(2):
                @pl.when(holds(d, t) & sends(d))
                def _(t=t, d=d):
                    z_copy(l, grp, d, t, t, -1).wait_send()

    turn[...] = jnp.zeros_like(turn)
    slots = [0]

    def make(src, dst, dev):
        slot = slots[0]
        slots[0] += 1
        return pltpu.make_async_remote_copy(src, dst, msg_send.at[slot], msg_recv.at[slot],
                                            device_id=dev, device_id_type=MESH)

    def message(src, dst, dev):
        m = make(src, dst, dev)
        m.start()
        return m

    share(0, (0, 1))
    for load in loads:
        load.wait()

    def block_rows(b):
        return pl.ds(al(b * toks, toks), toks)

    def half_cols(h):
        return pl.ds(al(h * half, half), half)

    unit = toks // 2
    total_rows = PAD + group
    tile = max(v for v in range(16, 401, 16) if total_rows % v == 0)
    part_rows = group // PARTS
    lanes = 128

    def plane_at(u):
        low = jnp.where(u <= z, z - u, u)
        zm = planes - 1 - z
        high = planes - 1 - jnp.where(u <= zm, zm - u, u)
        return jnp.where(2 * z < planes, low, high)

    for l in range(layers):
        last_layer = l + 1 == layers
        slots[0] = 0
        source = stream_in if l == 0 else strm.at[l - 1]

        def norm_step(r, _):
            at = al(r * 64, 64)
            wide = source[pl.ds(at, 64), :].astype(F32)
            scale = lax.rsqrt(jnp.mean(wide * wide, axis=1, keepdims=True) + epsilon)
            nrm[l, pl.ds(al(PAD + q * toks + at, 32), 64), :] = (
                wide * scale * gain[l:l + 1, :]).astype(BF16)
            return 0

        lax.fori_loop(0, toks // 64, norm_step, 0)

        @pl.when(z == 0)
        def _():
            nrm[l, 0:PAD, :] = jnp.zeros((PAD, width), BF16)

        def spot(b, j):
            return nrm.at[l, pl.ds(al(PAD + b * toks + j * unit, 32), unit), half_cols(c)]

        border = nrm.at[l, pl.ds(group, PAD), half_cols(c)]
        first = nrm.at[l, pl.ds(0, PAD), half_cols(c)]

        def halo_copy(k, dev, src, recv):
            return pltpu.make_async_remote_copy(
                src, first, halo_send.at[l, k], halo_recv.at[l, recv],
                device_id=dev, device_id_type=MESH)

        rise = halo_copy(0, up_dev, border, 0)
        spread = [halo_copy(k, (z * 4 + quad[k], c), first, 1) for k in (1, 2, 3)]
        swap_halo = halo_copy(4, core_dev, first, 2)

        @pl.when((q == 3) & (z < planes - 1))
        def _():
            rise.start()

        def halo_spread():
            @pl.when((q == 3) & (z > 0))
            def _():
                rise.wait_recv()
                for m in spread:
                    m.start()
                swap_halo.start()

        def halo_swap():
            @pl.when((q != 3) & (z > 0))
            def _():
                spread[0].wait_recv()
                swap_halo.start()

        def halo_finish():
            @pl.when(z > 0)
            def _():
                swap_halo.wait()

            @pl.when((q == 3) & (z > 0))
            def _():
                for m in spread:
                    m.wait_send()

            @pl.when((q == 3) & (z < planes - 1))
            def _():
                rise.wait_send()

        own_near = [message(spot(q, j), spot(q, j), near_dev) for j in range(2)]
        passed, relays, own_far = [], {}, []

        def to_far(j):
            own_near[j].wait_send()
            own_far.append(message(spot(q, j), spot(q, j), far_dev))

        def pass_on(j):
            own_near[j].wait_recv()
            passed.append(message(spot(near, j), spot(near, j), far_dev))
            relays[1, j] = message(spot(near, j), spot(near, j), core_dev)

        def relay(which, j):
            (own_far if which == 2 else passed)[j].wait()
            b = far if which == 2 else diag
            relays[which, j] = message(spot(b, j), spot(b, j), core_dev)

        def gate_rows(at, size):
            both = jnp.dot(nrm[l, pl.ds(at, size), :], wvg[l], preferred_element_type=F32)
            gated = (both[:, :ch] * jax.nn.sigmoid(both[:, ch:])).astype(BF16)
            gat[pl.ds(at, size), :] = gated.astype(F32)

        def gate_part(t, plane):
            depth = pl.ds(al(plane * 4 * rows, 4 * rows), 4 * rows)

            def gate_step(r, _):
                at = pl.ds(al(r * tile, 16), tile)
                term = jnp.dot(nrm[l, at, depth], wvg[l, depth, :], preferred_element_type=F32)
                acc[at, :] = term if t == 0 else acc[at, :] + term
                return 0

            lax.fori_loop(0, total_rows // tile, gate_step, 0)

        def gate_pair(which, j):
            b = (q, near, far, diag)[which]
            gate_rows(al(PAD + b * toks + j * unit, 32), unit)

        if l == 0:
            pump(0, 0, 0)
            halo_spread()
            to_far(0)
            to_far(1)
            pump(0, 0, 1)
            pass_on(0)
            pass_on(1)
            share(0, (2,))
            relay(2, 0)
            relay(2, 1)
            for t in range(2, planes - 1):
                pump(0, 0, t)
            relay(3, 0)
            relay(3, 1)
            for ll in range(1, layers):
                share(ll, (0, 1, 2))
            pump(0, 1, 0)
            halo_swap()
            for m in relays.values():
                m.wait()
            halo_finish()
            gate_part(0, z)
            for t in range(1, planes):
                for d in range(2):
                    @pl.when(holds(d, t))
                    def _(t=t, d=d):
                        consume_one(0, 0, t, d)
                        gate_part(t, z - t if d == 0 else z + t)

            def gate_end(r, _):
                at = pl.ds(al(r * tile, 16), tile)
                gated = (acc[at, :ch] * jax.nn.sigmoid(acc[at, ch:])).astype(BF16)
                gat[at, :] = gated.astype(F32)
                return 0

            lax.fori_loop(0, total_rows // tile, gate_end, 0)
            pump(0, 1, 1)
        else:
            for t in range(2, planes - 1):
                pump(l, 0, t)
            halo_spread()
            to_far(0)
            to_far(1)
            pump(l, 1, 0)
            pass_on(0)
            pass_on(1)
            for t in range(1, planes):
                consume(l, 0, t)
            gate_pair(0, 0)
            gate_pair(0, 1)
            for j in range(2):
                relay(2, j)
                relays[1, j].wait()
                gate_pair(2, j)
            drain(l - 1, 0)
            pump(l, 1, 1)
            relay(3, 0)
            relays[2, 0].wait()
            gate_pair(1, 0)
            relay(3, 1)
            halo_swap()
            relays[2, 1].wait()
            gate_pair(1, 1)
            for j in range(2):
                relays[3, j].wait()
                gate_pair(3, j)
            for t in range(2, planes - 1):
                pump(l, 1, t)
            halo_finish()
            gate_rows(0, PAD)
            drain(l - 1, 1)

        lead = PAD - (taps_n - 1)
        step_rows = 64

        def conv_step(r, _):
            at = al(r * step_rows, step_rows)
            for lane in range(ch // lanes):
                cut = slice(lane * lanes, (lane + 1) * lanes)
                total = jnp.zeros((step_rows, lanes), F32)
                block = gat[pl.ds(at, step_rows + PAD), cut]
                for b in range(8):
                    moved = block if b == 0 else pltpu.roll(block, step_rows + PAD - b, 0)
                    for a in range(PAD // 8 + 1):
                        tap = 8 * a + b - lead
                        if 0 <= tap < taps_n:
                            total = total + taps[tap, l:l + 1, cut] * moved[8 * a:8 * a + step_rows]
                fil[pl.ds(at, step_rows), cut] = total
            return 0

        per = part_rows // step_rows
        sums = []
        for part in range(PARTS):
            lax.fori_loop(part * per, (part + 1) * per, conv_step, 0)
            wide = fil[part * part_rows:(part + 1) * part_rows, :]
            first_sum = jnp.sum(wide, axis=1, keepdims=True)
            second_sum = jnp.sum(wide * wide, axis=1, keepdims=True)
            lane_id = lax.broadcasted_iota(jnp.int32, (part_rows, lanes), 1)
            stat = jnp.where(lane_id == 0, first_sum, jnp.where(lane_id == 1, second_sum, 0.0))
            ssend[l, part] = jnp.transpose(stat)[0:2, :]
            sums.append([message(ssend.at[l, part], srecv.at[l, part, k], dev)
                         for k, dev in enumerate(plane_devs)])
        if l == 0:
            for t in range(2, planes - 1):
                pump(l, 1, t)
        if not last_layer:
            pump(l + 1, 0, 0)
        for part in range(PARTS):
            span = slice(part * part_rows, (part + 1) * part_rows)
            for m in sums[part]:
                m.wait()
            whole = ssend[l, part]
            for k in range(len(plane_devs)):
                whole = whole + srecv[l, part, k]
            turn[0:2, :] = whole
            stat = jnp.transpose(turn[...])
            mean_value = stat[:, 0:1] / width
            variance = stat[:, 1:2] / width - mean_value * mean_value
            act[span, :] = jax.nn.silu((fil[span, :] - mean_value) * lax.rsqrt(variance + epsilon)
                                       * cgain[l:l + 1, :]).astype(BF16)

        def out_cols(h, u):
            return pl.ds(al(plane_at(u) * 4 * rows + h * chunk, chunk), chunk)

        def stage_swap(u):
            if u > 0:
                consume(l, 1, u)
            weights = wo[l, :, out_cols(1 - c, u)]
            for m, pair in enumerate(((near, diag), (far, q))):
                for k, b in enumerate(pair):
                    dsend[l, u, m, k] = jnp.dot(act[block_rows(b), :], weights,
                                                preferred_element_type=F32).astype(BF16)
                swaps[u, m] = message(dsend.at[l, u, m], drecv.at[l, u, m], core_dev)

        def stage_first(u):
            weights = wo[l, :, out_cols(c, u)]

            def partial(b, m, k):
                return (jnp.dot(act[block_rows(b), :], weights, preferred_element_type=F32)
                        + drecv[l, u, m, k].astype(F32))

            swaps[u, 0].wait()
            for k, b in enumerate((far, diag)):
                term = partial(b, 0, k).astype(BF16)
                for j in range(2):
                    asend[l, u, j, k] = term[j * unit:(j + 1) * unit]
            for j in range(2):
                firsts[u, j] = message(asend.at[l, u, j], arecv.at[l, u, j], far_dev)
            swaps[u, 1].wait()
            through[u] = partial(near, 1, 0)
            mine[u] = partial(q, 1, 1) + source[:, out_cols(c, u)].astype(F32)

        def stage_second(u, j):
            span = slice(j * unit, (j + 1) * unit)
            firsts[u, j].wait()
            bsend[l, u, j] = (through[u, span] + arecv[l, u, j, 1].astype(F32)).astype(BF16)
            seconds[u, j] = message(bsend.at[l, u, j], brecv.at[l, u, j], near_dev)
            mine[u, span] = mine[u, span] + arecv[l, u, j, 0].astype(F32)

        def stage_last(u, j):
            span = slice(j * unit, (j + 1) * unit)
            seconds[u, j].wait()
            strm[l, span, out_cols(c, u)] = (mine[u, span] + brecv[l, u, j].astype(F32)).astype(BF16)
            piece = strm.at[l, span, out_cols(c, u)]
            lasts[u, j] = message(piece, piece, core_dev)
            if last_layer:
                write(u, j, c)

        def write(u, j, h):
            span = slice(j * unit, (j + 1) * unit)
            pltpu.make_async_copy(strm.at[l, span, out_cols(h, u)], out.at[span, out_cols(h, u)],
                                  out_sem.at[0]).start()

        def finish(u, j):
            lasts[u, j].wait()
            if last_layer:
                write(u, j, 1 - c)

        swaps, firsts, seconds, lasts = {}, {}, {}, {}
        lag = 4
        for i in range(planes + lag + 1):
            if i < planes:
                stage_swap(i)
            if 1 <= i <= planes:
                stage_first(i - 1)
            for j in range(2):
                if 0 <= i - lag < planes:
                    stage_second(i - lag, j)
                if 0 <= i - lag - 1 < planes:
                    stage_last(i - lag - 1, j)
            if not last_layer and i == lag + 2:
                pump(l + 1, 0, 1)
            if last_layer and i == planes:
                drain(l, 0)
                drain(l, 1)
        for u in range(planes):
            for j in range(2):
                finish(u, j)

    pltpu.make_async_copy(strm.at[layers - 1], out, out_sem.at[0]).wait()


def fused(n, layers):
    def body(stream_in, norm_gain, value_weight, gate_weight, conv_taps, channel_gain, out_weight):
        toks, width = stream_in.shape
        taps_n = conv_taps.shape[1]
        rows, cols = value_weight.shape[1], value_weight.shape[2]
        ch, half, group, planes = cols // 4, width // 2, 4 * toks, n // 4
        chunk = 2 * rows
        taps = jnp.transpose(conv_taps, (1, 0, 2))
        hbm = pl.BlockSpec(memory_space=pltpu.HBM)
        msgs = 12 + 7 * PARTS + 8 * planes
        return pl.pallas_call(
            functools.partial(kernel, n, layers, taps_n),
            out_shape=jax.ShapeDtypeStruct((toks, width), BF16),
            in_specs=[hbm] * 7,
            out_specs=hbm,
            scratch_shapes=[
                pltpu.VMEM((toks, width), BF16),
                pltpu.VMEM((layers, width), F32),
                pltpu.VMEM((taps_n, layers, ch), F32),
                pltpu.VMEM((layers, ch), F32),
                pltpu.VMEM((layers, width, 2 * ch), BF16),
                pltpu.VMEM((layers, ch, width), BF16),
                pltpu.VMEM((layers, PAD + group, width), BF16),
                pltpu.VMEM((PAD + group, ch), F32),
                pltpu.VMEM((group, ch), F32),
                pltpu.VMEM((group, ch), BF16),
                pltpu.VMEM((layers, PARTS, 2, group // PARTS), F32),
                pltpu.VMEM((layers, PARTS, 7, 2, group // PARTS), F32),
                pltpu.VMEM((layers, planes, 2, 2, toks, chunk), BF16),
                pltpu.VMEM((layers, planes, 2, 2, toks, chunk), BF16),
                pltpu.VMEM((layers, planes, 2, 2, toks // 2, chunk), BF16),
                pltpu.VMEM((layers, planes, 2, 2, toks // 2, chunk), BF16),
                pltpu.VMEM((layers, planes, 2, toks // 2, chunk), BF16),
                pltpu.VMEM((layers, planes, 2, toks // 2, chunk), BF16),
                pltpu.VMEM((planes, toks, chunk), F32),
                pltpu.VMEM((planes, toks, chunk), F32),
                pltpu.VMEM((layers, toks, width), BF16),
                pltpu.VMEM((PAD + group, 2 * ch), F32),
                pltpu.VMEM((128, group // PARTS), F32),
                pltpu.SemaphoreType.DMA((4,)),
                pltpu.SemaphoreType.DMA((1,)),
                pltpu.SemaphoreType.DMA((layers * 3,)),
                pltpu.SemaphoreType.DMA((layers * 3, 3)),
                pltpu.SemaphoreType.DMA((layers * 3, 3)),
                pltpu.SemaphoreType.DMA((layers * 4, planes - 1)),
                pltpu.SemaphoreType.DMA((2 * (planes - 1) * (4 * layers + 2),)),
                pltpu.SemaphoreType.DMA((layers, 5)),
                pltpu.SemaphoreType.DMA((layers, 3)),
                pltpu.SemaphoreType.DMA((msgs,)),
                pltpu.SemaphoreType.DMA((msgs,)),
            ],
            compiler_params=pltpu.CompilerParams(
                collective_id=0, has_side_effects=True, vmem_limit_bytes=62 * 2**20),
        )(stream_in, norm_gain, value_weight, gate_weight, taps, channel_gain, out_weight)

    return body


def passed_along(value, axis, steps):
    count = lax.axis_size(axis)
    leading, last = (max(0, -steps), min(count, count - steps))
    return lax.ppermute(value, axis, [(source, source + steps) for source in range(leading, last)])


def general(stream_in, norm_gain, value_weight, gate_weight, conv_taps, channel_gain, out_weight):
    stream = stream_in
    tok_rows = stream_in.shape[0]
    width = stream_in.shape[1]
    taps_n = conv_taps.shape[1]
    local_cols = value_weight.shape[2]
    for layer in range(norm_gain.shape[0]):
        wide = stream.astype(F32)
        normed = (
            wide
            * lax.rsqrt(jnp.mean(wide * wide, axis=1, keepdims=True) + epsilon)
            * norm_gain[layer]
        ).astype(BF16)
        value = jnp.dot(normed, lax.all_gather(value_weight[layer], "sp", axis=0, tiled=True),
                        preferred_element_type=F32)
        gate = jnp.dot(normed, lax.all_gather(gate_weight[layer], "sp", axis=0, tiled=True),
                       preferred_element_type=F32)
        gated = (value * jax.nn.sigmoid(gate)).astype(BF16)
        earlier = passed_along(gated[tok_rows - (taps_n - 1):], "sp", 1)
        padded = jnp.concatenate([earlier, gated], axis=0).astype(F32)
        taps = conv_taps[layer]
        filtered = jnp.zeros((tok_rows, local_cols), F32)
        for tap in range(taps_n):
            filtered = filtered + taps[tap] * padded[tap:tap + tok_rows]
        sum_first, sum_second = lax.psum(
            (jnp.sum(filtered, axis=1), jnp.sum(filtered * filtered, axis=1)), "tp")
        mean_value = (sum_first / width)[:, None]
        variance = (sum_second / width)[:, None] - mean_value * mean_value
        activated = jax.nn.silu(
            (filtered - mean_value) * lax.rsqrt(variance + epsilon) * channel_gain[layer]
        ).astype(BF16)
        whole_out = lax.all_gather(out_weight[layer], "sp", axis=1, tiled=True)
        terms = jnp.dot(activated, whole_out, preferred_element_type=F32)
        summed = lax.psum(terms.astype(BF16), "tp").astype(F32)
        stream = (wide + summed).astype(BF16)
    return stream


def solution(mesh):
    n, tp = mesh.shape["sp"], mesh.shape["tp"]

    def body(stream_in, norm_gain, value_weight, *rest):
        rows, cols = value_weight.shape[1], value_weight.shape[2]
        quads = tp == 2 and n % 4 == 0 and n >= 8 and rows % 128 == 0 and cols % 512 == 0
        fits = stream_in.shape[0] % 64 == 0 and rest[1].shape[1] <= PAD
        chosen = fused(n, norm_gain.shape[0]) if quads and fits else general
        return chosen(stream_in, norm_gain, value_weight, *rest)

    return jax.shard_map(
        body,
        mesh=mesh,
        in_specs=(
            P("sp", None),
            P(),
            P(None, "sp", "tp"),
            P(None, "sp", "tp"),
            P(None, None, "tp"),
            P(None, "tp"),
            P(None, "tp", "sp"),
        ),
        out_specs=P("sp", None),
        check_vma=False,
    )
```

```python
import functools

import jax
import jax.numpy as jnp
from jax import lax
from jax.experimental import pallas as pl
from jax.experimental.pallas import tpu as pltpu
from jax.sharding import PartitionSpec as P

epsilon = 1e-05
MESH = pl.DeviceIdType.MESH
F32 = jnp.float32
BF16 = jnp.bfloat16
PAD = 32
PARTS = 2


def kernel(n, layers, taps_n, stream_hbm, gain_hbm, vw, gw, taps_hbm, cgain_hbm, ow, out,
           stream_in, gain, taps, cgain, wvg, wo, nrm, gat, fil, act, ssend, srecv, dsend, drecv,
           asend, arecv, bsend, brecv, mine, through, strm, acc, turn,
           squares, qsend, qrecv, edge_out, edge_in,
           in_sem, out_sem, loc_sem, wx_send, wx_recv, z_send, z_recv, halo_send, halo_recv,
           msg_send, msg_recv):
    planes = n // 4
    s = lax.axis_index("sp")
    c = lax.axis_index("tp")
    z, q = s // 4, s % 4
    y, x = q // 2, q % 2
    quad = [q, q + 1 - 2 * x, q + 2 - 4 * y, 3 - q]
    toks, width = stream_in.shape
    group = 4 * toks
    rows, cols = vw.shape[1], vw.shape[2]
    ch = cols // 4
    half = width // 2
    chunk = 2 * rows
    near = (1 - c) * quad[1] + c * quad[2]
    far = c * quad[1] + (1 - c) * quad[2]
    diag = quad[3]
    near_dev, far_dev, core_dev = (z * 4 + near, c), (z * 4 + far, c), (s, 1 - c)
    up_dev, down_dev = (s + 4, c), (s - 4, c)

    def al(v, m):
        return pl.multiple_of(v, m)

    barrier = pltpu.get_barrier_semaphore()
    plane_devs = [(z * 4 + quad[k], cc) for k in range(4) for cc in (c, 1 - c)][1:]
    for dev in plane_devs:
        pl.semaphore_signal(barrier, inc=1, device_id=dev, device_id_type=MESH)

    @pl.when(z < planes - 1)
    def _():
        pl.semaphore_signal(barrier, inc=1, device_id=up_dev, device_id_type=MESH)

    @pl.when(z > 0)
    def _():
        pl.semaphore_signal(barrier, inc=1, device_id=down_dev, device_id_type=MESH)

    own_ch = pl.ds(al(q * ch, ch), ch)
    loads = [pltpu.make_async_copy(a, b, in_sem.at[k]) for k, (a, b) in enumerate((
        (stream_hbm, stream_in), (gain_hbm, gain), (taps_hbm.at[:, :, own_ch], taps),
        (cgain_hbm.at[:, own_ch], cgain)))]
    for load in loads:
        load.start()

    shared = {}

    def shared_copy(l, kind, k):
        mine_rows = pl.ds(al(s * rows, rows), rows)
        span = pl.ds(al(quad[k] * ch, ch), ch)
        if kind == 2:
            src, dst = ow.at[l, span, :], wo.at[l, :, mine_rows]
        else:
            src = (vw, gw)[kind].at[l, :, span]
            dst = wvg.at[l, mine_rows, pl.ds(kind * ch, ch)]
        idx = l * 3 + kind
        if k == 0:
            copy = pltpu.make_async_copy(src, dst, loc_sem.at[idx])
        else:
            copy = pltpu.make_async_remote_copy(
                src, dst, wx_send.at[idx, k - 1], wx_recv.at[idx, k - 1],
                device_id=(z * 4 + quad[k], c), device_id_type=MESH)
        copy.start()
        shared[l, kind, k] = copy

    def share(l, kinds, ks=(1, 2, 3)):
        for k in ks:
            for kind in kinds:
                shared_copy(l, kind, k)

    for l in range(layers):
        share(l, (0, 1, 2), (0,))

    pl.semaphore_wait(barrier, len(plane_devs) + (z < planes - 1).astype(jnp.int32)
                      + (z > 0).astype(jnp.int32))

    def z_copy(l, grp, d, t, hop, k):
        plane = z - t if d == 0 else z + t
        if k < 0:
            block = pl.ds(al(plane * 4 * rows, rows), 4 * rows)
        elif pieces(l, grp) == 4:
            block = pl.ds(al((plane * 4 + quad[k]) * rows, rows), rows)
        else:
            block = pl.ds(al((plane * 4 + 2 * k) * rows, rows), 2 * rows)
        ref = wvg.at[l, block, :] if grp == 0 else wo.at[l, :, block]
        idx = (l * 2 + grp) * 2 + d
        return pltpu.make_async_remote_copy(
            ref, ref, z_send.at[idx, hop], z_recv.at[first_recv(l, grp) + (d * (planes - 1) + hop) * pieces(l, grp) + max(k, 0)],
            device_id=up_dev if d == 0 else down_dev, device_id_type=MESH)

    def pieces(l, grp):
        return 4 if l == 0 else 2

    def first_recv(l, grp):
        return 2 * (planes - 1) * sum(pieces(*divmod(i, 2)) for i in range(l * 2 + grp))

    def holds(d, t):
        return z >= t if d == 0 else z + t < planes

    def sends(d):
        return z < planes - 1 if d == 0 else z > 0

    def pump(l, grp, t, ks=None):
        kinds = (0, 1) if grp == 0 else (2,)
        if t == 0 and pieces(l, grp) == 2:
            for k in range(4):
                for kind in kinds:
                    shared[l, kind, k].wait()
        for k in ks or range(pieces(l, grp)):
            if t == 0 and pieces(l, grp) == 4:
                for kind in kinds:
                    shared[l, kind, k].wait()
            for d in range(2):
                @pl.when(holds(d, t) & sends(d))
                def _(k=k, d=d):
                    if t > 0:
                        z_copy(l, grp, d, t, t - 1, k).wait_recv()
                    z_copy(l, grp, d, t, t, k).start()

    def consume_one(l, grp, t, d):
        @pl.when(jnp.logical_not(sends(d)))
        def _():
            for k in range(pieces(l, grp)):
                z_copy(l, grp, d, t, t - 1, k).wait_recv()

    def consume(l, grp, t):
        for d in range(2):
            @pl.when(holds(d, t))
            def _(d=d):
                consume_one(l, grp, t, d)

    def drain(l, grp):
        for t in range(planes - 1):
            for d in range(2):
                @pl.when(holds(d, t) & sends(d))
                def _(t=t, d=d):
                    z_copy(l, grp, d, t, t, -1).wait_send()

    turn[...] = jnp.zeros_like(turn)
    slots = {}

    def message(name, src, dst, dev):
        slot = slots.setdefault(name, len(slots))
        m = pltpu.make_async_remote_copy(src, dst, msg_send.at[slot], msg_recv.at[slot],
                                         device_id=dev, device_id_type=MESH)
        m.start()
        return m

    share(0, (0, 1))
    for load in loads:
        load.wait()

    def block_rows(b):
        return pl.ds(al(b * toks, toks), toks)

    def half_cols(h):
        return pl.ds(al(h * half, half), half)

    unit = toks // 2
    total_rows = PAD + group
    tile = max(v for v in range(16, 401, 16) if total_rows % v == 0)
    part_rows = group // PARTS
    lanes = 128

    def plane_at(u):
        low = jnp.where(u <= z, z - u, u)
        zm = planes - 1 - z
        high = planes - 1 - jnp.where(u <= zm, zm - u, u)
        return jnp.where(2 * z < planes, low, high)

    def norm_step(r, _):
        at = al(r * 64, 64)
        wide = stream_in[pl.ds(at, 64), :].astype(F32)
        scale = lax.rsqrt(jnp.mean(wide * wide, axis=1, keepdims=True) + epsilon)
        nrm[0, pl.ds(al(PAD + q * toks + at, 32), 64), :] = (
            wide * scale * gain[0:1, :]).astype(BF16)
        return 0

    class Halo:
        def __init__(self, l, border, first):
            def copy(k, dev, src, recv):
                return pltpu.make_async_remote_copy(
                    src, first, halo_send.at[l, k], halo_recv.at[l, recv],
                    device_id=dev, device_id_type=MESH)

            self.up = copy(0, up_dev, border, 0)
            self.side = [copy(k, (z * 4 + quad[k], c), first, 1) for k in (1, 2, 3)]
            self.core = copy(4, core_dev, first, 2)

        def rise(self):
            @pl.when((q == 3) & (z < planes - 1))
            def _():
                self.up.start()

        def spread(self):
            @pl.when((q == 3) & (z > 0))
            def _():
                self.up.wait_recv()
                for m in self.side:
                    m.start()
                self.core.start()

        def swap(self):
            @pl.when((q != 3) & (z > 0))
            def _():
                self.side[0].wait_recv()
                self.core.start()

        def finish(self):
            @pl.when(z > 0)
            def _():
                self.core.wait()

            @pl.when((q == 3) & (z > 0))
            def _():
                for m in self.side:
                    m.wait_send()

            @pl.when((q == 3) & (z < planes - 1))
            def _():
                self.up.wait_send()

    def spot(b, j):
        return nrm.at[0, pl.ds(al(PAD + b * toks + j * unit, 32), unit), half_cols(c)]

    def to_far(j):
        own_near[j].wait_send()
        own_far.append(message(("far", j), spot(q, j), spot(q, j), far_dev))

    def pass_on(j):
        own_near[j].wait_recv()
        passed.append(message(("pass", j), spot(near, j), spot(near, j), far_dev))
        relays[1, j] = message(("core", 1, j), spot(near, j), spot(near, j), core_dev)

    def relay(which, j):
        (own_far if which == 2 else passed)[j].wait()
        b = far if which == 2 else diag
        relays[which, j] = message(("core", which, j), spot(b, j), spot(b, j), core_dev)

    def gate_part(l, t, plane, start, count, size):
        depth = pl.ds(al(plane * 4 * rows, 4 * rows), 4 * rows)

        def gate_step(r, _):
            at = pl.ds(al(start + r * size, 16), size)
            term = jnp.dot(nrm[l, at, depth], wvg[l, depth, :], preferred_element_type=F32)
            acc[at, :] = term if t == 0 else acc[at, :] + term
            return 0

        lax.fori_loop(0, count // size, gate_step, 0)

    for l in range(layers):
        last_layer = l + 1 == layers
        source = stream_in if l == 0 else strm.at[l - 1]

        if l == 0:
            lax.fori_loop(0, toks // 64, norm_step, 0)

            @pl.when(z == 0)
            def _():
                for ll in range(layers):
                    nrm[ll, 0:PAD, :] = jnp.zeros((PAD, width), BF16)

            edge = Halo(0, nrm.at[0, pl.ds(group, PAD), half_cols(c)],
                        nrm.at[0, pl.ds(0, PAD), half_cols(c)])
            edge.rise()
            own_near = [message(("near", j), spot(q, j), spot(q, j), near_dev) for j in range(2)]
            passed, relays, own_far = [], {}, []
            pump(0, 0, 0, (0,))
            pump(0, 1, 0, (0,))
            pump(0, 0, 0, (1, 2, 3))
            edge.spread()
            to_far(0)
            to_far(1)
            pump(0, 0, 1)
            pass_on(0)
            pass_on(1)
            share(0, (2,))
            relay(2, 0)
            relay(2, 1)
            for t in range(2, planes - 1):
                pump(0, 0, t)
            relay(3, 0)
            relay(3, 1)
            for ll in range(1, layers):
                share(ll, (0, 1, 2))
            pump(0, 1, 0, (1, 2, 3))
            edge.swap()
            for m in relays.values():
                m.wait()
            edge.finish()
            gate_part(0, 0, z, 0, total_rows, tile)
            for t in range(1, planes):
                for d in range(2):
                    @pl.when(holds(d, t))
                    def _(t=t, d=d):
                        consume_one(0, 0, t, d)
                        gate_part(0, t, z - t if d == 0 else z + t, 0, total_rows, tile)

            def gate_end(r, _):
                at = pl.ds(al(r * tile, 16), tile)
                gated = (acc[at, :ch] * jax.nn.sigmoid(acc[at, ch:])).astype(BF16)
                gat[at, :] = gated.astype(F32)
                return 0

            lax.fori_loop(0, total_rows // tile, gate_end, 0)
            pump(0, 1, 1)

        lead = PAD - (taps_n - 1)
        step_rows = 64

        def conv_step(r, _):
            at = al(r * step_rows, step_rows)
            for lane in range(ch // lanes):
                cut = slice(lane * lanes, (lane + 1) * lanes)
                total = jnp.zeros((step_rows, lanes), F32)
                block = gat[pl.ds(at, step_rows + PAD), cut]
                for b in range(8):
                    moved = block if b == 0 else pltpu.roll(block, step_rows + PAD - b, 0)
                    for a in range(PAD // 8 + 1):
                        tap = 8 * a + b - lead
                        if 0 <= tap < taps_n:
                            total = total + taps[tap, l:l + 1, cut] * moved[8 * a:8 * a + step_rows]
                fil[pl.ds(at, step_rows), cut] = total
            return 0

        per = part_rows // step_rows
        sums = []
        for part in range(PARTS):
            lax.fori_loop(part * per, (part + 1) * per, conv_step, 0)
            wide = fil[part * part_rows:(part + 1) * part_rows, :]
            first_sum = jnp.sum(wide, axis=1, keepdims=True)
            second_sum = jnp.sum(wide * wide, axis=1, keepdims=True)
            lane_id = lax.broadcasted_iota(jnp.int32, (part_rows, lanes), 1)
            stat = jnp.where(lane_id == 0, first_sum, jnp.where(lane_id == 1, second_sum, 0.0))
            ssend[l, part] = jnp.transpose(stat)[0:2, :]
            sums.append([message(("sum", part, k), ssend.at[l, part], srecv.at[l, part, k], dev)
                         for k, dev in enumerate(plane_devs)])
        for t in range(2, planes - 1):
            pump(l, 1, t)
        if not last_layer:
            pump(l + 1, 0, 0)
        for part in range(PARTS):
            span = slice(part * part_rows, (part + 1) * part_rows)
            for m in sums[part]:
                m.wait()
            whole = ssend[l, part]
            for k in range(len(plane_devs)):
                whole = whole + srecv[l, part, k]
            turn[0:2, 0:part_rows] = whole
            stat = jnp.transpose(turn[:, 0:part_rows])
            mean_value = stat[:, 0:1] / width
            variance = stat[:, 1:2] / width - mean_value * mean_value
            act[span, :] = jax.nn.silu((fil[span, :] - mean_value) * lax.rsqrt(variance + epsilon)
                                       * cgain[l:l + 1, :]).astype(BF16)

        def out_cols(h, u):
            return pl.ds(al(plane_at(u) * 4 * rows + h * chunk, chunk), chunk)

        def stage_swap(u):
            if u > 0:
                consume(l, 1, u)
            weights = wo[l, :, out_cols(1 - c, u)]
            for m, pair in enumerate(((near, diag), (far, q))):
                for k, b in enumerate(pair):
                    dsend[l, u, m, k] = jnp.dot(act[block_rows(b), :], weights,
                                                preferred_element_type=F32).astype(BF16)
                swaps[u, m] = message(("swap", u, m), dsend.at[l, u, m], drecv.at[l, u, m], core_dev)

        def stage_first(u):
            weights = wo[l, :, out_cols(c, u)]

            def partial(b, m, k):
                return (jnp.dot(act[block_rows(b), :], weights, preferred_element_type=F32)
                        + drecv[l, u, m, k].astype(F32))

            swaps[u, 0].wait()
            for k, b in enumerate((far, diag)):
                term = partial(b, 0, k).astype(BF16)
                for j in range(2):
                    asend[l, u, j, k] = term[j * unit:(j + 1) * unit]
            for j in range(2):
                firsts[u, j] = message(("first", u, j), asend.at[l, u, j], arecv.at[l, u, j], far_dev)
            swaps[u, 1].wait()
            through[u] = partial(near, 1, 0)
            mine[u] = partial(q, 1, 1) + source[:, out_cols(c, u)].astype(F32)

        def stage_second(u, j):
            span = slice(j * unit, (j + 1) * unit)
            firsts[u, j].wait()
            bsend[l, u, j] = (through[u, span] + arecv[l, u, j, 1].astype(F32)).astype(BF16)
            seconds[u, j] = message(("second", u, j), bsend.at[l, u, j], brecv.at[l, u, j], near_dev)
            mine[u, span] = mine[u, span] + arecv[l, u, j, 0].astype(F32)

        def stage_last(u, j):
            span = slice(j * unit, (j + 1) * unit)
            seconds[u, j].wait()
            final = (mine[u, span] + brecv[l, u, j].astype(F32)).astype(BF16)
            strm[l, span, out_cols(c, u)] = final
            if last_layer:
                piece = strm.at[l, span, out_cols(c, u)]
                lasts[u, j] = message(("last", u, j), piece, piece, core_dev)
                write(u, j, c)
            else:
                wide = final.astype(F32)
                nrm[l + 1, pl.ds(al(PAD + q * toks + j * unit, 32), unit), out_cols(c, u)] = (
                    wide * gain[l + 1:l + 2, out_cols(c, u)]).astype(BF16)
                square = wide * wide
                folded = sum(square[:, k * lanes:(k + 1) * lanes] for k in range(chunk // lanes))
                squares[span, :] = folded if u == 0 else squares[span, :] + folded

        def write(u, j, h):
            span = slice(j * unit, (j + 1) * unit)
            pltpu.make_async_copy(strm.at[l, span, out_cols(h, u)], out.at[span, out_cols(h, u)],
                                  out_sem.at[0]).start()

        def finish(u, j):
            lasts[u, j].wait()
            write(u, j, 1 - c)

        def lot(b, u):
            return nrm.at[l + 1, pl.ds(al(PAD + b * toks, 32), toks), out_cols(c, u)]

        def pass_chunk(kind, u, b, dev):
            moves[kind, u] = message((kind, u), lot(b, u), lot(b, u), dev)

        def gather(u):
            pass_chunk("g_near", u, q, near_dev)
            pass_chunk("g_far", u, q, far_dev)
            pass_chunk("c_own", u, q, core_dev)

        def forward(u):
            moves["g_near", u].wait()
            pass_chunk("g_pass", u, near, far_dev)
            pass_chunk("c_near", u, near, core_dev)

        def cross_far(u):
            moves["g_far", u].wait()
            pass_chunk("c_far", u, far, core_dev)

        def cross_diag(u):
            moves["g_pass", u].wait()
            pass_chunk("c_diag", u, diag, core_dev)

        def gate_chunk(u):
            if u > 0:
                consume(l + 1, 0, u)
            for kind in ("c_own", "c_near", "c_far", "c_diag"):
                moves[kind, u].wait()
            gate_part(l + 1, u, plane_at(u), PAD, group, toks)

        def send_squares():
            lane_id = lax.broadcasted_iota(jnp.int32, (toks, lanes), 1)
            total = jnp.sum(squares[...], axis=1, keepdims=True)
            qsend[l] = jnp.transpose(jnp.where(lane_id == 0, total, 0.0))[0:2, :]
            return [message(("square", k), qsend.at[l], qrecv.at[l, k], dev)
                    for k, dev in enumerate(plane_devs)]

        def row_scale(whole):
            turn[0:2, 0:toks] = whole
            return lax.rsqrt(jnp.transpose(turn[:, 0:toks])[:, 0:1] / width + epsilon)

        def send_edge(edge):
            norms[0].wait()
            scale = row_scale(qsend[l] + qrecv[l, 0])[toks - PAD:]
            for u in range(planes):
                edge_out[l, :, pl.ds(al(plane_at(u) * chunk, chunk), chunk)] = (
                    strm[l, toks - PAD:, out_cols(c, u)].astype(F32) * scale
                    * gain[l + 1:l + 2, out_cols(c, u)]).astype(BF16)
            edge.rise()

        def gate_final(edge):
            edge.finish()

            @pl.when(z > 0)
            def _():
                for p in range(planes):
                    for h in range(2):
                        at = p * 4 * rows + h * chunk
                        nrm[l + 1, 0:PAD, at:at + chunk] = edge_in[l, h, :, p * chunk:(p + 1) * chunk]

            both = jnp.dot(nrm[l + 1, 0:PAD, :], wvg[l + 1], preferred_element_type=F32)
            gat[0:PAD, :] = (both[:, :ch] * jax.nn.sigmoid(both[:, ch:])).astype(BF16).astype(F32)
            for m in norms[1:]:
                m.wait()
            for k in range(4):
                mate = qsend[l] if k == 0 else qrecv[l, 2 * k - 1]
                scale = row_scale(mate + qrecv[l, 2 * k])
                at = pl.ds(al(PAD + quad[k] * toks, 32), toks)
                value, gate = acc[at, :ch] * scale, acc[at, ch:] * scale
                gat[at, :] = (value * jax.nn.sigmoid(gate)).astype(BF16).astype(F32)

        swaps, firsts, seconds, lasts, moves = {}, {}, {}, {}, {}
        lag = 4
        for i in range(planes + lag + 1):
            if i < planes:
                stage_swap(i)
            if 1 <= i <= planes:
                stage_first(i - 1)
            for j in range(2):
                if 0 <= i - lag < planes:
                    stage_second(i - lag, j)
                if 0 <= i - lag - 1 < planes:
                    stage_last(i - lag - 1, j)
            if not last_layer:
                if i - lag - 1 >= 0:
                    gather(i - lag - 1)
                if i - lag - 3 >= 0:
                    forward(i - lag - 3)
                if i == lag + 2:
                    pump(l + 1, 0, 1)
            if last_layer and i == planes:
                drain(l, 0)
                drain(l, 1)
        if last_layer:
            for u in range(planes):
                for j in range(2):
                    finish(u, j)
        else:
            edge = Halo(l + 1, edge_out.at[l], edge_in.at[l, c])
            norms = send_squares()
            cross_far(0)
            send_edge(edge)
            ahead = planes - 2
            for u in range(ahead, planes + ahead):
                if u < planes:
                    forward(u)
                    cross_far(u - ahead + 1)
                elif u - ahead + 1 < planes:
                    cross_far(u - ahead + 1)
                cross_diag(u - ahead)
                if u == ahead:
                    for t in range(2, planes - 1):
                        pump(l + 1, 0, t)
                if u == ahead + 1:
                    edge.spread()
                    pump(l + 1, 1, 0)
                gate_chunk(u - ahead)
                if u == ahead + 2:
                    drain(l, 0)
                    drain(l, 1)
            edge.swap()
            gate_final(edge)
            pump(l + 1, 1, 1)

    pltpu.make_async_copy(strm.at[layers - 1], out, out_sem.at[0]).wait()


def fused(n, layers):
    def body(stream_in, norm_gain, value_weight, gate_weight, conv_taps, channel_gain, out_weight):
        toks, width = stream_in.shape
        taps_n = conv_taps.shape[1]
        rows, cols = value_weight.shape[1], value_weight.shape[2]
        ch, half, group, planes = cols // 4, width // 2, 4 * toks, n // 4
        chunk = 2 * rows
        taps = jnp.transpose(conv_taps, (1, 0, 2))
        hbm = pl.BlockSpec(memory_space=pltpu.HBM)
        msgs = 12 + 7 + 7 * PARTS + 15 * planes
        return pl.pallas_call(
            functools.partial(kernel, n, layers, taps_n),
            out_shape=jax.ShapeDtypeStruct((toks, width), BF16),
            in_specs=[hbm] * 7,
            out_specs=hbm,
            scratch_shapes=[
                pltpu.VMEM((toks, width), BF16),
                pltpu.VMEM((layers, width), F32),
                pltpu.VMEM((taps_n, layers, ch), F32),
                pltpu.VMEM((layers, ch), F32),
                pltpu.VMEM((layers, width, 2 * ch), BF16),
                pltpu.VMEM((layers, ch, width), BF16),
                pltpu.VMEM((layers, PAD + group, width), BF16),
                pltpu.VMEM((PAD + group, ch), F32),
                pltpu.VMEM((group, ch), F32),
                pltpu.VMEM((group, ch), BF16),
                pltpu.VMEM((layers, PARTS, 2, group // PARTS), F32),
                pltpu.VMEM((layers, PARTS, 7, 2, group // PARTS), F32),
                pltpu.VMEM((layers, planes, 2, 2, toks, chunk), BF16),
                pltpu.VMEM((layers, planes, 2, 2, toks, chunk), BF16),
                pltpu.VMEM((layers, planes, 2, 2, toks // 2, chunk), BF16),
                pltpu.VMEM((layers, planes, 2, 2, toks // 2, chunk), BF16),
                pltpu.VMEM((layers, planes, 2, toks // 2, chunk), BF16),
                pltpu.VMEM((layers, planes, 2, toks // 2, chunk), BF16),
                pltpu.VMEM((planes, toks, chunk), F32),
                pltpu.VMEM((planes, toks, chunk), F32),
                pltpu.VMEM((layers, toks, width), BF16),
                pltpu.VMEM((PAD + group, 2 * ch), F32),
                pltpu.VMEM((128, group), F32),
                pltpu.VMEM((toks, 128), F32),
                pltpu.VMEM((layers, 2, toks), F32),
                pltpu.VMEM((layers, 7, 2, toks), F32),
                pltpu.VMEM((layers, PAD, half), BF16),
                pltpu.VMEM((layers, 2, PAD, half), BF16),
                pltpu.SemaphoreType.DMA((4,)),
                pltpu.SemaphoreType.DMA((1,)),
                pltpu.SemaphoreType.DMA((layers * 3,)),
                pltpu.SemaphoreType.DMA((layers * 3, 3)),
                pltpu.SemaphoreType.DMA((layers * 3, 3)),
                pltpu.SemaphoreType.DMA((layers * 4, planes - 1)),
                pltpu.SemaphoreType.DMA((2 * (planes - 1) * (4 * layers + 4),)),
                pltpu.SemaphoreType.DMA((layers, 5)),
                pltpu.SemaphoreType.DMA((layers, 3)),
                pltpu.SemaphoreType.DMA((msgs,)),
                pltpu.SemaphoreType.DMA((msgs,)),
            ],
            compiler_params=pltpu.CompilerParams(
                collective_id=0, has_side_effects=True, vmem_limit_bytes=62 * 2**20),
        )(stream_in, norm_gain, value_weight, gate_weight, taps, channel_gain, out_weight)

    return body


def passed_along(value, axis, steps):
    count = lax.axis_size(axis)
    leading, last = (max(0, -steps), min(count, count - steps))
    return lax.ppermute(value, axis, [(source, source + steps) for source in range(leading, last)])


def general(stream_in, norm_gain, value_weight, gate_weight, conv_taps, channel_gain, out_weight):
    stream = stream_in
    tok_rows = stream_in.shape[0]
    width = stream_in.shape[1]
    taps_n = conv_taps.shape[1]
    local_cols = value_weight.shape[2]
    for layer in range(norm_gain.shape[0]):
        wide = stream.astype(F32)
        normed = (
            wide
            * lax.rsqrt(jnp.mean(wide * wide, axis=1, keepdims=True) + epsilon)
            * norm_gain[layer]
        ).astype(BF16)
        value = jnp.dot(normed, lax.all_gather(value_weight[layer], "sp", axis=0, tiled=True),
                        preferred_element_type=F32)
        gate = jnp.dot(normed, lax.all_gather(gate_weight[layer], "sp", axis=0, tiled=True),
                       preferred_element_type=F32)
        gated = (value * jax.nn.sigmoid(gate)).astype(BF16)
        earlier = passed_along(gated[tok_rows - (taps_n - 1):], "sp", 1)
        padded = jnp.concatenate([earlier, gated], axis=0).astype(F32)
        taps = conv_taps[layer]
        filtered = jnp.zeros((tok_rows, local_cols), F32)
        for tap in range(taps_n):
            filtered = filtered + taps[tap] * padded[tap:tap + tok_rows]
        sum_first, sum_second = lax.psum(
            (jnp.sum(filtered, axis=1), jnp.sum(filtered * filtered, axis=1)), "tp")
        mean_value = (sum_first / width)[:, None]
        variance = (sum_second / width)[:, None] - mean_value * mean_value
        activated = jax.nn.silu(
            (filtered - mean_value) * lax.rsqrt(variance + epsilon) * channel_gain[layer]
        ).astype(BF16)
        whole_out = lax.all_gather(out_weight[layer], "sp", axis=1, tiled=True)
        terms = jnp.dot(activated, whole_out, preferred_element_type=F32)
        summed = lax.psum(terms.astype(BF16), "tp").astype(F32)
        stream = (wide + summed).astype(BF16)
    return stream


def solution(mesh):
    n, tp = mesh.shape["sp"], mesh.shape["tp"]

    def body(stream_in, norm_gain, value_weight, *rest):
        rows, cols = value_weight.shape[1], value_weight.shape[2]
        quads = tp == 2 and n % 4 == 0 and n >= 8 and rows % 128 == 0 and cols % 512 == 0
        fits = stream_in.shape[0] % 64 == 0 and rest[1].shape[1] <= PAD
        chosen = fused(n, norm_gain.shape[0]) if quads and fits else general
        return chosen(stream_in, norm_gain, value_weight, *rest)

    return jax.shard_map(
        body,
        mesh=mesh,
        in_specs=(
            P("sp", None),
            P(),
            P(None, "sp", "tp"),
            P(None, "sp", "tp"),
            P(None, None, "tp"),
            P(None, "tp"),
            P(None, "tp", "sp"),
        ),
        out_specs=P("sp", None),
        check_vma=False,
    )
```

```python
import functools

import jax
import jax.numpy as jnp
from jax import lax
from jax.experimental import pallas as pl
from jax.experimental.pallas import tpu as pltpu
from jax.sharding import PartitionSpec as P

epsilon = 1e-05
MESH = pl.DeviceIdType.MESH
F32 = jnp.float32
BF16 = jnp.bfloat16
PAD = 32
PARTS = 2


def kernel(n, layers, taps_n, stream_hbm, gain_hbm, vw, gw, taps_hbm, cgain_hbm, ow, out,
           stream_in, gain, taps, cgain, wvg, wo, nrm, gat, fil, act, ssend, srecv, dsend, drecv,
           asend, arecv, bsend, brecv, mine, through, strm, acc, turn,
           squares, qsend, qrecv, edge_out, edge_in,
           in_sem, out_sem, loc_sem, wx_send, wx_recv, z_send, z_recv, halo_send, halo_recv,
           msg_send, msg_recv):
    planes = n // 4
    s = lax.axis_index("sp")
    c = lax.axis_index("tp")
    z, q = s // 4, s % 4
    y, x = q // 2, q % 2
    quad = [q, q + 1 - 2 * x, q + 2 - 4 * y, 3 - q]
    toks, width = stream_in.shape
    group = 4 * toks
    rows, cols = vw.shape[1], vw.shape[2]
    ch = cols // 4
    half = width // 2
    chunk = 2 * rows
    near = (1 - c) * quad[1] + c * quad[2]
    far = c * quad[1] + (1 - c) * quad[2]
    diag = quad[3]
    near_dev, far_dev, core_dev = (z * 4 + near, c), (z * 4 + far, c), (s, 1 - c)
    up_dev, down_dev = (s + 4, c), (s - 4, c)

    def al(v, m):
        return pl.multiple_of(v, m)

    barrier = pltpu.get_barrier_semaphore()
    plane_devs = [(z * 4 + quad[k], cc) for k in range(4) for cc in (c, 1 - c)][1:]
    for dev in plane_devs:
        pl.semaphore_signal(barrier, inc=1, device_id=dev, device_id_type=MESH)

    @pl.when(z < planes - 1)
    def _():
        pl.semaphore_signal(barrier, inc=1, device_id=up_dev, device_id_type=MESH)

    @pl.when(z > 0)
    def _():
        pl.semaphore_signal(barrier, inc=1, device_id=down_dev, device_id_type=MESH)

    own_ch = pl.ds(al(q * ch, ch), ch)
    loads = [pltpu.make_async_copy(a, b, in_sem.at[k]) for k, (a, b) in enumerate((
        (stream_hbm, stream_in), (gain_hbm, gain), (taps_hbm.at[:, :, own_ch], taps),
        (cgain_hbm.at[:, own_ch], cgain)))]
    for load in loads:
        load.start()

    shared = {}

    def shared_copy(l, kind, k):
        mine_rows = pl.ds(al(s * rows, rows), rows)
        span = pl.ds(al(quad[k] * ch, ch), ch)
        if kind == 2:
            src, dst = ow.at[l, span, :], wo.at[l, :, mine_rows]
        else:
            src = (vw, gw)[kind].at[l, :, span]
            dst = wvg.at[l, mine_rows, pl.ds(kind * ch, ch)]
        idx = l * 3 + kind
        if k == 0:
            copy = pltpu.make_async_copy(src, dst, loc_sem.at[idx])
        else:
            copy = pltpu.make_async_remote_copy(
                src, dst, wx_send.at[0], wx_recv.at[idx, k - 1],
                device_id=(z * 4 + quad[k], c), device_id_type=MESH)
        copy.start()
        shared[l, kind, k] = copy

    def share(l, kinds, ks=(1, 2, 3)):
        for k in ks:
            for kind in kinds:
                shared_copy(l, kind, k)

    for l in range(layers):
        share(l, (0, 1, 2), (0,))

    pl.semaphore_wait(barrier, len(plane_devs) + (z < planes - 1).astype(jnp.int32)
                      + (z > 0).astype(jnp.int32))

    def z_copy(l, grp, d, t, hop, first, count, pair):
        plane = z - t if d == 0 else z + t
        block = pl.ds(al((plane * 4 + first) * rows, rows), count * rows)
        ref = wvg.at[l, block, :] if grp == 0 else wo.at[l, :, block]
        idx = (l * 2 + grp) * 2 + d
        return pltpu.make_async_remote_copy(
            ref, ref, z_send.at[idx, hop], z_recv.at[idx, hop, pair],
            device_id=up_dev if d == 0 else down_dev, device_id_type=MESH)

    def z_pair(l, grp, d, t, hop, pair):
        return z_copy(l, grp, d, t, hop, 2 * (y + pair - 2 * y * pair), 2, pair)

    def holds(d, t):
        return z >= t if d == 0 else z + t < planes

    def sends(d):
        return z < planes - 1 if d == 0 else z > 0

    def pump(l, grp, t, ks=(0, 1, 2, 3)):
        if t == 0:
            for k in ks:
                for kind in ((0, 1) if grp == 0 else (2,)):
                    if k:
                        shared[l, kind, k].wait_recv()
                    else:
                        shared[l, kind, k].wait()
                if l == 0:
                    for d in range(2):
                        @pl.when(sends(d))
                        def _(k=k, d=d):
                            z_copy(l, grp, d, 0, 0, quad[k], 1, k // 2).start()
        if t > 0 or l > 0:
            for pair in range(2):
                for d in range(2):
                    @pl.when(holds(d, t) & sends(d))
                    def _(pair=pair, d=d):
                        if t > 0:
                            z_pair(l, grp, d, t, t - 1, pair).wait_recv()
                        z_pair(l, grp, d, t, t, pair).start()

    def consume_one(l, grp, t, d):
        @pl.when(jnp.logical_not(sends(d)))
        def _():
            for pair in range(2):
                z_pair(l, grp, d, t, t - 1, pair).wait_recv()

    def consume(l, grp, t):
        for d in range(2):
            @pl.when(holds(d, t))
            def _(d=d):
                consume_one(l, grp, t, d)

    def drain(l, grp):
        for t in range(planes - 1):
            for d in range(2):
                @pl.when(holds(d, t) & sends(d))
                def _(t=t, d=d):
                    z_copy(l, grp, d, t, t, 0, 4, 0).wait_send()

    turn[...] = jnp.zeros_like(turn)
    slots, kinds_sent = {}, {}

    def message(name, src, dst, dev, sender):
        slot = slots.setdefault(name, len(slots))
        kind = kinds_sent.setdefault(sender, len(kinds_sent))
        m = pltpu.make_async_remote_copy(src, dst, msg_send.at[kind], msg_recv.at[slot],
                                         device_id=dev, device_id_type=MESH)
        m.start()
        return m

    def all_sent(sender, ref):
        pltpu.make_async_remote_copy(ref, ref, msg_send.at[kinds_sent[sender]], msg_recv.at[0],
                                     device_id=core_dev, device_id_type=MESH).wait_send()

    share(0, (0, 1))

    def block_rows(b):
        return pl.ds(al(b * toks, toks), toks)

    def half_cols(h):
        return pl.ds(al(h * half, half), half)

    unit = toks // 2
    total_rows = PAD + group
    tile = max(v for v in range(16, 401, 16) if total_rows % v == 0)
    part_rows = group // PARTS
    lanes = 128

    def plane_at(u):
        low = jnp.where(u <= z, z - u, u)
        zm = planes - 1 - z
        high = planes - 1 - jnp.where(u <= zm, zm - u, u)
        return jnp.where(2 * z < planes, low, high)

    def norm_step(r, _):
        at = al(r * 64, 64)
        wide = stream_in[pl.ds(at, 64), :].astype(F32)
        scale = lax.rsqrt(jnp.mean(wide * wide, axis=1, keepdims=True) + epsilon)
        nrm[0, pl.ds(al(PAD + q * toks + at, 32), 64), :] = (
            wide * scale * gain[0:1, :]).astype(BF16)
        return 0

    class Halo:
        def __init__(self, l, border, first):
            def copy(k, dev, src, recv):
                return pltpu.make_async_remote_copy(
                    src, first, halo_send.at[l, k], halo_recv.at[l, recv],
                    device_id=dev, device_id_type=MESH)

            self.up = copy(0, up_dev, border, 0)
            self.side = [copy(k, (z * 4 + quad[k], c), first, 1) for k in (1, 2, 3)]
            self.core = copy(4, core_dev, first, 2)

        def rise(self):
            @pl.when((q == 3) & (z < planes - 1))
            def _():
                self.up.start()

        def spread(self):
            @pl.when((q == 3) & (z > 0))
            def _():
                self.up.wait_recv()
                for m in self.side:
                    m.start()
                self.core.start()

        def swap(self):
            @pl.when((q != 3) & (z > 0))
            def _():
                self.side[0].wait_recv()
                self.core.start()

        def finish(self):
            @pl.when(z > 0)
            def _():
                self.core.wait()

            @pl.when((q == 3) & (z > 0))
            def _():
                for m in self.side:
                    m.wait_send()

            @pl.when((q == 3) & (z < planes - 1))
            def _():
                self.up.wait_send()

    def spot(b, j):
        return nrm.at[0, pl.ds(al(PAD + b * toks + j * unit, 32), unit), half_cols(c)]

    def to_far(j):
        own_near[j].wait_send()
        own_far.append(message(("g_far", j), spot(q, j), spot(q, j), far_dev, "ag"))

    def pass_on(j):
        own_near[j].wait_recv()
        passed.append(message(("g_pass", j), spot(near, j), spot(near, j), far_dev, "ag"))
        relays[1, j] = message(("c_near", j), spot(near, j), spot(near, j), core_dev, "ag")

    def relay(which, j):
        (own_far if which == 2 else passed)[j].wait_recv()
        b = far if which == 2 else diag
        relays[which, j] = message(("c_far" if which == 2 else "c_diag", j), spot(b, j), spot(b, j), core_dev, "ag")

    def gate_part(l, t, plane, start, count, size):
        depth = pl.ds(al(plane * 4 * rows, 4 * rows), 4 * rows)

        def gate_step(r, _):
            at = pl.ds(al(start + r * size, 16), size)
            term = jnp.dot(nrm[l, at, depth], wvg[l, depth, :], preferred_element_type=F32)
            acc[at, :] = term if t == 0 else acc[at, :] + term
            return 0

        lax.fori_loop(0, count // size, gate_step, 0)

    for l in range(layers):
        last_layer = l + 1 == layers
        source = stream_in if l == 0 else strm.at[l - 1]

        if l == 0:
            pump(0, 0, 0, (0,))
            pump(0, 1, 0, (0,))
            for load in loads:
                load.wait()
            lax.fori_loop(0, toks // 64, norm_step, 0)

            @pl.when(z == 0)
            def _():
                for ll in range(layers):
                    nrm[ll, 0:PAD, :] = jnp.zeros((PAD, width), BF16)

            edge = Halo(0, nrm.at[0, pl.ds(group, PAD), half_cols(c)],
                        nrm.at[0, pl.ds(0, PAD), half_cols(c)])
            edge.rise()
            own_near = [message(("g_near", j), spot(q, j), spot(q, j), near_dev, ("near", j)) for j in range(2)]
            passed, relays, own_far = [], {}, []
            pump(0, 0, 0, (1, 2, 3))
            edge.spread()
            to_far(0)
            to_far(1)
            pump(0, 0, 1)
            pass_on(0)
            pass_on(1)
            share(0, (2,))
            relay(2, 0)
            relay(2, 1)
            for t in range(2, planes - 1):
                pump(0, 0, t)
            relay(3, 0)
            relay(3, 1)
            for ll in range(1, layers):
                share(ll, (0, 1, 2))
            pump(0, 1, 0, (1, 2, 3))
            edge.swap()
            for m in relays.values():
                m.wait_recv()
            edge.finish()
            gate_part(0, 0, z, 0, total_rows, tile)
            for t in range(1, planes):
                for d in range(2):
                    @pl.when(holds(d, t))
                    def _(t=t, d=d):
                        consume_one(0, 0, t, d)
                        gate_part(0, t, z - t if d == 0 else z + t, 0, total_rows, tile)

            def gate_end(r, _):
                at = pl.ds(al(r * tile, 16), tile)
                gated = (acc[at, :ch] * jax.nn.sigmoid(acc[at, ch:])).astype(BF16)
                gat[at, :] = gated.astype(F32)
                return 0

            lax.fori_loop(0, total_rows // tile, gate_end, 0)
            pump(0, 1, 1)

        lead = PAD - (taps_n - 1)
        step_rows = 64

        def conv_step(r, _):
            at = al(r * step_rows, step_rows)
            for lane in range(ch // lanes):
                cut = slice(lane * lanes, (lane + 1) * lanes)
                total = jnp.zeros((step_rows, lanes), F32)
                block = gat[pl.ds(at, step_rows + PAD), cut]
                for b in range(8):
                    moved = block if b == 0 else pltpu.roll(block, step_rows + PAD - b, 0)
                    for a in range(PAD // 8 + 1):
                        tap = 8 * a + b - lead
                        if 0 <= tap < taps_n:
                            total = total + taps[tap, l:l + 1, cut] * moved[8 * a:8 * a + step_rows]
                fil[pl.ds(at, step_rows), cut] = total
            return 0

        per = part_rows // step_rows
        sums = []
        for part in range(PARTS):
            lax.fori_loop(part * per, (part + 1) * per, conv_step, 0)
            wide = fil[part * part_rows:(part + 1) * part_rows, :]
            first_sum = jnp.sum(wide, axis=1, keepdims=True)
            second_sum = jnp.sum(wide * wide, axis=1, keepdims=True)
            lane_id = lax.broadcasted_iota(jnp.int32, (part_rows, lanes), 1)
            stat = jnp.where(lane_id == 0, first_sum, jnp.where(lane_id == 1, second_sum, 0.0))
            ssend[l, part] = jnp.transpose(stat)[0:2, :]
            sums.append([message(("sum", part, k), ssend.at[l, part], srecv.at[l, part, k], dev, "sum")
                         for k, dev in enumerate(plane_devs)])
        for t in range(2, planes - 1):
            pump(l, 1, t)
        if not last_layer:
            pump(l + 1, 0, 0)
        for part in range(PARTS):
            span = slice(part * part_rows, (part + 1) * part_rows)
            for m in sums[part]:
                m.wait_recv()
            whole = ssend[l, part]
            for k in range(len(plane_devs)):
                whole = whole + srecv[l, part, k]
            turn[0:2, 0:part_rows] = whole
            stat = jnp.transpose(turn[:, 0:part_rows])
            mean_value = stat[:, 0:1] / width
            variance = stat[:, 1:2] / width - mean_value * mean_value
            act[span, :] = jax.nn.silu((fil[span, :] - mean_value) * lax.rsqrt(variance + epsilon)
                                       * cgain[l:l + 1, :]).astype(BF16)

        def out_cols(h, u):
            return pl.ds(al(plane_at(u) * 4 * rows + h * chunk, chunk), chunk)

        def stage_swap(u):
            if u > 0:
                consume(l, 1, u)
            weights = wo[l, :, out_cols(1 - c, u)]
            for m, pair in enumerate(((near, diag), (far, q))):
                for k, b in enumerate(pair):
                    dsend[l, u, m, k] = jnp.dot(act[block_rows(b), :], weights,
                                                preferred_element_type=F32).astype(BF16)
                swaps[u, m] = message(("swap", u, m), dsend.at[l, u, m], drecv.at[l, u, m], core_dev, "swap")

        def stage_first(u):
            weights = wo[l, :, out_cols(c, u)]

            def partial(b, m, k):
                return (jnp.dot(act[block_rows(b), :], weights, preferred_element_type=F32)
                        + drecv[l, u, m, k].astype(F32))

            swaps[u, 0].wait_recv()
            for k, b in enumerate((far, diag)):
                term = partial(b, 0, k).astype(BF16)
                for j in range(2):
                    asend[l, u, j, k] = term[j * unit:(j + 1) * unit]
            for j in range(2):
                firsts[u, j] = message(("first", u, j), asend.at[l, u, j], arecv.at[l, u, j], far_dev, "first")
            swaps[u, 1].wait_recv()
            through[u] = partial(near, 1, 0)
            mine[u] = partial(q, 1, 1) + source[:, out_cols(c, u)].astype(F32)

        def stage_second(u, j):
            span = slice(j * unit, (j + 1) * unit)
            firsts[u, j].wait_recv()
            bsend[l, u, j] = (through[u, span] + arecv[l, u, j, 1].astype(F32)).astype(BF16)
            seconds[u, j] = message(("second", u, j), bsend.at[l, u, j], brecv.at[l, u, j], near_dev, "second")
            mine[u, span] = mine[u, span] + arecv[l, u, j, 0].astype(F32)

        def stage_last(u, j):
            span = slice(j * unit, (j + 1) * unit)
            seconds[u, j].wait_recv()
            final = (mine[u, span] + brecv[l, u, j].astype(F32)).astype(BF16)
            strm[l, span, out_cols(c, u)] = final
            if last_layer:
                piece = strm.at[l, span, out_cols(c, u)]
                lasts[u, j] = message(("c_own" if j else "c_near", u), piece, piece, core_dev, "last")
                write(u, j, c)
            else:
                wide = final.astype(F32)
                nrm[l + 1, pl.ds(al(PAD + q * toks + j * unit, 32), unit), out_cols(c, u)] = (
                    wide * gain[l + 1:l + 2, out_cols(c, u)]).astype(BF16)
                square = wide * wide
                folded = sum(square[:, k * lanes:(k + 1) * lanes] for k in range(chunk // lanes))
                squares[span, :] = folded if u == 0 else squares[span, :] + folded

        def write(u, j, h):
            span = slice(j * unit, (j + 1) * unit)
            pltpu.make_async_copy(strm.at[l, span, out_cols(h, u)], out.at[span, out_cols(h, u)],
                                  out_sem.at[0]).start()

        def finish(u, j):
            lasts[u, j].wait_recv()
            write(u, j, 1 - c)

        def lot(b, u):
            return nrm.at[l + 1, pl.ds(al(PAD + b * toks, 32), toks), out_cols(c, u)]

        def pass_chunk(kind, u, b, dev):
            moves[kind, u] = message((kind, u), lot(b, u), lot(b, u), dev, kind[0])

        def gather(u):
            pass_chunk("g_near", u, q, near_dev)
            pass_chunk("g_far", u, q, far_dev)
            pass_chunk("c_own", u, q, core_dev)

        def forward(u):
            moves["g_near", u].wait_recv()
            pass_chunk("g_pass", u, near, far_dev)
            pass_chunk("c_near", u, near, core_dev)

        def cross_far(u):
            moves["g_far", u].wait_recv()
            pass_chunk("c_far", u, far, core_dev)

        def cross_diag(u):
            moves["g_pass", u].wait_recv()
            pass_chunk("c_diag", u, diag, core_dev)

        def gate_chunk(u):
            if u > 0:
                consume(l + 1, 0, u)
            for kind in ("c_own", "c_near", "c_far", "c_diag"):
                moves[kind, u].wait_recv()
            gate_part(l + 1, u, plane_at(u), PAD, group, toks)

        def send_squares():
            lane_id = lax.broadcasted_iota(jnp.int32, (toks, lanes), 1)
            total = jnp.sum(squares[...], axis=1, keepdims=True)
            qsend[l] = jnp.transpose(jnp.where(lane_id == 0, total, 0.0))[0:2, :]
            return [message(("square", k), qsend.at[l], qrecv.at[l, k], dev, "square")
                    for k, dev in enumerate(plane_devs)]

        def row_scale(whole):
            turn[0:2, 0:toks] = whole
            return lax.rsqrt(jnp.transpose(turn[:, 0:toks])[:, 0:1] / width + epsilon)

        def send_edge(edge):
            norms[0].wait_recv()
            scale = row_scale(qsend[l] + qrecv[l, 0])[toks - PAD:]
            for u in range(planes):
                edge_out[l, :, pl.ds(al(plane_at(u) * chunk, chunk), chunk)] = (
                    strm[l, toks - PAD:, out_cols(c, u)].astype(F32) * scale
                    * gain[l + 1:l + 2, out_cols(c, u)]).astype(BF16)
            edge.rise()

        def gate_final(edge):
            edge.finish()

            @pl.when(z > 0)
            def _():
                for p in range(planes):
                    for h in range(2):
                        at = p * 4 * rows + h * chunk
                        nrm[l + 1, 0:PAD, at:at + chunk] = edge_in[l, h, :, p * chunk:(p + 1) * chunk]

            both = jnp.dot(nrm[l + 1, 0:PAD, :], wvg[l + 1], preferred_element_type=F32)
            gat[0:PAD, :] = (both[:, :ch] * jax.nn.sigmoid(both[:, ch:])).astype(BF16).astype(F32)
            for m in norms[1:]:
                m.wait_recv()
            for k in range(4):
                mate = qsend[l] if k == 0 else qrecv[l, 2 * k - 1]
                scale = row_scale(mate + qrecv[l, 2 * k])
                at = pl.ds(al(PAD + quad[k] * toks, 32), toks)
                value, gate = acc[at, :ch] * scale, acc[at, ch:] * scale
                gat[at, :] = (value * jax.nn.sigmoid(gate)).astype(BF16).astype(F32)

        swaps, firsts, seconds, lasts, moves = {}, {}, {}, {}, {}
        lag = 4
        for i in range(planes + lag + 1):
            if i < planes:
                stage_swap(i)
            if 1 <= i <= planes:
                stage_first(i - 1)
            for j in range(2):
                if 0 <= i - lag < planes:
                    stage_second(i - lag, j)
                if 0 <= i - lag - 1 < planes:
                    stage_last(i - lag - 1, j)
            if not last_layer:
                if i - lag - 1 >= 0:
                    gather(i - lag - 1)
                if i - lag - 3 >= 0:
                    forward(i - lag - 3)
                if i == lag + 2:
                    pump(l + 1, 0, 1)
            if last_layer and i == planes:
                drain(l, 0)
                drain(l, 1)
                pltpu.make_async_remote_copy(
                    wvg.at[:, 0:9 * rows // 2, :], wvg.at[:, 0:9 * rows // 2, :], wx_send.at[0],
                    wx_recv.at[0, 0], device_id=core_dev, device_id_type=MESH).wait_send()
                all_sent("ag", nrm.at[0, PAD:PAD + 5 * toks // 2, :])
                all_sent("sum", srecv)
                if layers > 1:
                    all_sent("square", qrecv.at[0:layers - 1])
                    all_sent("g", nrm.at[1:layers, PAD:PAD + 3 * toks, 0:half])
                    all_sent("c", nrm.at[1:layers, PAD:PAD + group, 0:half])
        if last_layer:
            for u in range(planes):
                for j in range(2):
                    finish(u, j)
        else:
            edge = Halo(l + 1, edge_out.at[l], edge_in.at[l, c])
            norms = send_squares()
            cross_far(0)
            send_edge(edge)
            ahead = planes - 2
            for u in range(ahead, planes + ahead):
                if u < planes:
                    forward(u)
                    cross_far(u - ahead + 1)
                elif u - ahead + 1 < planes:
                    cross_far(u - ahead + 1)
                cross_diag(u - ahead)
                if u == ahead:
                    for t in range(2, planes - 1):
                        pump(l + 1, 0, t)
                if u == ahead + 1:
                    edge.spread()
                    pump(l + 1, 1, 0)
                gate_chunk(u - ahead)
                if u == ahead + 2:
                    drain(l, 0)
                    drain(l, 1)
            edge.swap()
            gate_final(edge)
            pump(l + 1, 1, 1)

    all_sent("swap", dsend)
    all_sent("first", asend)
    all_sent("second", bsend)
    all_sent("last", strm.at[layers - 1, :, 0:half])
    pltpu.make_async_copy(strm.at[layers - 1], out, out_sem.at[0]).wait()


def fused(n, layers):
    def body(stream_in, norm_gain, value_weight, gate_weight, conv_taps, channel_gain, out_weight):
        toks, width = stream_in.shape
        taps_n = conv_taps.shape[1]
        rows, cols = value_weight.shape[1], value_weight.shape[2]
        ch, half, group, planes = cols // 4, width // 2, 4 * toks, n // 4
        chunk = 2 * rows
        taps = jnp.transpose(conv_taps, (1, 0, 2))
        hbm = pl.BlockSpec(memory_space=pltpu.HBM)
        msgs = 7 + 7 * PARTS + 13 * planes
        return pl.pallas_call(
            functools.partial(kernel, n, layers, taps_n),
            out_shape=jax.ShapeDtypeStruct((toks, width), BF16),
            in_specs=[hbm] * 7,
            out_specs=hbm,
            scratch_shapes=[
                pltpu.VMEM((toks, width), BF16),
                pltpu.VMEM((layers, width), F32),
                pltpu.VMEM((taps_n, layers, ch), F32),
                pltpu.VMEM((layers, ch), F32),
                pltpu.VMEM((layers, width, 2 * ch), BF16),
                pltpu.VMEM((layers, ch, width), BF16),
                pltpu.VMEM((layers, PAD + group, width), BF16),
                pltpu.VMEM((PAD + group, ch), F32),
                pltpu.VMEM((group, ch), F32),
                pltpu.VMEM((group, ch), BF16),
                pltpu.VMEM((layers, PARTS, 2, group // PARTS), F32),
                pltpu.VMEM((layers, PARTS, 7, 2, group // PARTS), F32),
                pltpu.VMEM((layers, planes, 2, 2, toks, chunk), BF16),
                pltpu.VMEM((layers, planes, 2, 2, toks, chunk), BF16),
                pltpu.VMEM((layers, planes, 2, 2, toks // 2, chunk), BF16),
                pltpu.VMEM((layers, planes, 2, 2, toks // 2, chunk), BF16),
                pltpu.VMEM((layers, planes, 2, toks // 2, chunk), BF16),
                pltpu.VMEM((layers, planes, 2, toks // 2, chunk), BF16),
                pltpu.VMEM((planes, toks, chunk), F32),
                pltpu.VMEM((planes, toks, chunk), F32),
                pltpu.VMEM((layers, toks, width), BF16),
                pltpu.VMEM((PAD + group, 2 * ch), F32),
                pltpu.VMEM((128, group), F32),
                pltpu.VMEM((toks, 128), F32),
                pltpu.VMEM((layers, 2, toks), F32),
                pltpu.VMEM((layers, 7, 2, toks), F32),
                pltpu.VMEM((layers, PAD, half), BF16),
                pltpu.VMEM((layers, 2, PAD, half), BF16),
                pltpu.SemaphoreType.DMA((4,)),
                pltpu.SemaphoreType.DMA((1,)),
                pltpu.SemaphoreType.DMA((layers * 3,)),
                pltpu.SemaphoreType.DMA((1,)),
                pltpu.SemaphoreType.DMA((layers * 3, 3)),
                pltpu.SemaphoreType.DMA((layers * 4, planes - 1)),
                pltpu.SemaphoreType.DMA((layers * 4, planes - 1, 2)),
                pltpu.SemaphoreType.DMA((layers, 5)),
                pltpu.SemaphoreType.DMA((layers, 3)),
                pltpu.SemaphoreType.DMA((11,)),
                pltpu.SemaphoreType.DMA((msgs,)),
            ],
            compiler_params=pltpu.CompilerParams(
                collective_id=0, has_side_effects=True, vmem_limit_bytes=62 * 2**20),
        )(stream_in, norm_gain, value_weight, gate_weight, taps, channel_gain, out_weight)

    return body


def passed_along(value, axis, steps):
    count = lax.axis_size(axis)
    leading, last = (max(0, -steps), min(count, count - steps))
    return lax.ppermute(value, axis, [(source, source + steps) for source in range(leading, last)])


def general(stream_in, norm_gain, value_weight, gate_weight, conv_taps, channel_gain, out_weight):
    stream = stream_in
    tok_rows = stream_in.shape[0]
    width = stream_in.shape[1]
    taps_n = conv_taps.shape[1]
    local_cols = value_weight.shape[2]
    for layer in range(norm_gain.shape[0]):
        wide = stream.astype(F32)
        normed = (
            wide
            * lax.rsqrt(jnp.mean(wide * wide, axis=1, keepdims=True) + epsilon)
            * norm_gain[layer]
        ).astype(BF16)
        value = jnp.dot(normed, lax.all_gather(value_weight[layer], "sp", axis=0, tiled=True),
                        preferred_element_type=F32)
        gate = jnp.dot(normed, lax.all_gather(gate_weight[layer], "sp", axis=0, tiled=True),
                       preferred_element_type=F32)
        gated = (value * jax.nn.sigmoid(gate)).astype(BF16)
        earlier = passed_along(gated[tok_rows - (taps_n - 1):], "sp", 1)
        padded = jnp.concatenate([earlier, gated], axis=0).astype(F32)
        taps = conv_taps[layer]
        filtered = jnp.zeros((tok_rows, local_cols), F32)
        for tap in range(taps_n):
            filtered = filtered + taps[tap] * padded[tap:tap + tok_rows]
        sum_first, sum_second = lax.psum(
            (jnp.sum(filtered, axis=1), jnp.sum(filtered * filtered, axis=1)), "tp")
        mean_value = (sum_first / width)[:, None]
        variance = (sum_second / width)[:, None] - mean_value * mean_value
        activated = jax.nn.silu(
            (filtered - mean_value) * lax.rsqrt(variance + epsilon) * channel_gain[layer]
        ).astype(BF16)
        whole_out = lax.all_gather(out_weight[layer], "sp", axis=1, tiled=True)
        terms = jnp.dot(activated, whole_out, preferred_element_type=F32)
        summed = lax.psum(terms.astype(BF16), "tp").astype(F32)
        stream = (wide + summed).astype(BF16)
    return stream


def solution(mesh):
    n, tp = mesh.shape["sp"], mesh.shape["tp"]

    def body(stream_in, norm_gain, value_weight, *rest):
        rows, cols = value_weight.shape[1], value_weight.shape[2]
        quads = tp == 2 and n % 4 == 0 and n >= 8 and rows % 128 == 0 and cols % 512 == 0
        fits = stream_in.shape[0] % 64 == 0 and rest[1].shape[1] <= PAD
        chosen = fused(n, norm_gain.shape[0]) if quads and fits else general
        return chosen(stream_in, norm_gain, value_weight, *rest)

    return jax.shard_map(
        body,
        mesh=mesh,
        in_specs=(
            P("sp", None),
            P(),
            P(None, "sp", "tp"),
            P(None, "sp", "tp"),
            P(None, None, "tp"),
            P(None, "tp"),
            P(None, "tp", "sp"),
        ),
        out_specs=P("sp", None),
        check_vma=False,
    )
```

```python
import functools

import jax
import jax.numpy as jnp
from jax import lax
from jax.experimental import pallas as pl
from jax.experimental.pallas import tpu as pltpu
from jax.sharding import PartitionSpec as P

epsilon = 1e-05
MESH = pl.DeviceIdType.MESH
F32 = jnp.float32
BF16 = jnp.bfloat16
PAD = 32
PARTS = 2


def kernel(n, layers, taps_n, stream_hbm, gain_hbm, vw, gw, taps_hbm, cgain_hbm, ow, out,
           stream_in, gain, taps, cgain, wvg, wo, nrm, gat, fil, act, ssend, srecv, dsend, drecv,
           asend, arecv, bsend, brecv, mine, through, strm, acc, turn,
           squares, qsend, qrecv, edge_out, edge_in,
           in_sem, out_sem, loc_sem, wx_send, wx_recv, z_send, z_recv, halo_send, halo_recv,
           msg_send, msg_recv):
    planes = n // 4
    s = lax.axis_index("sp")
    c = lax.axis_index("tp")
    z, q = s // 4, s % 4
    y, x = q // 2, q % 2
    quad = [q, q + 1 - 2 * x, q + 2 - 4 * y, 3 - q]
    toks, width = stream_in.shape
    group = 4 * toks
    rows, cols = vw.shape[1], vw.shape[2]
    ch = cols // 4
    half = width // 2
    chunk = 2 * rows
    near = (1 - c) * quad[1] + c * quad[2]
    far = c * quad[1] + (1 - c) * quad[2]
    diag = quad[3]
    near_dev, far_dev, core_dev = (z * 4 + near, c), (z * 4 + far, c), (s, 1 - c)
    up_dev, down_dev = (s + 4, c), (s - 4, c)

    def al(v, m):
        return pl.multiple_of(v, m)

    barrier = pltpu.get_barrier_semaphore()
    plane_devs = [(z * 4 + quad[k], cc) for k in range(4) for cc in (c, 1 - c)][1:]
    for dev in plane_devs:
        pl.semaphore_signal(barrier, inc=1, device_id=dev, device_id_type=MESH)

    @pl.when(z < planes - 1)
    def _():
        pl.semaphore_signal(barrier, inc=1, device_id=up_dev, device_id_type=MESH)

    @pl.when(z > 0)
    def _():
        pl.semaphore_signal(barrier, inc=1, device_id=down_dev, device_id_type=MESH)

    own_ch = pl.ds(al(q * ch, ch), ch)
    loads = [pltpu.make_async_copy(a, b, in_sem.at[k]) for k, (a, b) in enumerate((
        (stream_hbm, stream_in), (gain_hbm, gain), (taps_hbm.at[:, :, own_ch], taps),
        (cgain_hbm.at[:, own_ch], cgain)))]
    for load in loads:
        load.start()

    shared = {}

    def shared_copy(l, kind, k):
        mine_rows = pl.ds(al(s * rows, rows), rows)
        span = pl.ds(al(quad[k] * ch, ch), ch)
        if kind == 2:
            src, dst = ow.at[l, span, :], wo.at[l, :, mine_rows]
        else:
            src = (vw, gw)[kind].at[l, :, span]
            dst = wvg.at[l, mine_rows, pl.ds(kind * ch, ch)]
        idx = l * 3 + kind
        if k == 0:
            copy = pltpu.make_async_copy(src, dst, loc_sem.at[idx])
        else:
            copy = pltpu.make_async_remote_copy(
                src, dst, wx_send.at[0], wx_recv.at[idx, k - 1],
                device_id=(z * 4 + quad[k], c), device_id_type=MESH)
        copy.start()
        shared[l, kind, k] = copy

    def share(l, kinds, ks=(1, 2, 3)):
        for k in ks:
            for kind in kinds:
                shared_copy(l, kind, k)

    for l in range(layers):
        share(l, (0, 1, 2), (0,))

    pl.semaphore_wait(barrier, len(plane_devs) + (z < planes - 1).astype(jnp.int32)
                      + (z > 0).astype(jnp.int32))

    def z_copy(l, grp, d, t, hop, first, count, pair):
        plane = z - t if d == 0 else z + t
        block = pl.ds(al((plane * 4 + first) * rows, rows), count * rows)
        ref = wvg.at[l, block, :] if grp == 0 else wo.at[l, :, block]
        idx = (l * 2 + grp) * 2 + d
        return pltpu.make_async_remote_copy(
            ref, ref, z_send.at[idx, hop], z_recv.at[idx, hop, pair],
            device_id=up_dev if d == 0 else down_dev, device_id_type=MESH)

    def z_pair(l, grp, d, t, hop, pair):
        return z_copy(l, grp, d, t, hop, 2 * (y + pair - 2 * y * pair), 2, pair)

    def holds(d, t):
        return z >= t if d == 0 else z + t < planes

    def sends(d):
        return z < planes - 1 if d == 0 else z > 0

    def pump(l, grp, t, ks=(0, 1, 2, 3)):
        if t == 0:
            for k in ks:
                for kind in ((0, 1) if grp == 0 else (2,)):
                    if k:
                        shared[l, kind, k].wait_recv()
                    else:
                        shared[l, kind, k].wait()
                if l == 0:
                    for d in range(2):
                        @pl.when(sends(d))
                        def _(k=k, d=d):
                            z_copy(l, grp, d, 0, 0, quad[k], 1, k // 2).start()
        if t > 0 or l > 0:
            for pair in range(2):
                for d in range(2):
                    @pl.when(holds(d, t) & sends(d))
                    def _(pair=pair, d=d):
                        if t > 0:
                            z_pair(l, grp, d, t, t - 1, pair).wait_recv()
                        z_pair(l, grp, d, t, t, pair).start()

    def consume_one(l, grp, t, d):
        @pl.when(jnp.logical_not(sends(d)))
        def _():
            for pair in range(2):
                z_pair(l, grp, d, t, t - 1, pair).wait_recv()

    def consume(l, grp, t):
        for d in range(2):
            @pl.when(holds(d, t))
            def _(d=d):
                consume_one(l, grp, t, d)

    def drain(l, grp):
        for t in range(planes - 1):
            for d in range(2):
                @pl.when(holds(d, t) & sends(d))
                def _(t=t, d=d):
                    z_copy(l, grp, d, t, t, 0, 4, 0).wait_send()

    turn[...] = jnp.zeros_like(turn)
    slots, kinds_sent = {}, {}

    def message(name, src, dst, dev, sender):
        slot = slots.setdefault(name, len(slots))
        kind = kinds_sent.setdefault(sender, len(kinds_sent))
        m = pltpu.make_async_remote_copy(src, dst, msg_send.at[kind], msg_recv.at[slot],
                                         device_id=dev, device_id_type=MESH)
        m.start()
        return m

    def all_came(name, ref):
        pltpu.make_async_remote_copy(ref, ref, msg_send.at[0], msg_recv.at[slots[name]],
                                     device_id=core_dev, device_id_type=MESH).wait_recv()

    def all_sent(sender, ref):
        pltpu.make_async_remote_copy(ref, ref, msg_send.at[kinds_sent[sender]], msg_recv.at[0],
                                     device_id=core_dev, device_id_type=MESH).wait_send()

    share(0, (0, 1))

    def block_rows(b):
        return pl.ds(al(b * toks, toks), toks)

    def half_cols(h):
        return pl.ds(al(h * half, half), half)

    unit = toks // 2
    total_rows = PAD + group
    tile = max(v for v in range(16, 401, 16) if total_rows % v == 0)
    bounds = (0, 3 * toks, group)
    lanes = 128

    def plane_at(u):
        low = jnp.where(u <= z, z - u, u)
        zm = planes - 1 - z
        high = planes - 1 - jnp.where(u <= zm, zm - u, u)
        return jnp.where(2 * z < planes, low, high)

    def norm_step(r, _):
        at = al(r * 64, 64)
        wide = stream_in[pl.ds(at, 64), :].astype(F32)
        scale = lax.rsqrt(jnp.mean(wide * wide, axis=1, keepdims=True) + epsilon)
        nrm[0, pl.ds(al(PAD + q * toks + at, 32), 64), :] = (
            wide * scale * gain[0:1, :]).astype(BF16)
        return 0

    class Halo:
        def __init__(self, l, border, first):
            def copy(k, dev, src, recv):
                return pltpu.make_async_remote_copy(
                    src, first, halo_send.at[l, k], halo_recv.at[l, recv],
                    device_id=dev, device_id_type=MESH)

            self.up = copy(0, up_dev, border, 0)
            self.side = [copy(k, (z * 4 + quad[k], c), first, 1) for k in (1, 2, 3)]
            self.core = copy(4, core_dev, first, 2)

        def rise(self):
            @pl.when((q == 3) & (z < planes - 1))
            def _():
                self.up.start()

        def spread(self):
            @pl.when((q == 3) & (z > 0))
            def _():
                self.up.wait_recv()
                for m in self.side:
                    m.start()
                self.core.start()

        def swap(self):
            @pl.when((q != 3) & (z > 0))
            def _():
                self.side[0].wait_recv()
                self.core.start()

        def finish(self):
            @pl.when(z > 0)
            def _():
                self.core.wait()

            @pl.when((q == 3) & (z > 0))
            def _():
                for m in self.side:
                    m.wait_send()

            @pl.when((q == 3) & (z < planes - 1))
            def _():
                self.up.wait_send()

    def spot(b, j):
        return nrm.at[0, pl.ds(al(PAD + b * toks + j * unit, 32), unit), half_cols(c)]

    def to_far(j):
        own_near[j].wait_send()
        own_far.append(message(("g_far", j), spot(q, j), spot(q, j), far_dev, "ag"))

    def pass_on(j):
        own_near[j].wait_recv()
        passed.append(message(("g_pass", j), spot(near, j), spot(near, j), far_dev, "ag"))
        relays[1, j] = message(("c", 0), spot(near, j), spot(near, j), core_dev, "ag")

    def relay(which, j):
        (own_far if which == 2 else passed)[j].wait_recv()
        b = far if which == 2 else diag
        relays[which, j] = message(("c", 0), spot(b, j), spot(b, j), core_dev, "ag")

    def gate_part(l, t, plane, start, count, size):
        depth = pl.ds(al(plane * 4 * rows, 4 * rows), 4 * rows)

        def gate_step(r, _):
            at = pl.ds(al(start + r * size, 16), size)
            term = jnp.dot(nrm[l, at, depth], wvg[l, depth, :], preferred_element_type=F32)
            acc[at, :] = term if t == 0 else acc[at, :] + term
            return 0

        lax.fori_loop(0, count // size, gate_step, 0)

    for l in range(layers):
        last_layer = l + 1 == layers
        source = stream_in if l == 0 else strm.at[l - 1]

        if l == 0:
            pump(0, 0, 0, (0,))
            pump(0, 1, 0, (0,))
            for load in loads:
                load.wait()
            lax.fori_loop(0, toks // 64, norm_step, 0)

            @pl.when(z == 0)
            def _():
                for ll in range(layers):
                    nrm[ll, 0:PAD, :] = jnp.zeros((PAD, width), BF16)

            edge = Halo(0, nrm.at[0, pl.ds(group, PAD), half_cols(c)],
                        nrm.at[0, pl.ds(0, PAD), half_cols(c)])
            edge.rise()
            own_near = [message(("g_near", j), spot(q, j), spot(q, j), near_dev, ("near", j)) for j in range(2)]
            passed, relays, own_far = [], {}, []
            pump(0, 0, 0, (1, 2, 3))
            edge.spread()
            to_far(0)
            to_far(1)
            pump(0, 0, 1)
            pass_on(0)
            pass_on(1)
            share(0, (2,))
            relay(2, 0)
            relay(2, 1)
            for t in range(2, planes - 1):
                pump(0, 0, t)
            relay(3, 0)
            relay(3, 1)
            for ll in range(1, layers):
                share(ll, (0, 1, 2))
            pump(0, 1, 0, (1, 2, 3))
            edge.swap()
            all_came(("c", 0), nrm.at[0, PAD:PAD + 3 * toks, 0:half])
            edge.finish()
            gate_part(0, 0, z, 0, total_rows, tile)
            for t in range(1, planes):
                for d in range(2):
                    @pl.when(holds(d, t))
                    def _(t=t, d=d):
                        consume_one(0, 0, t, d)
                        gate_part(0, t, z - t if d == 0 else z + t, 0, total_rows, tile)

            def gate_end(r, _):
                at = pl.ds(al(r * tile, 16), tile)
                gated = (acc[at, :ch] * jax.nn.sigmoid(acc[at, ch:])).astype(BF16)
                gat[at, :] = gated.astype(F32)
                return 0

            lax.fori_loop(0, total_rows // tile, gate_end, 0)
            pump(0, 1, 1)

        lead = PAD - (taps_n - 1)
        step_rows = 64

        def conv_step(r, _):
            at = al(r * step_rows, step_rows)
            for lane in range(ch // lanes):
                cut = slice(lane * lanes, (lane + 1) * lanes)
                total = jnp.zeros((step_rows, lanes), F32)
                block = gat[pl.ds(at, step_rows + PAD), cut]
                for b in range(8):
                    moved = block if b == 0 else pltpu.roll(block, step_rows + PAD - b, 0)
                    for a in range(PAD // 8 + 1):
                        tap = 8 * a + b - lead
                        if 0 <= tap < taps_n:
                            total = total + taps[tap, l:l + 1, cut] * moved[8 * a:8 * a + step_rows]
                fil[pl.ds(at, step_rows), cut] = total
            return 0

        sums = []
        for part in range(PARTS):
            low, high = bounds[part:part + 2]
            lax.fori_loop(low // step_rows, high // step_rows, conv_step, 0)
            wide = fil[low:high, :]
            first_sum = jnp.sum(wide, axis=1, keepdims=True)
            second_sum = jnp.sum(wide * wide, axis=1, keepdims=True)
            lane_id = lax.broadcasted_iota(jnp.int32, (high - low, lanes), 1)
            stat = jnp.where(lane_id == 0, first_sum, jnp.where(lane_id == 1, second_sum, 0.0))
            ssend[l, :, low:high] = jnp.transpose(stat)[0:2, :]
            sums.append([message(("sum", part), ssend.at[l, :, low:high], srecv.at[l, k, :, low:high],
                                 dev, "sum") for k, dev in enumerate(plane_devs)])
        for t in range(2, planes - 1):
            pump(l, 1, t)
        if not last_layer:
            pump(l + 1, 0, 0)
        for part in range(PARTS):
            low, high = bounds[part:part + 2]
            all_came(("sum", part), srecv.at[l, :, :, low:high])
            whole = ssend[l, :, low:high]
            for k in range(len(plane_devs)):
                whole = whole + srecv[l, k, :, low:high]
            turn[0:2, low:high] = whole
            stat = jnp.transpose(turn[:, low:high])
            mean_value = stat[:, 0:1] / width
            variance = stat[:, 1:2] / width - mean_value * mean_value
            act[low:high, :] = jax.nn.silu((fil[low:high, :] - mean_value) * lax.rsqrt(variance + epsilon)
                                           * cgain[l:l + 1, :]).astype(BF16)

        def out_cols(h, u):
            return pl.ds(al(plane_at(u) * 4 * rows + h * chunk, chunk), chunk)

        def stage_swap(u):
            if u > 0:
                consume(l, 1, u)
            weights = wo[l, :, out_cols(1 - c, u)]
            for m, pair in enumerate(((near, diag), (far, q))):
                for k, b in enumerate(pair):
                    dsend[l, u, m, k] = jnp.dot(act[block_rows(b), :], weights,
                                                preferred_element_type=F32).astype(BF16)
                swaps[u, m] = message(("swap", u, m), dsend.at[l, u, m], drecv.at[l, u, m], core_dev, "swap")

        def stage_first(u):
            weights = wo[l, :, out_cols(c, u)]

            def partial(b, m, k):
                return (jnp.dot(act[block_rows(b), :], weights, preferred_element_type=F32)
                        + drecv[l, u, m, k].astype(F32))

            swaps[u, 0].wait_recv()
            for k, b in enumerate((far, diag)):
                term = partial(b, 0, k).astype(BF16)
                for j in range(2):
                    asend[l, u, j, k] = term[j * unit:(j + 1) * unit]
            for j in range(2):
                firsts[u, j] = message(("first", u, j), asend.at[l, u, j], arecv.at[l, u, j], far_dev, "first")
            swaps[u, 1].wait_recv()
            through[u] = partial(near, 1, 0)
            mine[u] = partial(q, 1, 1) + source[:, out_cols(c, u)].astype(F32)

        def stage_take(u, j):
            span = slice(j * unit, (j + 1) * unit)
            firsts[u, j].wait_recv()
            bsend[l, u, j] = (through[u, span] + arecv[l, u, j, 1].astype(F32)).astype(BF16)
            mine[u, span] = mine[u, span] + arecv[l, u, j, 0].astype(F32)

        def stage_give(u, j):
            seconds[u, j] = message(("second", u, j), bsend.at[l, u, j], brecv.at[l, u, j], near_dev,
                                    "second")

        def stage_last(u, j):
            span = slice(j * unit, (j + 1) * unit)
            seconds[u, j].wait_recv()
            final = (mine[u, span] + brecv[l, u, j].astype(F32)).astype(BF16)
            strm[l, span, out_cols(c, u)] = final
            if last_layer:
                piece, place = strm.at[l, span, out_cols(c, u)], out.at[span, out_cols(c, u)]
                message(("c", 0), piece, place, core_dev, "last")
                pltpu.make_async_copy(piece, place, out_sem.at[0]).start()
            else:
                wide = final.astype(F32)
                nrm[l + 1, pl.ds(al(PAD + q * toks + j * unit, 32), unit), out_cols(c, u)] = (
                    wide * gain[l + 1:l + 2, out_cols(c, u)]).astype(BF16)
                square = wide * wide
                folded = sum(square[:, k * lanes:(k + 1) * lanes] for k in range(chunk // lanes))
                squares[span, :] = folded if u == 0 else squares[span, :] + folded

        def lot(b, u):
            return nrm.at[l + 1, pl.ds(al(PAD + b * toks, 32), toks), out_cols(c, u)]

        def pass_chunk(kind, u, b, dev):
            moves[kind, u] = message((kind if kind[0] == "g" else "c", u), lot(b, u), lot(b, u), dev, kind[0])

        def gather(u):
            pass_chunk("g_near", u, q, near_dev)
            pass_chunk("c_own", u, q, core_dev)

        def forward(u):
            moves["g_near", u].wait_recv()
            pass_chunk("g_far", u, q, far_dev)
            pass_chunk("g_pass", u, near, far_dev)
            pass_chunk("c_near", u, near, core_dev)

        def cross_far(u):
            moves["g_far", u].wait_recv()
            pass_chunk("c_far", u, far, core_dev)

        def cross_diag(u):
            moves["g_pass", u].wait_recv()
            pass_chunk("c_diag", u, diag, core_dev)

        def gate_chunk(u):
            if u > 0:
                consume(l + 1, 0, u)
            all_came(("c", u), nrm.at[l + 1, PAD:PAD + group, 0:chunk])
            gate_part(l + 1, u, plane_at(u), PAD, group, toks)

        def send_squares():
            lane_id = lax.broadcasted_iota(jnp.int32, (toks, lanes), 1)
            total = jnp.sum(squares[...], axis=1, keepdims=True)
            qsend[l] = jnp.transpose(jnp.where(lane_id == 0, total, 0.0))[0:2, :]
            return [message(("square", k > 0), qsend.at[l], qrecv.at[l, k], dev, "square")
                    for k, dev in enumerate(plane_devs)]

        def row_scale(whole):
            turn[0:2, 0:toks] = whole
            return lax.rsqrt(jnp.transpose(turn[:, 0:toks])[:, 0:1] / width + epsilon)

        def send_edge(edge):
            norms[0].wait_recv()
            scale = row_scale(qsend[l] + qrecv[l, 0])[toks - PAD:]
            for u in range(planes):
                edge_out[l, :, pl.ds(al(plane_at(u) * chunk, chunk), chunk)] = (
                    strm[l, toks - PAD:, out_cols(c, u)].astype(F32) * scale
                    * gain[l + 1:l + 2, out_cols(c, u)]).astype(BF16)
            edge.rise()

        def gate_final(edge):
            u = planes - 1
            consume(l + 1, 0, u)
            edge.finish()

            @pl.when(z > 0)
            def _():
                for p in range(planes):
                    for h in range(2):
                        at = p * 4 * rows + h * chunk
                        nrm[l + 1, 0:PAD, at:at + chunk] = edge_in[l, h, :, p * chunk:(p + 1) * chunk]

            both = jnp.dot(nrm[l + 1, 0:PAD, :], wvg[l + 1], preferred_element_type=F32)
            gat[0:PAD, :] = (both[:, :ch] * jax.nn.sigmoid(both[:, ch:])).astype(BF16).astype(F32)
            all_came(("square", True), qrecv.at[l, 1:])
            all_came(("c", u), nrm.at[l + 1, PAD:PAD + group, 0:chunk])
            depth = pl.ds(al(plane_at(u) * 4 * rows, 4 * rows), 4 * rows)
            for k in range(4):
                mate = qsend[l] if k == 0 else qrecv[l, 2 * k - 1]
                scale = row_scale(mate + qrecv[l, 2 * k])
                at = pl.ds(al(PAD + quad[k] * toks, 32), toks)
                both = acc[at, :] + jnp.dot(nrm[l + 1, at, depth], wvg[l + 1, depth, :],
                                            preferred_element_type=F32)
                value, gate = both[:, :ch] * scale, both[:, ch:] * scale
                gat[at, :] = (value * jax.nn.sigmoid(gate)).astype(BF16).astype(F32)

        swaps, firsts, seconds, lasts, moves = {}, {}, {}, {}, {}
        for u in range(planes - 1):
            stage_swap(u)
            if u > 0:
                stage_first(u - 1)
        stage_first(planes - 2)
        stage_swap(planes - 1)
        stage_first(planes - 1)
        if last_layer:
            drain(l, 0)
            drain(l, 1)
            pltpu.make_async_remote_copy(
                wvg.at[:, 0:9 * rows // 2, :], wvg.at[:, 0:9 * rows // 2, :], wx_send.at[0],
                wx_recv.at[0, 0], device_id=core_dev, device_id_type=MESH).wait_send()
            all_sent("ag", nrm.at[0, PAD:PAD + 5 * toks // 2, :])
            all_sent("sum", srecv)
            if layers > 1:
                all_sent("square", qrecv.at[0:layers - 1])
                all_sent("g", nrm.at[1:layers, PAD:PAD + 3 * toks, 0:half])
                all_sent("c", nrm.at[1:layers, PAD:PAD + group, 0:half])
        for u in range(planes - 1):
            for j in range(2):
                stage_take(u, j)
            if u + 2 == planes:
                for uu in range(planes - 1):
                    for j in range(2):
                        stage_give(uu, j)
        for j in range(2):
            stage_take(planes - 1, j)
            stage_give(planes - 1, j)
        if not last_layer:
            pump(l + 1, 0, 1)
        for u in range(planes):
            for j in range(2):
                stage_last(u, j)
            if not last_layer:
                gather(u)
                if u >= 2:
                    forward(u - 2)
        if not last_layer:
            edge = Halo(l + 1, edge_out.at[l], edge_in.at[l, c])
            norms = send_squares()
            cross_far(0)
            send_edge(edge)
            ahead = planes - 2
            for u in range(ahead, planes + ahead):
                if u < planes:
                    forward(u)
                    cross_far(u - ahead + 1)
                elif u - ahead + 1 < planes:
                    cross_far(u - ahead + 1)
                cross_diag(u - ahead)
                if u == ahead:
                    for t in range(2, planes - 1):
                        pump(l + 1, 0, t)
                if u == ahead + 1:
                    edge.spread()
                    pump(l + 1, 1, 0)
                if u - ahead < planes - 1:
                    gate_chunk(u - ahead)
                if u == ahead + 2:
                    drain(l, 0)
                    drain(l, 1)
            edge.swap()
            gate_final(edge)
            pump(l + 1, 1, 1)

    all_sent("swap", dsend)
    all_sent("first", asend)
    all_sent("second", bsend)
    all_sent("last", strm.at[layers - 1, :, 0:half])
    whole_half = strm.at[layers - 1, :, 0:half]
    pltpu.make_async_copy(whole_half, out.at[:, 0:half], out_sem.at[0]).wait()
    all_came(("c", 0), whole_half)


def fused(n, layers):
    def body(stream_in, norm_gain, value_weight, gate_weight, conv_taps, channel_gain, out_weight):
        toks, width = stream_in.shape
        taps_n = conv_taps.shape[1]
        rows, cols = value_weight.shape[1], value_weight.shape[2]
        ch, half, group, planes = cols // 4, width // 2, 4 * toks, n // 4
        chunk = 2 * rows
        taps = jnp.transpose(conv_taps, (1, 0, 2))
        hbm = pl.BlockSpec(memory_space=pltpu.HBM)
        msgs = 2 + PARTS + 10 * planes
        return pl.pallas_call(
            functools.partial(kernel, n, layers, taps_n),
            out_shape=jax.ShapeDtypeStruct((toks, width), BF16),
            in_specs=[hbm] * 7,
            out_specs=hbm,
            scratch_shapes=[
                pltpu.VMEM((toks, width), BF16),
                pltpu.VMEM((layers, width), F32),
                pltpu.VMEM((taps_n, layers, ch), F32),
                pltpu.VMEM((layers, ch), F32),
                pltpu.VMEM((layers, width, 2 * ch), BF16),
                pltpu.VMEM((layers, ch, width), BF16),
                pltpu.VMEM((layers, PAD + group, width), BF16),
                pltpu.VMEM((PAD + group, ch), F32),
                pltpu.VMEM((group, ch), F32),
                pltpu.VMEM((group, ch), BF16),
                pltpu.VMEM((layers, 2, group), F32),
                pltpu.VMEM((layers, 7, 2, group), F32),
                pltpu.VMEM((layers, planes, 2, 2, toks, chunk), BF16),
                pltpu.VMEM((layers, planes, 2, 2, toks, chunk), BF16),
                pltpu.VMEM((layers, planes, 2, 2, toks // 2, chunk), BF16),
                pltpu.VMEM((layers, planes, 2, 2, toks // 2, chunk), BF16),
                pltpu.VMEM((layers, planes, 2, toks // 2, chunk), BF16),
                pltpu.VMEM((layers, planes, 2, toks // 2, chunk), BF16),
                pltpu.VMEM((planes, toks, chunk), F32),
                pltpu.VMEM((planes, toks, chunk), F32),
                pltpu.VMEM((layers, toks, width), BF16),
                pltpu.VMEM((PAD + group, 2 * ch), F32),
                pltpu.VMEM((128, group), F32),
                pltpu.VMEM((toks, 128), F32),
                pltpu.VMEM((layers, 2, toks), F32),
                pltpu.VMEM((layers, 7, 2, toks), F32),
                pltpu.VMEM((layers, PAD, half), BF16),
                pltpu.VMEM((layers, 2, PAD, half), BF16),
                pltpu.SemaphoreType.DMA((4,)),
                pltpu.SemaphoreType.DMA((1,)),
                pltpu.SemaphoreType.DMA((layers * 3,)),
                pltpu.SemaphoreType.DMA((1,)),
                pltpu.SemaphoreType.DMA((layers * 3, 3)),
                pltpu.SemaphoreType.DMA((layers * 4, planes - 1)),
                pltpu.SemaphoreType.DMA((layers * 4, planes - 1, 2)),
                pltpu.SemaphoreType.DMA((layers, 5)),
                pltpu.SemaphoreType.DMA((layers, 3)),
                pltpu.SemaphoreType.DMA((11,)),
                pltpu.SemaphoreType.DMA((msgs,)),
            ],
            compiler_params=pltpu.CompilerParams(
                collective_id=0, has_side_effects=True, vmem_limit_bytes=62 * 2**20),
        )(stream_in, norm_gain, value_weight, gate_weight, taps, channel_gain, out_weight)

    return body


def passed_along(value, axis, steps):
    count = lax.axis_size(axis)
    leading, last = (max(0, -steps), min(count, count - steps))
    return lax.ppermute(value, axis, [(source, source + steps) for source in range(leading, last)])


def general(stream_in, norm_gain, value_weight, gate_weight, conv_taps, channel_gain, out_weight):
    stream = stream_in
    tok_rows = stream_in.shape[0]
    width = stream_in.shape[1]
    taps_n = conv_taps.shape[1]
    local_cols = value_weight.shape[2]
    for layer in range(norm_gain.shape[0]):
        wide = stream.astype(F32)
        normed = (
            wide
            * lax.rsqrt(jnp.mean(wide * wide, axis=1, keepdims=True) + epsilon)
            * norm_gain[layer]
        ).astype(BF16)
        value = jnp.dot(normed, lax.all_gather(value_weight[layer], "sp", axis=0, tiled=True),
                        preferred_element_type=F32)
        gate = jnp.dot(normed, lax.all_gather(gate_weight[layer], "sp", axis=0, tiled=True),
                       preferred_element_type=F32)
        gated = (value * jax.nn.sigmoid(gate)).astype(BF16)
        earlier = passed_along(gated[tok_rows - (taps_n - 1):], "sp", 1)
        padded = jnp.concatenate([earlier, gated], axis=0).astype(F32)
        taps = conv_taps[layer]
        filtered = jnp.zeros((tok_rows, local_cols), F32)
        for tap in range(taps_n):
            filtered = filtered + taps[tap] * padded[tap:tap + tok_rows]
        sum_first, sum_second = lax.psum(
            (jnp.sum(filtered, axis=1), jnp.sum(filtered * filtered, axis=1)), "tp")
        mean_value = (sum_first / width)[:, None]
        variance = (sum_second / width)[:, None] - mean_value * mean_value
        activated = jax.nn.silu(
            (filtered - mean_value) * lax.rsqrt(variance + epsilon) * channel_gain[layer]
        ).astype(BF16)
        whole_out = lax.all_gather(out_weight[layer], "sp", axis=1, tiled=True)
        terms = jnp.dot(activated, whole_out, preferred_element_type=F32)
        summed = lax.psum(terms.astype(BF16), "tp").astype(F32)
        stream = (wide + summed).astype(BF16)
    return stream


def solution(mesh):
    n, tp = mesh.shape["sp"], mesh.shape["tp"]

    def body(stream_in, norm_gain, value_weight, *rest):
        rows, cols = value_weight.shape[1], value_weight.shape[2]
        quads = tp == 2 and n % 4 == 0 and n >= 8 and rows % 128 == 0 and cols % 512 == 0
        fits = stream_in.shape[0] % 64 == 0 and rest[1].shape[1] <= PAD
        chosen = fused(n, norm_gain.shape[0]) if quads and fits else general
        return chosen(stream_in, norm_gain, value_weight, *rest)

    return jax.shard_map(
        body,
        mesh=mesh,
        in_specs=(
            P("sp", None),
            P(),
            P(None, "sp", "tp"),
            P(None, "sp", "tp"),
            P(None, None, "tp"),
            P(None, "tp"),
            P(None, "tp", "sp"),
        ),
        out_specs=P("sp", None),
        check_vma=False,
    )
```

```python
import functools

import jax
import jax.numpy as jnp
from jax import lax
from jax.experimental import pallas as pl
from jax.experimental.pallas import tpu as pltpu
from jax.sharding import PartitionSpec as P

epsilon = 1e-05
MESH = pl.DeviceIdType.MESH
F32 = jnp.float32
BF16 = jnp.bfloat16
PAD = 32
PARTS = 2
EARLY = ((1, 0), (2, 0), (1, 1), (2, 1), (3, 0), (3, 1))


def kernel(n, layers, taps_n, stream_hbm, gain_hbm, vw, gw, taps_hbm, cgain_hbm, ow, out,
           stream_in, gain, taps, cgain, wvg, wo, nrm, gat, fil, act, ssend, srecv, dsend, drecv,
           asend, arecv, bsend, brecv, mine, through, strm, acc, turn,
           squares, qsend, qrecv, edge_out, edge_in,
           in_sem, out_sem, loc_sem, wx_send, wx_recv, z_send, z_recv, halo_send, halo_recv,
           msg_send, msg_recv):
    planes = n // 4
    s = lax.axis_index("sp")
    c = lax.axis_index("tp")
    z, q = s // 4, s % 4
    y, x = q // 2, q % 2
    quad = [q, q + 1 - 2 * x, q + 2 - 4 * y, 3 - q]
    toks, width = stream_in.shape
    group = 4 * toks
    rows, cols = vw.shape[1], vw.shape[2]
    ch = cols // 4
    half = width // 2
    chunk = 2 * rows
    near = (1 - c) * quad[1] + c * quad[2]
    far = c * quad[1] + (1 - c) * quad[2]
    diag = quad[3]
    near_dev, far_dev, core_dev = (z * 4 + near, c), (z * 4 + far, c), (s, 1 - c)
    up_dev, down_dev = (s + 4, c), (s - 4, c)

    def al(v, m):
        return pl.multiple_of(v, m)

    barrier = pltpu.get_barrier_semaphore()
    plane_devs = [(z * 4 + quad[k], cc) for k in range(4) for cc in (c, 1 - c)][1:]
    for dev in plane_devs:
        pl.semaphore_signal(barrier, inc=1, device_id=dev, device_id_type=MESH)

    @pl.when(z < planes - 1)
    def _():
        pl.semaphore_signal(barrier, inc=1, device_id=up_dev, device_id_type=MESH)

    @pl.when(z > 0)
    def _():
        pl.semaphore_signal(barrier, inc=1, device_id=down_dev, device_id_type=MESH)

    own_ch = pl.ds(al(q * ch, ch), ch)
    loads = [pltpu.make_async_copy(a, b, in_sem.at[k]) for k, (a, b) in enumerate((
        (stream_hbm, stream_in), (gain_hbm, gain), (taps_hbm.at[:, :, own_ch], taps),
        (cgain_hbm.at[:, own_ch], cgain)))]
    for load in loads:
        load.start()

    shared = {}

    def shared_copy(l, kind, k):
        mine_rows = pl.ds(al(s * rows, rows), rows)
        span = pl.ds(al(quad[k] * ch, ch), ch)
        if kind == 2:
            src, dst = ow.at[l, span, :], wo.at[l, :, mine_rows]
        else:
            src = (vw, gw)[kind].at[l, :, span]
            dst = wvg.at[l, mine_rows, pl.ds(kind * ch, ch)]
        idx = l * 3 + kind
        if k == 0:
            copy = pltpu.make_async_copy(src, dst, loc_sem.at[idx])
        else:
            copy = pltpu.make_async_remote_copy(
                src, dst, wx_send.at[0], wx_recv.at[idx, k - 1],
                device_id=(z * 4 + quad[k], c), device_id_type=MESH)
        copy.start()
        shared[l, kind, k] = copy

    def share(l, kinds, ks=(1, 2, 3)):
        for k in ks:
            for kind in kinds:
                shared_copy(l, kind, k)

    for l in range(layers):
        share(l, (0, 1, 2), (0,))

    pl.semaphore_wait(barrier, len(plane_devs) + (z < planes - 1).astype(jnp.int32)
                      + (z > 0).astype(jnp.int32))

    def z_copy(l, grp, d, t, hop, first, count, pair, kind=None):
        plane = z - t if d == 0 else z + t
        block = pl.ds(al((plane * 4 + first) * rows, rows), count * rows)
        ref = wvg.at[l, block, :] if grp == 0 else wo.at[l, :, block]
        if kind is not None:
            ref = wvg.at[l, block, kind * ch:(kind + 1) * ch]
        idx = (l * 2 + grp) * 2 + d
        return pltpu.make_async_remote_copy(
            ref, ref, z_send.at[idx, hop], z_recv.at[idx, hop, pair],
            device_id=up_dev if d == 0 else down_dev, device_id_type=MESH)

    def z_pair(l, grp, d, t, hop, pair):
        return z_copy(l, grp, d, t, hop, 2 * (y + pair - 2 * y * pair), 2, pair)

    def holds(d, t):
        return z >= t if d == 0 else z + t < planes

    def sends(d):
        return z < planes - 1 if d == 0 else z > 0

    def pump_early():
        for k, kind in EARLY:
            shared[0, kind, k].wait_recv()
            for d in range(2):
                @pl.when(sends(d))
                def _(k=k, d=d, kind=kind):
                    z_copy(0, 0, d, 0, 0, quad[k], 1, k // 2, kind).start()

    def pump(l, grp, t, ks=(0, 1, 2, 3), pairs=(0, 1)):
        if t == 0:
            for k in ks:
                for kind in ((0, 1) if grp == 0 else (2,)):
                    if k:
                        shared[l, kind, k].wait_recv()
                    else:
                        shared[l, kind, k].wait()
                if l == 0:
                    for d in range(2):
                        @pl.when(sends(d))
                        def _(k=k, d=d):
                            z_copy(l, grp, d, 0, 0, quad[k], 1, k // 2).start()
        if t > 0 or l > 0:
            for pair in pairs:
                for d in range(2):
                    @pl.when(holds(d, t) & sends(d))
                    def _(pair=pair, d=d):
                        if t > 0:
                            z_pair(l, grp, d, t, t - 1, pair).wait_recv()
                        z_pair(l, grp, d, t, t, pair).start()

    def consume_one(l, grp, t, d):
        @pl.when(jnp.logical_not(sends(d)))
        def _():
            for pair in range(2):
                z_pair(l, grp, d, t, t - 1, pair).wait_recv()

    def consume(l, grp, t):
        for d in range(2):
            @pl.when(holds(d, t))
            def _(d=d):
                consume_one(l, grp, t, d)

    def drain(l, grp):
        for t in range(planes - 1):
            for d in range(2):
                @pl.when(holds(d, t) & sends(d))
                def _(t=t, d=d):
                    z_copy(l, grp, d, t, t, 0, 4, 0).wait_send()

    turn[...] = jnp.zeros_like(turn)
    slots, kinds_sent = {}, {}

    def message(name, src, dst, dev, sender):
        slot = slots.setdefault(name, len(slots))
        kind = kinds_sent.setdefault(sender, len(kinds_sent))
        m = pltpu.make_async_remote_copy(src, dst, msg_send.at[kind], msg_recv.at[slot],
                                         device_id=dev, device_id_type=MESH)
        m.start()
        return m

    def all_came(name, ref):
        pltpu.make_async_remote_copy(ref, ref, msg_send.at[0], msg_recv.at[slots[name]],
                                     device_id=core_dev, device_id_type=MESH).wait_recv()

    def all_sent(sender, ref):
        pltpu.make_async_remote_copy(ref, ref, msg_send.at[kinds_sent[sender]], msg_recv.at[0],
                                     device_id=core_dev, device_id_type=MESH).wait_send()

    for k, kind in EARLY:
        shared_copy(0, kind, k)

    def block_rows(b):
        return pl.ds(al(b * toks, toks), toks)

    def half_cols(h):
        return pl.ds(al(h * half, half), half)

    unit = toks // 2
    total_rows = PAD + group
    tile = max(v for v in range(16, 401, 16) if total_rows % v == 0)
    bounds = (0, 3 * toks, group)
    lanes = 128

    def plane_at(u):
        low = jnp.where(u <= z, z - u, u)
        zm = planes - 1 - z
        high = planes - 1 - jnp.where(u <= zm, zm - u, u)
        return jnp.where(2 * z < planes, low, high)

    def norm_step(r, _):
        at = al(r * 64, 64)
        wide = stream_in[pl.ds(at, 64), :].astype(F32)
        scale = lax.rsqrt(jnp.mean(wide * wide, axis=1, keepdims=True) + epsilon)
        nrm[0, pl.ds(al(PAD + q * toks + at, 32), 64), :] = (
            wide * scale * gain[0:1, :]).astype(BF16)
        return 0

    class Halo:
        def __init__(self, l, border, first):
            def copy(k, dev, src, recv):
                return pltpu.make_async_remote_copy(
                    src, first, halo_send.at[l, k], halo_recv.at[l, recv],
                    device_id=dev, device_id_type=MESH)

            self.up = copy(0, up_dev, border, 0)
            self.side = [copy(k, (z * 4 + quad[k], c), first, 1) for k in (1, 2, 3)]
            self.core = copy(4, core_dev, first, 2)

        def rise(self):
            @pl.when((q == 3) & (z < planes - 1))
            def _():
                self.up.start()

        def spread(self):
            @pl.when((q == 3) & (z > 0))
            def _():
                self.up.wait_recv()
                for m in self.side:
                    m.start()
                self.core.start()

        def swap(self):
            @pl.when((q != 3) & (z > 0))
            def _():
                self.side[0].wait_recv()
                self.core.start()

        def finish(self):
            @pl.when(z > 0)
            def _():
                self.core.wait()

            @pl.when((q == 3) & (z > 0))
            def _():
                for m in self.side:
                    m.wait_send()

            @pl.when((q == 3) & (z < planes - 1))
            def _():
                self.up.wait_send()

    def spot(b, j):
        return nrm.at[0, pl.ds(al(PAD + b * toks + j * unit, 32), unit), half_cols(c)]

    def to_far(j):
        own_near[j].wait_send()
        own_far.append(message(("g_far", j), spot(q, j), spot(q, j), far_dev, "ag"))

    def pass_on(j):
        own_near[j].wait_recv()
        passed.append(message(("g_pass", j), spot(near, j), spot(near, j), far_dev, "ag"))
        relays[1, j] = message(("c", 0), spot(near, j), spot(near, j), core_dev, "ag")

    def relay(which, j):
        (own_far if which == 2 else passed)[j].wait_recv()
        b = far if which == 2 else diag
        relays[which, j] = message(("c", 0), spot(b, j), spot(b, j), core_dev, "ag")

    def gate_part(l, t, plane, start, count, size):
        depth = pl.ds(al(plane * 4 * rows, 4 * rows), 4 * rows)

        def gate_step(r, _):
            at = pl.ds(al(start + r * size, 16), size)
            term = jnp.dot(nrm[l, at, depth], wvg[l, depth, :], preferred_element_type=F32)
            acc[at, :] = term if t == 0 else acc[at, :] + term
            return 0

        lax.fori_loop(0, count // size, gate_step, 0)

    for l in range(layers):
        last_layer = l + 1 == layers
        source = stream_in if l == 0 else strm.at[l - 1]

        if l == 0:
            pump(0, 0, 0, (0,))
            pump(0, 1, 0, (0,))
            for load in loads:
                load.wait()
            lax.fori_loop(0, toks // 64, norm_step, 0)

            @pl.when(z == 0)
            def _():
                for ll in range(layers):
                    nrm[ll, 0:PAD, :] = jnp.zeros((PAD, width), BF16)

            edge = Halo(0, nrm.at[0, pl.ds(group, PAD), half_cols(c)],
                        nrm.at[0, pl.ds(0, PAD), half_cols(c)])
            edge.rise()
            own_near = [message(("g_near", j), spot(q, j), spot(q, j), near_dev, ("near", j)) for j in range(2)]
            passed, relays, own_far = [], {}, []
            pump_early()
            edge.spread()
            to_far(0)
            to_far(1)
            pump(0, 0, 1)
            pass_on(0)
            pass_on(1)
            share(0, (2,))
            relay(2, 0)
            relay(2, 1)
            for t in range(2, planes - 1):
                pump(0, 0, t)
            relay(3, 0)
            relay(3, 1)
            for ll in range(1, layers):
                share(ll, (0, 1, 2))
            pump(0, 1, 0, (1, 2, 3))
            edge.swap()
            all_came(("c", 0), nrm.at[0, PAD:PAD + 3 * toks, 0:half])
            edge.finish()
            gate_part(0, 0, z, 0, total_rows, tile)
            for t in range(1, planes):
                for d in range(2):
                    @pl.when(holds(d, t))
                    def _(t=t, d=d):
                        consume_one(0, 0, t, d)
                        gate_part(0, t, z - t if d == 0 else z + t, 0, total_rows, tile)

            def gate_end(r, _):
                at = pl.ds(al(r * tile, 16), tile)
                gated = (acc[at, :ch] * jax.nn.sigmoid(acc[at, ch:])).astype(BF16)
                gat[at, :] = gated.astype(F32)
                return 0

            lax.fori_loop(0, total_rows // tile, gate_end, 0)
            pump(0, 1, 1)

        lead = PAD - (taps_n - 1)
        step_rows = 128

        def conv_step(r, _):
            at = al(r * step_rows, step_rows)
            for lane in range(ch // lanes):
                cut = slice(lane * lanes, (lane + 1) * lanes)
                total = [None, None]
                block = gat[pl.ds(at, step_rows + PAD), cut]
                for b in range(8):
                    moved = block if b == 0 else pltpu.roll(block, step_rows + PAD - b, 0)
                    for a in range(PAD // 8 + 1):
                        tap = 8 * a + b - lead
                        if 0 <= tap < taps_n:
                            term = taps[tap, l:l + 1, cut] * moved[8 * a:8 * a + step_rows]
                            total[a % 2] = term if total[a % 2] is None else total[a % 2] + term
                fil[pl.ds(at, step_rows), cut] = total[0] + total[1]
            return 0

        sums = []
        for part in range(PARTS):
            low, high = bounds[part:part + 2]
            lax.fori_loop(low // step_rows, high // step_rows, conv_step, 0)
            wide = fil[low:high, :]
            first_sum = jnp.sum(wide, axis=1, keepdims=True)
            second_sum = jnp.sum(wide * wide, axis=1, keepdims=True)
            lane_id = lax.broadcasted_iota(jnp.int32, (high - low, lanes), 1)
            stat = jnp.where(lane_id == 0, first_sum, jnp.where(lane_id == 1, second_sum, 0.0))
            ssend[l, :, low:high] = jnp.transpose(stat)[0:2, :]
            sums.append([message(("sum", part), ssend.at[l, :, low:high], srecv.at[l, k, :, low:high],
                                 dev, "sum") for k, dev in enumerate(plane_devs)])
        for t in range(2, planes - 1):
            pump(l, 1, t)
        if not last_layer:
            pump(l + 1, 0, 0)
        for part in range(PARTS):
            low, high = bounds[part:part + 2]
            all_came(("sum", part), srecv.at[l, :, :, low:high])
            whole = ssend[l, :, low:high]
            for k in range(len(plane_devs)):
                whole = whole + srecv[l, k, :, low:high]
            turn[0:2, low:high] = whole
            stat = jnp.transpose(turn[:, low:high])
            mean_value = stat[:, 0:1] / width
            variance = stat[:, 1:2] / width - mean_value * mean_value
            act[low:high, :] = jax.nn.silu((fil[low:high, :] - mean_value) * lax.rsqrt(variance + epsilon)
                                           * cgain[l:l + 1, :]).astype(BF16)

        def out_cols(h, u):
            return pl.ds(al(plane_at(u) * 4 * rows + h * chunk, chunk), chunk)

        def stage_swap(u):
            if u > 0:
                consume(l, 1, u)
            weights = wo[l, :, out_cols(1 - c, u)]
            for m, pair in enumerate(((near, diag), (far, q))):
                for k, b in enumerate(pair):
                    dsend[l, u, m, k] = jnp.dot(act[block_rows(b), :], weights,
                                                preferred_element_type=F32).astype(BF16)
                swaps[u, m] = message(("swap", u, m), dsend.at[l, u, m], drecv.at[l, u, m], core_dev, "swap")

        def stage_first(u):
            weights = wo[l, :, out_cols(c, u)]

            def partial(b, m, k):
                return (jnp.dot(act[block_rows(b), :], weights, preferred_element_type=F32)
                        + drecv[l, u, m, k].astype(F32))

            swaps[u, 0].wait_recv()
            for k, b in enumerate((far, diag)):
                term = partial(b, 0, k).astype(BF16)
                for j in range(2):
                    asend[l, u, j, k] = term[j * unit:(j + 1) * unit]
            for j in range(2):
                firsts[u, j] = message(("first", u, j), asend.at[l, u, j], arecv.at[l, u, j], far_dev, "first")
            swaps[u, 1].wait_recv()
            through[u] = partial(near, 1, 0)
            mine[u] = partial(q, 1, 1) + source[:, out_cols(c, u)].astype(F32)

        def stage_take(u, j):
            span = slice(j * unit, (j + 1) * unit)
            firsts[u, j].wait_recv()
            bsend[l, u, j] = (through[u, span] + arecv[l, u, j, 1].astype(F32)).astype(BF16)
            mine[u, span] = mine[u, span] + arecv[l, u, j, 0].astype(F32)

        def stage_give(u, j):
            seconds[u, j] = message(("second", u, j), bsend.at[l, u, j], brecv.at[l, u, j], near_dev,
                                    "second")

        def stage_last(u, j):
            span = slice(j * unit, (j + 1) * unit)
            seconds[u, j].wait_recv()
            final = (mine[u, span] + brecv[l, u, j].astype(F32)).astype(BF16)
            strm[l, span, out_cols(c, u)] = final
            if last_layer:
                piece, place = strm.at[l, span, out_cols(c, u)], out.at[span, out_cols(c, u)]
                message(("c", 0), piece, place, core_dev, "last")
                pltpu.make_async_copy(piece, place, out_sem.at[0]).start()
            else:
                wide = final.astype(F32)
                nrm[l + 1, pl.ds(al(PAD + q * toks + j * unit, 32), unit), out_cols(c, u)] = (
                    wide * gain[l + 1:l + 2, out_cols(c, u)]).astype(BF16)
                square = wide * wide
                folded = sum(square[:, k * lanes:(k + 1) * lanes] for k in range(chunk // lanes))
                squares[span, :] = folded if u == 0 else squares[span, :] + folded

        def lot(b, u):
            return nrm.at[l + 1, pl.ds(al(PAD + b * toks, 32), toks), out_cols(c, u)]

        def pass_chunk(kind, u, b, dev):
            moves[kind, u] = message((kind if kind[0] == "g" else "c", u), lot(b, u), lot(b, u), dev, kind[0])

        def gather(u):
            pass_chunk("g_near", u, q, near_dev)
            pass_chunk("c_own", u, q, core_dev)

        def forward(u):
            moves["g_near", u].wait_recv()
            pass_chunk("g_far", u, q, far_dev)
            pass_chunk("g_pass", u, near, far_dev)
            pass_chunk("c_near", u, near, core_dev)

        def cross_far(u):
            moves["g_far", u].wait_recv()
            pass_chunk("c_far", u, far, core_dev)

        def cross_diag(u):
            moves["g_pass", u].wait_recv()
            pass_chunk("c_diag", u, diag, core_dev)

        def gate_chunk(u):
            if u > 0:
                consume(l + 1, 0, u)
            all_came(("c", u), nrm.at[l + 1, PAD:PAD + group, 0:chunk])
            gate_part(l + 1, u, plane_at(u), PAD, group, toks)

        def send_squares():
            lane_id = lax.broadcasted_iota(jnp.int32, (toks, lanes), 1)
            total = jnp.sum(squares[...], axis=1, keepdims=True)
            qsend[l] = jnp.transpose(jnp.where(lane_id == 0, total, 0.0))[0:2, :]
            return [message(("square", k > 0), qsend.at[l], qrecv.at[l, k], dev, "square")
                    for k, dev in enumerate(plane_devs)]

        def row_scale(whole):
            turn[0:2, 0:toks] = whole
            return lax.rsqrt(jnp.transpose(turn[:, 0:toks])[:, 0:1] / width + epsilon)

        def send_edge(edge):
            norms[0].wait_recv()
            scale = row_scale(qsend[l] + qrecv[l, 0])[toks - PAD:]
            for u in range(planes):
                edge_out[l, :, pl.ds(al(plane_at(u) * chunk, chunk), chunk)] = (
                    strm[l, toks - PAD:, out_cols(c, u)].astype(F32) * scale
                    * gain[l + 1:l + 2, out_cols(c, u)]).astype(BF16)
            edge.rise()

        def gate_final(edge):
            u = planes - 1
            consume(l + 1, 0, u)
            edge.finish()

            @pl.when(z > 0)
            def _():
                for p in range(planes):
                    for h in range(2):
                        at = p * 4 * rows + h * chunk
                        nrm[l + 1, 0:PAD, at:at + chunk] = edge_in[l, h, :, p * chunk:(p + 1) * chunk]

            both = jnp.dot(nrm[l + 1, 0:PAD, :], wvg[l + 1], preferred_element_type=F32)
            gat[0:PAD, :] = (both[:, :ch] * jax.nn.sigmoid(both[:, ch:])).astype(BF16).astype(F32)
            all_came(("square", True), qrecv.at[l, 1:])
            all_came(("c", u), nrm.at[l + 1, PAD:PAD + group, 0:chunk])
            depth = pl.ds(al(plane_at(u) * 4 * rows, 4 * rows), 4 * rows)
            for k in range(4):
                mate = qsend[l] if k == 0 else qrecv[l, 2 * k - 1]
                scale = row_scale(mate + qrecv[l, 2 * k])
                at = pl.ds(al(PAD + quad[k] * toks, 32), toks)
                both = acc[at, :] + jnp.dot(nrm[l + 1, at, depth], wvg[l + 1, depth, :],
                                            preferred_element_type=F32)
                value, gate = both[:, :ch] * scale, both[:, ch:] * scale
                gat[at, :] = (value * jax.nn.sigmoid(gate)).astype(BF16).astype(F32)

        swaps, firsts, seconds, lasts, moves = {}, {}, {}, {}, {}
        for u in range(planes - 1):
            stage_swap(u)
            if u > 0:
                stage_first(u - 1)
        stage_first(planes - 2)
        stage_swap(planes - 1)
        stage_first(planes - 1)
        if last_layer:
            drain(l, 0)
            drain(l, 1)
            pltpu.make_async_remote_copy(
                wvg.at[:, 0:9 * rows // 2, :], wvg.at[:, 0:9 * rows // 2, :], wx_send.at[0],
                wx_recv.at[0, 0], device_id=core_dev, device_id_type=MESH).wait_send()
            all_sent("ag", nrm.at[0, PAD:PAD + 5 * toks // 2, :])
            all_sent("sum", srecv)
            if layers > 1:
                all_sent("square", qrecv.at[0:layers - 1])
                all_sent("g", nrm.at[1:layers, PAD:PAD + 3 * toks, 0:half])
                all_sent("c", nrm.at[1:layers, PAD:PAD + group, 0:half])
        for u in range(planes - 1):
            for j in range(2):
                stage_take(u, j)
            if u + 2 == planes:
                for uu in range(planes - 1):
                    for j in range(2):
                        stage_give(uu, j)
        for j in range(2):
            stage_take(planes - 1, j)
            stage_give(planes - 1, j)
        if not last_layer:
            pump(l + 1, 0, 1)
        for u in range(planes):
            for j in range(2):
                stage_last(u, j)
            if not last_layer:
                gather(u)
                if u >= 2:
                    forward(u - 2)
        if not last_layer:
            edge = Halo(l + 1, edge_out.at[l], edge_in.at[l, c])
            norms = send_squares()
            cross_far(0)
            send_edge(edge)
            ahead = planes - 2
            for u in range(ahead, planes + ahead):
                if u < planes:
                    forward(u)
                    cross_far(u - ahead + 1)
                elif u - ahead + 1 < planes:
                    cross_far(u - ahead + 1)
                cross_diag(u - ahead)
                if u == ahead:
                    for t in range(2, planes - 1):
                        pump(l + 1, 0, t)
                if u == ahead + 1:
                    edge.spread()
                    pump(l + 1, 1, 0)
                if u - ahead < planes - 1:
                    gate_chunk(u - ahead)
                if u == ahead + 2:
                    drain(l, 0)
                    drain(l, 1)
            edge.swap()
            gate_final(edge)
            pump(l + 1, 1, 1)

    all_sent("swap", dsend)
    all_sent("first", asend)
    all_sent("second", bsend)
    all_sent("last", strm.at[layers - 1, :, 0:half])
    whole_half = strm.at[layers - 1, :, 0:half]
    pltpu.make_async_copy(whole_half, out.at[:, 0:half], out_sem.at[0]).wait()
    all_came(("c", 0), whole_half)


def fused(n, layers):
    def body(stream_in, norm_gain, value_weight, gate_weight, conv_taps, channel_gain, out_weight):
        toks, width = stream_in.shape
        taps_n = conv_taps.shape[1]
        rows, cols = value_weight.shape[1], value_weight.shape[2]
        ch, half, group, planes = cols // 4, width // 2, 4 * toks, n // 4
        chunk = 2 * rows
        taps = jnp.transpose(conv_taps, (1, 0, 2))
        hbm = pl.BlockSpec(memory_space=pltpu.HBM)
        msgs = 2 + PARTS + 10 * planes
        return pl.pallas_call(
            functools.partial(kernel, n, layers, taps_n),
            out_shape=jax.ShapeDtypeStruct((toks, width), BF16),
            in_specs=[hbm] * 7,
            out_specs=hbm,
            scratch_shapes=[
                pltpu.VMEM((toks, width), BF16),
                pltpu.VMEM((layers, width), F32),
                pltpu.VMEM((taps_n, layers, ch), F32),
                pltpu.VMEM((layers, ch), F32),
                pltpu.VMEM((layers, width, 2 * ch), BF16),
                pltpu.VMEM((layers, ch, width), BF16),
                pltpu.VMEM((layers, PAD + group, width), BF16),
                pltpu.VMEM((PAD + group, ch), F32),
                pltpu.VMEM((group, ch), F32),
                pltpu.VMEM((group, ch), BF16),
                pltpu.VMEM((layers, 2, group), F32),
                pltpu.VMEM((layers, 7, 2, group), F32),
                pltpu.VMEM((layers, planes, 2, 2, toks, chunk), BF16),
                pltpu.VMEM((layers, planes, 2, 2, toks, chunk), BF16),
                pltpu.VMEM((layers, planes, 2, 2, toks // 2, chunk), BF16),
                pltpu.VMEM((layers, planes, 2, 2, toks // 2, chunk), BF16),
                pltpu.VMEM((layers, planes, 2, toks // 2, chunk), BF16),
                pltpu.VMEM((layers, planes, 2, toks // 2, chunk), BF16),
                pltpu.VMEM((planes, toks, chunk), F32),
                pltpu.VMEM((planes, toks, chunk), F32),
                pltpu.VMEM((layers, toks, width), BF16),
                pltpu.VMEM((PAD + group, 2 * ch), F32),
                pltpu.VMEM((128, group), F32),
                pltpu.VMEM((toks, 128), F32),
                pltpu.VMEM((layers, 2, toks), F32),
                pltpu.VMEM((layers, 7, 2, toks), F32),
                pltpu.VMEM((layers, PAD, half), BF16),
                pltpu.VMEM((layers, 2, PAD, half), BF16),
                pltpu.SemaphoreType.DMA((4,)),
                pltpu.SemaphoreType.DMA((1,)),
                pltpu.SemaphoreType.DMA((layers * 3,)),
                pltpu.SemaphoreType.DMA((1,)),
                pltpu.SemaphoreType.DMA((layers * 3, 3)),
                pltpu.SemaphoreType.DMA((layers * 4, planes - 1)),
                pltpu.SemaphoreType.DMA((layers * 4, planes - 1, 2)),
                pltpu.SemaphoreType.DMA((layers, 5)),
                pltpu.SemaphoreType.DMA((layers, 3)),
                pltpu.SemaphoreType.DMA((11,)),
                pltpu.SemaphoreType.DMA((msgs,)),
            ],
            compiler_params=pltpu.CompilerParams(
                collective_id=0, has_side_effects=True, vmem_limit_bytes=62 * 2**20),
        )(stream_in, norm_gain, value_weight, gate_weight, taps, channel_gain, out_weight)

    return body


def passed_along(value, axis, steps):
    count = lax.axis_size(axis)
    leading, last = (max(0, -steps), min(count, count - steps))
    return lax.ppermute(value, axis, [(source, source + steps) for source in range(leading, last)])


def general(stream_in, norm_gain, value_weight, gate_weight, conv_taps, channel_gain, out_weight):
    stream = stream_in
    tok_rows = stream_in.shape[0]
    width = stream_in.shape[1]
    taps_n = conv_taps.shape[1]
    local_cols = value_weight.shape[2]
    for layer in range(norm_gain.shape[0]):
        wide = stream.astype(F32)
        normed = (
            wide
            * lax.rsqrt(jnp.mean(wide * wide, axis=1, keepdims=True) + epsilon)
            * norm_gain[layer]
        ).astype(BF16)
        value = jnp.dot(normed, lax.all_gather(value_weight[layer], "sp", axis=0, tiled=True),
                        preferred_element_type=F32)
        gate = jnp.dot(normed, lax.all_gather(gate_weight[layer], "sp", axis=0, tiled=True),
                       preferred_element_type=F32)
        gated = (value * jax.nn.sigmoid(gate)).astype(BF16)
        earlier = passed_along(gated[tok_rows - (taps_n - 1):], "sp", 1)
        padded = jnp.concatenate([earlier, gated], axis=0).astype(F32)
        taps = conv_taps[layer]
        filtered = jnp.zeros((tok_rows, local_cols), F32)
        for tap in range(taps_n):
            filtered = filtered + taps[tap] * padded[tap:tap + tok_rows]
        sum_first, sum_second = lax.psum(
            (jnp.sum(filtered, axis=1), jnp.sum(filtered * filtered, axis=1)), "tp")
        mean_value = (sum_first / width)[:, None]
        variance = (sum_second / width)[:, None] - mean_value * mean_value
        activated = jax.nn.silu(
            (filtered - mean_value) * lax.rsqrt(variance + epsilon) * channel_gain[layer]
        ).astype(BF16)
        whole_out = lax.all_gather(out_weight[layer], "sp", axis=1, tiled=True)
        terms = jnp.dot(activated, whole_out, preferred_element_type=F32)
        summed = lax.psum(terms.astype(BF16), "tp").astype(F32)
        stream = (wide + summed).astype(BF16)
    return stream


def solution(mesh):
    n, tp = mesh.shape["sp"], mesh.shape["tp"]

    def body(stream_in, norm_gain, value_weight, *rest):
        rows, cols = value_weight.shape[1], value_weight.shape[2]
        quads = tp == 2 and n % 4 == 0 and n >= 8 and rows % 128 == 0 and cols % 512 == 0
        fits = stream_in.shape[0] % 64 == 0 and rest[1].shape[1] <= PAD
        chosen = fused(n, norm_gain.shape[0]) if quads and fits else general
        return chosen(stream_in, norm_gain, value_weight, *rest)

    return jax.shard_map(
        body,
        mesh=mesh,
        in_specs=(
            P("sp", None),
            P(),
            P(None, "sp", "tp"),
            P(None, "sp", "tp"),
            P(None, None, "tp"),
            P(None, "tp"),
            P(None, "tp", "sp"),
        ),
        out_specs=P("sp", None),
        check_vma=False,
    )
```

```python
import functools

import jax
import jax.numpy as jnp
from jax import lax
from jax.experimental import pallas as pl
from jax.experimental.pallas import tpu as pltpu
from jax.sharding import PartitionSpec as P

epsilon = 1e-05
MESH = pl.DeviceIdType.MESH
F32 = jnp.float32
BF16 = jnp.bfloat16
PAD = 32
PARTS = 2
EARLY = ((1, 0), (2, 0), (1, 1), (2, 1), (3, 0), (3, 1))


def kernel(n, layers, taps_n, stream_hbm, gain_hbm, vw, gw, taps_hbm, cgain_hbm, ow, out,
           stream_in, gain, taps, cgain, wvg, wo, nrm, gat, fil, act, ssend, srecv, dsend, drecv,
           asend, arecv, bsend, brecv, mine, through, strm, acc, turn,
           squares, qsend, qrecv, edge_out, edge_in,
           in_sem, out_sem, loc_sem, wx_send, wx_recv, z_send, z_recv, halo_send, halo_recv,
           msg_send, msg_recv):
    planes = n // 4
    s = lax.axis_index("sp")
    c = lax.axis_index("tp")
    z, q = s // 4, s % 4
    y, x = q // 2, q % 2
    quad = [q, q + 1 - 2 * x, q + 2 - 4 * y, 3 - q]
    toks, width = stream_in.shape
    group = 4 * toks
    rows, cols = vw.shape[1], vw.shape[2]
    ch = cols // 4
    half = width // 2
    chunk = 2 * rows
    near = (1 - c) * quad[1] + c * quad[2]
    far = c * quad[1] + (1 - c) * quad[2]
    diag = quad[3]
    near_dev, far_dev, core_dev = (z * 4 + near, c), (z * 4 + far, c), (s, 1 - c)
    up_dev, down_dev = (s + 4, c), (s - 4, c)

    def al(v, m):
        return pl.multiple_of(v, m)

    barrier = pltpu.get_barrier_semaphore()
    plane_devs = [(z * 4 + quad[k], cc) for k in range(4) for cc in (c, 1 - c)][1:]
    for dev in plane_devs:
        pl.semaphore_signal(barrier, inc=1, device_id=dev, device_id_type=MESH)

    @pl.when(z < planes - 1)
    def _():
        pl.semaphore_signal(barrier, inc=1, device_id=up_dev, device_id_type=MESH)

    @pl.when(z > 0)
    def _():
        pl.semaphore_signal(barrier, inc=1, device_id=down_dev, device_id_type=MESH)

    own_ch = pl.ds(al(q * ch, ch), ch)
    loads = [pltpu.make_async_copy(a, b, in_sem.at[k]) for k, (a, b) in enumerate((
        (stream_hbm, stream_in), (gain_hbm, gain), (taps_hbm.at[:, :, own_ch], taps),
        (cgain_hbm.at[:, own_ch], cgain)))]
    for load in loads:
        load.start()

    shared = {}

    def shared_copy(l, kind, k):
        mine_rows = pl.ds(al(s * rows, rows), rows)
        span = pl.ds(al(quad[k] * ch, ch), ch)
        if kind == 2:
            src, dst = ow.at[l, span, :], wo.at[l, :, mine_rows]
        else:
            src = (vw, gw)[kind].at[l, :, span]
            dst = wvg.at[l, mine_rows, pl.ds(kind * ch, ch)]
        idx = l * 3 + kind
        if k == 0:
            copy = pltpu.make_async_copy(src, dst, loc_sem.at[idx])
        else:
            copy = pltpu.make_async_remote_copy(
                src, dst, wx_send.at[0],
                wx_recv.at[idx * 3 + k - 1 if l == 0 else 7 + 2 * l + kind // 2],
                device_id=(z * 4 + quad[k], c), device_id_type=MESH)
        copy.start()
        shared[l, kind, k] = copy

    def share(l, kinds, ks=(1, 2, 3)):
        for k in ks:
            for kind in kinds:
                shared_copy(l, kind, k)

    for l in range(layers):
        share(l, (0, 1, 2), (0,))

    pl.semaphore_wait(barrier, len(plane_devs) + (z < planes - 1).astype(jnp.int32)
                      + (z > 0).astype(jnp.int32))

    def z_copy(l, grp, d, t, hop, first, count, pair, kind=None):
        plane = z - t if d == 0 else z + t
        block = pl.ds(al((plane * 4 + first) * rows, rows), count * rows)
        ref = wvg.at[l, block, :] if grp == 0 else wo.at[l, :, block]
        if kind is not None:
            ref = wvg.at[l, block, kind * ch:(kind + 1) * ch]
        idx = (l * 2 + grp) * 2 + d
        return pltpu.make_async_remote_copy(
            ref, ref, z_send.at[idx, hop], z_recv.at[idx, hop, pair],
            device_id=up_dev if d == 0 else down_dev, device_id_type=MESH)

    def z_pair(l, grp, d, t, hop, pair):
        return z_copy(l, grp, d, t, hop, 2 * (y + pair - 2 * y * pair), 2, pair)

    def holds(d, t):
        return z >= t if d == 0 else z + t < planes

    def sends(d):
        return z < planes - 1 if d == 0 else z > 0

    def pump_early():
        for k, kind in EARLY:
            shared[0, kind, k].wait_recv()
            for d in range(2):
                @pl.when(sends(d))
                def _(k=k, d=d, kind=kind):
                    z_copy(0, 0, d, 0, 0, quad[k], 1, k // 2, kind).start()

    def pump(l, grp, t, ks=(0, 1, 2, 3), pairs=(0, 1)):
        if t == 0:
            for k in ks:
                for kind in ((0, 1) if grp == 0 else (2,)):
                    if k == 0:
                        shared[l, kind, k].wait()
                    elif l == 0:
                        shared[l, kind, k].wait_recv()
                if l == 0:
                    for d in range(2):
                        @pl.when(sends(d))
                        def _(k=k, d=d):
                            z_copy(l, grp, d, 0, 0, quad[k], 1, k // 2).start()
        if t == 0 and l > 0:
            three = wvg.at[l, 0:3 * rows, :] if grp == 0 else wo.at[l, :, 0:3 * rows]
            pltpu.make_async_remote_copy(three, three, wx_send.at[0], wx_recv.at[7 + 2 * l + grp],
                                         device_id=core_dev, device_id_type=MESH).wait_recv()
        if t > 0 or l > 0:
            for pair in pairs:
                for d in range(2):
                    @pl.when(holds(d, t) & sends(d))
                    def _(pair=pair, d=d):
                        if t > 0:
                            z_pair(l, grp, d, t, t - 1, pair).wait_recv()
                        z_pair(l, grp, d, t, t, pair).start()

    def consume_one(l, grp, t, d):
        @pl.when(jnp.logical_not(sends(d)))
        def _():
            for pair in range(2):
                z_pair(l, grp, d, t, t - 1, pair).wait_recv()

    def consume(l, grp, t):
        for d in range(2):
            @pl.when(holds(d, t))
            def _(d=d):
                consume_one(l, grp, t, d)

    def drain(l, grp):
        for t in range(planes - 1):
            for d in range(2):
                @pl.when(holds(d, t) & sends(d))
                def _(t=t, d=d):
                    z_copy(l, grp, d, t, t, 0, 4, 0).wait_send()

    turn[...] = jnp.zeros_like(turn)
    slots, kinds_sent = {}, {}

    def message(name, src, dst, dev, sender):
        slot = slots.setdefault(name, len(slots))
        kind = kinds_sent.setdefault(sender, len(kinds_sent))
        m = pltpu.make_async_remote_copy(src, dst, msg_send.at[kind], msg_recv.at[slot],
                                         device_id=dev, device_id_type=MESH)
        m.start()
        return m

    def all_came(name, ref):
        pltpu.make_async_remote_copy(ref, ref, msg_send.at[0], msg_recv.at[slots[name]],
                                     device_id=core_dev, device_id_type=MESH).wait_recv()

    def all_sent(sender, ref):
        pltpu.make_async_remote_copy(ref, ref, msg_send.at[kinds_sent[sender]], msg_recv.at[0],
                                     device_id=core_dev, device_id_type=MESH).wait_send()

    for k, kind in EARLY:
        shared_copy(0, kind, k)

    def block_rows(b):
        return pl.ds(al(b * toks, toks), toks)

    def half_cols(h):
        return pl.ds(al(h * half, half), half)

    unit = toks // 2
    total_rows = PAD + group
    tile = max(v for v in range(16, 401, 16) if total_rows % v == 0)
    bounds = (0, 3 * toks, group)
    lanes = 128

    def plane_at(u):
        low = jnp.where(u <= z, z - u, u)
        zm = planes - 1 - z
        high = planes - 1 - jnp.where(u <= zm, zm - u, u)
        return jnp.where(2 * z < planes, low, high)

    def norm_step(r, _):
        at = al(r * 64, 64)
        wide = stream_in[pl.ds(at, 64), :].astype(F32)
        scale = lax.rsqrt(jnp.mean(wide * wide, axis=1, keepdims=True) + epsilon)
        nrm[0, pl.ds(al(PAD + q * toks + at, 32), 64), :] = (
            wide * scale * gain[0:1, :]).astype(BF16)
        return 0

    class Halo:
        def __init__(self, l, border, first):
            def copy(k, dev, src, recv):
                return pltpu.make_async_remote_copy(
                    src, first, halo_send.at[l, k], halo_recv.at[l, recv],
                    device_id=dev, device_id_type=MESH)

            self.up = copy(0, up_dev, border, 0)
            self.side = [copy(k, (z * 4 + quad[k], c), first, 1) for k in (1, 2, 3)]
            self.core = copy(4, core_dev, first, 2)

        def rise(self):
            @pl.when((q == 3) & (z < planes - 1))
            def _():
                self.up.start()

        def spread(self):
            @pl.when((q == 3) & (z > 0))
            def _():
                self.up.wait_recv()
                for m in self.side:
                    m.start()
                self.core.start()

        def swap(self):
            @pl.when((q != 3) & (z > 0))
            def _():
                self.side[0].wait_recv()
                self.core.start()

        def finish(self):
            @pl.when(z > 0)
            def _():
                self.core.wait()

            @pl.when((q == 3) & (z > 0))
            def _():
                for m in self.side:
                    m.wait_send()

            @pl.when((q == 3) & (z < planes - 1))
            def _():
                self.up.wait_send()

    def spot(b, j):
        return nrm.at[0, pl.ds(al(PAD + b * toks + j * unit, 32), unit), half_cols(c)]

    def to_far(j):
        own_near[j].wait_send()
        own_far.append(message(("g_far", j), spot(q, j), spot(q, j), far_dev, "ag"))

    def pass_on(j):
        own_near[j].wait_recv()
        passed.append(message(("g_pass", j), spot(near, j), spot(near, j), far_dev, "ag"))
        relays[1, j] = message(("c", 0), spot(near, j), spot(near, j), core_dev, "ag")

    def relay(which, j):
        (own_far if which == 2 else passed)[j].wait_recv()
        b = far if which == 2 else diag
        relays[which, j] = message(("c", 0), spot(b, j), spot(b, j), core_dev, "ag")

    def gate_part(l, t, plane, start, count, size):
        depth = pl.ds(al(plane * 4 * rows, 4 * rows), 4 * rows)

        def gate_step(r, _):
            at = pl.ds(al(start + r * size, 16), size)
            term = jnp.dot(nrm[l, at, depth], wvg[l, depth, :], preferred_element_type=F32)
            acc[at, :] = term if t == 0 else acc[at, :] + term
            return 0

        lax.fori_loop(0, count // size, gate_step, 0)

    for l in range(layers):
        last_layer = l + 1 == layers
        source = stream_in if l == 0 else strm.at[l - 1]

        if l == 0:
            pump(0, 0, 0, (0,))
            pump(0, 1, 0, (0,))
            for load in loads:
                load.wait()
            lax.fori_loop(0, toks // 64, norm_step, 0)

            @pl.when(z == 0)
            def _():
                for ll in range(layers):
                    nrm[ll, 0:PAD, :] = jnp.zeros((PAD, width), BF16)

            edge = Halo(0, nrm.at[0, pl.ds(group, PAD), half_cols(c)],
                        nrm.at[0, pl.ds(0, PAD), half_cols(c)])
            edge.rise()
            own_near = [message(("g_near", j), spot(q, j), spot(q, j), near_dev, ("near", j)) for j in range(2)]
            passed, relays, own_far = [], {}, []
            pump_early()
            edge.spread()
            to_far(0)
            to_far(1)
            pump(0, 0, 1)
            pass_on(0)
            pass_on(1)
            share(0, (2,))
            relay(2, 0)
            relay(2, 1)
            for t in range(2, planes - 1):
                pump(0, 0, t)
            relay(3, 0)
            relay(3, 1)
            for ll in range(1, layers):
                share(ll, (0, 1, 2))
            pump(0, 1, 0, (1, 2, 3))
            edge.swap()
            all_came(("c", 0), nrm.at[0, PAD:PAD + 3 * toks, 0:half])
            edge.finish()
            gate_part(0, 0, z, 0, total_rows, tile)
            for t in range(1, planes):
                for d in range(2):
                    @pl.when(holds(d, t))
                    def _(t=t, d=d):
                        consume_one(0, 0, t, d)
                        gate_part(0, t, z - t if d == 0 else z + t, 0, total_rows, tile)

            def gate_end(r, _):
                at = pl.ds(al(r * tile, 16), tile)
                gated = (acc[at, :ch] * jax.nn.sigmoid(acc[at, ch:])).astype(BF16)
                gat[at, :] = gated.astype(F32)
                return 0

            lax.fori_loop(0, total_rows // tile, gate_end, 0)
            pump(0, 1, 1)

        lead = PAD - (taps_n - 1)
        step_rows = 128

        def conv_step(r, _):
            at = al(r * step_rows, step_rows)
            for lane in range(ch // lanes):
                cut = slice(lane * lanes, (lane + 1) * lanes)
                total = [None, None]
                block = gat[pl.ds(at, step_rows + PAD), cut]
                for b in range(8):
                    moved = block if b == 0 else pltpu.roll(block, step_rows + PAD - b, 0)
                    for a in range(PAD // 8 + 1):
                        tap = 8 * a + b - lead
                        if 0 <= tap < taps_n:
                            term = taps[tap, l:l + 1, cut] * moved[8 * a:8 * a + step_rows]
                            total[a % 2] = term if total[a % 2] is None else total[a % 2] + term
                fil[pl.ds(at, step_rows), cut] = total[0] + total[1]
            return 0

        sums = []
        for part in range(PARTS):
            low, high = bounds[part:part + 2]
            lax.fori_loop(low // step_rows, high // step_rows, conv_step, 0)
            wide = fil[low:high, :]
            first_sum = jnp.sum(wide, axis=1, keepdims=True)
            second_sum = jnp.sum(wide * wide, axis=1, keepdims=True)
            lane_id = lax.broadcasted_iota(jnp.int32, (high - low, lanes), 1)
            stat = jnp.where(lane_id == 0, first_sum, jnp.where(lane_id == 1, second_sum, 0.0))
            ssend[l, :, low:high] = jnp.transpose(stat)[0:2, :]
            sums.append([message(("sum", part), ssend.at[l, :, low:high], srecv.at[l, k, :, low:high],
                                 dev, "sum") for k, dev in enumerate(plane_devs)])
        for t in range(2, planes - 1):
            pump(l, 1, t)
        if not last_layer:
            pump(l + 1, 0, 0)
        for part in range(PARTS):
            low, high = bounds[part:part + 2]
            all_came(("sum", part), srecv.at[l, :, :, low:high])
            whole = ssend[l, :, low:high]
            for k in range(len(plane_devs)):
                whole = whole + srecv[l, k, :, low:high]
            turn[0:2, low:high] = whole
            stat = jnp.transpose(turn[:, low:high])
            mean_value = stat[:, 0:1] / width
            variance = stat[:, 1:2] / width - mean_value * mean_value
            act[low:high, :] = jax.nn.silu((fil[low:high, :] - mean_value) * lax.rsqrt(variance + epsilon)
                                           * cgain[l:l + 1, :]).astype(BF16)

        def out_cols(h, u):
            return pl.ds(al(plane_at(u) * 4 * rows + h * chunk, chunk), chunk)

        def stage_swap(u):
            if u > 0:
                consume(l, 1, u)
            weights = wo[l, :, out_cols(1 - c, u)]
            for m, pair in enumerate(((near, diag), (far, q))):
                for k, b in enumerate(pair):
                    dsend[l, u, m, k] = jnp.dot(act[block_rows(b), :], weights,
                                                preferred_element_type=F32).astype(BF16)
                swaps[u, m] = message(("swap", u, m), dsend.at[l, u, m], drecv.at[l, u, m], core_dev, "swap")

        def stage_first(u):
            weights = wo[l, :, out_cols(c, u)]

            def partial(b, m, k):
                return (jnp.dot(act[block_rows(b), :], weights, preferred_element_type=F32)
                        + drecv[l, u, m, k].astype(F32))

            swaps[u, 0].wait_recv()
            for k, b in enumerate((far, diag)):
                term = partial(b, 0, k).astype(BF16)
                for j in range(2):
                    asend[l, u, j, k] = term[j * unit:(j + 1) * unit]
            for j in range(2):
                firsts[u, j] = message(("first", u, j), asend.at[l, u, j], arecv.at[l, u, j], far_dev, "first")
            swaps[u, 1].wait_recv()
            through[u] = partial(near, 1, 0)
            mine[u] = partial(q, 1, 1) + source[:, out_cols(c, u)].astype(F32)

        def stage_take(u, j):
            span = slice(j * unit, (j + 1) * unit)
            firsts[u, j].wait_recv()
            bsend[l, u, j] = (through[u, span] + arecv[l, u, j, 1].astype(F32)).astype(BF16)
            mine[u, span] = mine[u, span] + arecv[l, u, j, 0].astype(F32)

        def stage_give(u, j):
            seconds[u, j] = message(("second", u, j), bsend.at[l, u, j], brecv.at[l, u, j], near_dev,
                                    "second")

        def stage_last(u, j):
            span = slice(j * unit, (j + 1) * unit)
            seconds[u, j].wait_recv()
            final = (mine[u, span] + brecv[l, u, j].astype(F32)).astype(BF16)
            strm[l, span, out_cols(c, u)] = final
            if last_layer:
                piece, place = strm.at[l, span, out_cols(c, u)], out.at[span, out_cols(c, u)]
                message(("c", 0), piece, place, core_dev, "last")
                pltpu.make_async_copy(piece, place, out_sem.at[0]).start()
            else:
                wide = final.astype(F32)
                nrm[l + 1, pl.ds(al(PAD + q * toks + j * unit, 32), unit), out_cols(c, u)] = (
                    wide * gain[l + 1:l + 2, out_cols(c, u)]).astype(BF16)
                square = wide * wide
                folded = sum(square[:, k * lanes:(k + 1) * lanes] for k in range(chunk // lanes))
                squares[span, :] = folded if u == 0 else squares[span, :] + folded

        def lot(b, u):
            return nrm.at[l + 1, pl.ds(al(PAD + b * toks, 32), toks), out_cols(c, u)]

        def pass_chunk(kind, u, b, dev):
            moves[kind, u] = message((kind if kind[0] == "g" else "c", u), lot(b, u), lot(b, u), dev, kind[0])

        def gather(u):
            pass_chunk("g_near", u, q, near_dev)
            pass_chunk("c_own", u, q, core_dev)

        def forward(u):
            moves["g_near", u].wait_recv()
            pass_chunk("g_far", u, q, far_dev)
            pass_chunk("g_pass", u, near, far_dev)
            pass_chunk("c_near", u, near, core_dev)

        def cross_far(u):
            moves["g_far", u].wait_recv()
            pass_chunk("c_far", u, far, core_dev)

        def cross_diag(u):
            moves["g_pass", u].wait_recv()
            pass_chunk("c_diag", u, diag, core_dev)

        def gate_chunk(u):
            if u > 0:
                consume(l + 1, 0, u)
            all_came(("c", u), nrm.at[l + 1, PAD:PAD + group, 0:chunk])
            gate_part(l + 1, u, plane_at(u), PAD, group, toks)

        def send_squares():
            lane_id = lax.broadcasted_iota(jnp.int32, (toks, lanes), 1)
            total = jnp.sum(squares[...], axis=1, keepdims=True)
            qsend[l] = jnp.transpose(jnp.where(lane_id == 0, total, 0.0))[0:2, :]
            return [message(("square", k > 0), qsend.at[l], qrecv.at[l, k], dev, "square")
                    for k, dev in enumerate(plane_devs)]

        def row_scale(whole):
            turn[0:2, 0:toks] = whole
            return lax.rsqrt(jnp.transpose(turn[:, 0:toks])[:, 0:1] / width + epsilon)

        def send_edge(edge):
            norms[0].wait_recv()
            scale = row_scale(qsend[l] + qrecv[l, 0])[toks - PAD:]
            for u in range(planes):
                edge_out[l, :, pl.ds(al(plane_at(u) * chunk, chunk), chunk)] = (
                    strm[l, toks - PAD:, out_cols(c, u)].astype(F32) * scale
                    * gain[l + 1:l + 2, out_cols(c, u)]).astype(BF16)
            edge.rise()

        def gate_final(edge):
            u = planes - 1
            consume(l + 1, 0, u)
            edge.finish()

            @pl.when(z > 0)
            def _():
                for p in range(planes):
                    for h in range(2):
                        at = p * 4 * rows + h * chunk
                        nrm[l + 1, 0:PAD, at:at + chunk] = edge_in[l, h, :, p * chunk:(p + 1) * chunk]

            both = jnp.dot(nrm[l + 1, 0:PAD, :], wvg[l + 1], preferred_element_type=F32)
            gat[0:PAD, :] = (both[:, :ch] * jax.nn.sigmoid(both[:, ch:])).astype(BF16).astype(F32)
            all_came(("square", True), qrecv.at[l, 1:])
            all_came(("c", u), nrm.at[l + 1, PAD:PAD + group, 0:chunk])
            depth = pl.ds(al(plane_at(u) * 4 * rows, 4 * rows), 4 * rows)
            for k in range(4):
                mate = qsend[l] if k == 0 else qrecv[l, 2 * k - 1]
                scale = row_scale(mate + qrecv[l, 2 * k])
                at = pl.ds(al(PAD + quad[k] * toks, 32), toks)
                both = acc[at, :] + jnp.dot(nrm[l + 1, at, depth], wvg[l + 1, depth, :],
                                            preferred_element_type=F32)
                value, gate = both[:, :ch] * scale, both[:, ch:] * scale
                gat[at, :] = (value * jax.nn.sigmoid(gate)).astype(BF16).astype(F32)

        swaps, firsts, seconds, lasts, moves = {}, {}, {}, {}, {}
        for u in range(planes - 1):
            stage_swap(u)
            if u > 0:
                stage_first(u - 1)
        stage_first(planes - 2)
        stage_swap(planes - 1)
        stage_first(planes - 1)
        if last_layer:
            drain(l, 0)
            drain(l, 1)
            pltpu.make_async_remote_copy(
                wvg.at[:, 0:9 * rows // 2, :], wvg.at[:, 0:9 * rows // 2, :], wx_send.at[0],
                wx_recv.at[0], device_id=core_dev, device_id_type=MESH).wait_send()
            all_sent("ag", nrm.at[0, PAD:PAD + 5 * toks // 2, :])
            all_sent("sum", srecv)
            if layers > 1:
                all_sent("square", qrecv.at[0:layers - 1])
                all_sent("g", nrm.at[1:layers, PAD:PAD + 3 * toks, 0:half])
                all_sent("c", nrm.at[1:layers, PAD:PAD + group, 0:half])
        for u in range(planes - 1):
            for j in range(2):
                stage_take(u, j)
            if u + 2 == planes:
                for uu in range(planes - 1):
                    for j in range(2):
                        stage_give(uu, j)
        for j in range(2):
            stage_take(planes - 1, j)
            stage_give(planes - 1, j)
        if not last_layer:
            pump(l + 1, 0, 1)
        for u in range(planes):
            for j in range(2):
                stage_last(u, j)
            if not last_layer:
                gather(u)
                if u >= 2:
                    forward(u - 2)
        if not last_layer:
            edge = Halo(l + 1, edge_out.at[l], edge_in.at[l, c])
            norms = send_squares()
            cross_far(0)
            send_edge(edge)
            ahead = planes - 2
            for u in range(ahead, planes + ahead):
                if u < planes:
                    forward(u)
                    cross_far(u - ahead + 1)
                elif u - ahead + 1 < planes:
                    cross_far(u - ahead + 1)
                cross_diag(u - ahead)
                if u == ahead:
                    for t in range(2, planes - 1):
                        pump(l + 1, 0, t)
                if u == ahead + 1:
                    edge.spread()
                    pump(l + 1, 1, 0)
                if u - ahead < planes - 1:
                    gate_chunk(u - ahead)
                if u == ahead + 2:
                    drain(l, 0)
                    drain(l, 1)
            edge.swap()
            gate_final(edge)
            pump(l + 1, 1, 1)

    all_sent("swap", dsend)
    all_sent("first", asend)
    all_sent("second", bsend)
    all_sent("last", strm.at[layers - 1, :, 0:half])
    whole_half = strm.at[layers - 1, :, 0:half]
    pltpu.make_async_copy(whole_half, out.at[:, 0:half], out_sem.at[0]).wait()
    all_came(("c", 0), whole_half)


def fused(n, layers):
    def body(stream_in, norm_gain, value_weight, gate_weight, conv_taps, channel_gain, out_weight):
        toks, width = stream_in.shape
        taps_n = conv_taps.shape[1]
        rows, cols = value_weight.shape[1], value_weight.shape[2]
        ch, half, group, planes = cols // 4, width // 2, 4 * toks, n // 4
        chunk = 2 * rows
        taps = jnp.transpose(conv_taps, (1, 0, 2))
        hbm = pl.BlockSpec(memory_space=pltpu.HBM)
        msgs = 2 + PARTS + 10 * planes
        return pl.pallas_call(
            functools.partial(kernel, n, layers, taps_n),
            out_shape=jax.ShapeDtypeStruct((toks, width), BF16),
            in_specs=[hbm] * 7,
            out_specs=hbm,
            scratch_shapes=[
                pltpu.VMEM((toks, width), BF16),
                pltpu.VMEM((layers, width), F32),
                pltpu.VMEM((taps_n, layers, ch), F32),
                pltpu.VMEM((layers, ch), F32),
                pltpu.VMEM((layers, width, 2 * ch), BF16),
                pltpu.VMEM((layers, ch, width), BF16),
                pltpu.VMEM((layers, PAD + group, width), BF16),
                pltpu.VMEM((PAD + group, ch), F32),
                pltpu.VMEM((group, ch), F32),
                pltpu.VMEM((group, ch), BF16),
                pltpu.VMEM((layers, 2, group), F32),
                pltpu.VMEM((layers, 7, 2, group), F32),
                pltpu.VMEM((layers, planes, 2, 2, toks, chunk), BF16),
                pltpu.VMEM((layers, planes, 2, 2, toks, chunk), BF16),
                pltpu.VMEM((layers, planes, 2, 2, toks // 2, chunk), BF16),
                pltpu.VMEM((layers, planes, 2, 2, toks // 2, chunk), BF16),
                pltpu.VMEM((layers, planes, 2, toks // 2, chunk), BF16),
                pltpu.VMEM((layers, planes, 2, toks // 2, chunk), BF16),
                pltpu.VMEM((planes, toks, chunk), F32),
                pltpu.VMEM((planes, toks, chunk), F32),
                pltpu.VMEM((layers, toks, width), BF16),
                pltpu.VMEM((PAD + group, 2 * ch), F32),
                pltpu.VMEM((128, group), F32),
                pltpu.VMEM((toks, 128), F32),
                pltpu.VMEM((layers, 2, toks), F32),
                pltpu.VMEM((layers, 7, 2, toks), F32),
                pltpu.VMEM((layers, PAD, half), BF16),
                pltpu.VMEM((layers, 2, PAD, half), BF16),
                pltpu.SemaphoreType.DMA((4,)),
                pltpu.SemaphoreType.DMA((1,)),
                pltpu.SemaphoreType.DMA((layers * 3,)),
                pltpu.SemaphoreType.DMA((1,)),
                pltpu.SemaphoreType.DMA((7 + 2 * layers,)),
                pltpu.SemaphoreType.DMA((layers * 4, planes - 1)),
                pltpu.SemaphoreType.DMA((layers * 4, planes - 1, 2)),
                pltpu.SemaphoreType.DMA((layers, 5)),
                pltpu.SemaphoreType.DMA((layers, 3)),
                pltpu.SemaphoreType.DMA((11,)),
                pltpu.SemaphoreType.DMA((msgs,)),
            ],
            compiler_params=pltpu.CompilerParams(
                collective_id=0, has_side_effects=True, vmem_limit_bytes=62 * 2**20),
        )(stream_in, norm_gain, value_weight, gate_weight, taps, channel_gain, out_weight)

    return body


def passed_along(value, axis, steps):
    count = lax.axis_size(axis)
    leading, last = (max(0, -steps), min(count, count - steps))
    return lax.ppermute(value, axis, [(source, source + steps) for source in range(leading, last)])


def general(stream_in, norm_gain, value_weight, gate_weight, conv_taps, channel_gain, out_weight):
    stream = stream_in
    tok_rows = stream_in.shape[0]
    width = stream_in.shape[1]
    taps_n = conv_taps.shape[1]
    local_cols = value_weight.shape[2]
    for layer in range(norm_gain.shape[0]):
        wide = stream.astype(F32)
        normed = (
            wide
            * lax.rsqrt(jnp.mean(wide * wide, axis=1, keepdims=True) + epsilon)
            * norm_gain[layer]
        ).astype(BF16)
        value = jnp.dot(normed, lax.all_gather(value_weight[layer], "sp", axis=0, tiled=True),
                        preferred_element_type=F32)
        gate = jnp.dot(normed, lax.all_gather(gate_weight[layer], "sp", axis=0, tiled=True),
                       preferred_element_type=F32)
        gated = (value * jax.nn.sigmoid(gate)).astype(BF16)
        earlier = passed_along(gated[tok_rows - (taps_n - 1):], "sp", 1)
        padded = jnp.concatenate([earlier, gated], axis=0).astype(F32)
        taps = conv_taps[layer]
        filtered = jnp.zeros((tok_rows, local_cols), F32)
        for tap in range(taps_n):
            filtered = filtered + taps[tap] * padded[tap:tap + tok_rows]
        sum_first, sum_second = lax.psum(
            (jnp.sum(filtered, axis=1), jnp.sum(filtered * filtered, axis=1)), "tp")
        mean_value = (sum_first / width)[:, None]
        variance = (sum_second / width)[:, None] - mean_value * mean_value
        activated = jax.nn.silu(
            (filtered - mean_value) * lax.rsqrt(variance + epsilon) * channel_gain[layer]
        ).astype(BF16)
        whole_out = lax.all_gather(out_weight[layer], "sp", axis=1, tiled=True)
        terms = jnp.dot(activated, whole_out, preferred_element_type=F32)
        summed = lax.psum(terms.astype(BF16), "tp").astype(F32)
        stream = (wide + summed).astype(BF16)
    return stream


def solution(mesh):
    n, tp = mesh.shape["sp"], mesh.shape["tp"]

    def body(stream_in, norm_gain, value_weight, *rest):
        rows, cols = value_weight.shape[1], value_weight.shape[2]
        quads = tp == 2 and n % 4 == 0 and n >= 8 and rows % 128 == 0 and cols % 512 == 0
        fits = stream_in.shape[0] % 64 == 0 and rest[1].shape[1] <= PAD
        chosen = fused(n, norm_gain.shape[0]) if quads and fits else general
        return chosen(stream_in, norm_gain, value_weight, *rest)

    return jax.shard_map(
        body,
        mesh=mesh,
        in_specs=(
            P("sp", None),
            P(),
            P(None, "sp", "tp"),
            P(None, "sp", "tp"),
            P(None, None, "tp"),
            P(None, "tp"),
            P(None, "tp", "sp"),
        ),
        out_specs=P("sp", None),
        check_vma=False,
    )
```
